32 devices in a mesh: grp: 2 (over y), st: 8 (over z, core), tp: 2 (over x).
Axes of the slice: x: 2, y: 2, z: 4, core: 2. Of those that a mesh axis runs over, the one named last changes fastest.
Arguments:
- tokens: bfloat16 [8192, 2048], P(('grp', 'st')), parts along dimension 0, may hold values from -6 to 6
- owners: int32 [128, 4], P(('grp', 'st')), parts along dimension 0, may hold values from 0 to 7, all different within a row; in each aligned block of 8 rows (0 to 7, 8 to 15, ...) at most 8 rows name the same one
- entries: int32 [128, 4], P(('grp', 'st')), parts along dimension 0, may hold values from 0 to 15
- store: bfloat16 [256, 64, 2048], P(('grp', 'st')), parts along dimension 0, may hold values from -600 to 600
- mixer_query_weight: bfloat16 [2048, 1024], P(None, 'tp'), may hold values from -0.125 to 0.125
- mixer_key_weight: bfloat16 [2048, 1024], P(None, 'tp'), may hold values from -0.125 to 0.125
- mixer_value_weight: bfloat16 [2048, 1024], P(None, 'tp'), may hold values from -0.125 to 0.125
- strength_weight: bfloat16 [2048, 8], P(None, 'tp'), may hold values from -0.125 to 0.125
- decay_weight: bfloat16 [2048, 8], P(None, 'tp'), may hold values from -0.125 to 0.125
- head_decay_rate: float32 [8], P('tp'), may hold values from 0.003 to 0.15
- extra_forgetting_exponent: float32 [8192, 8], P(('grp', 'st'), 'tp'), parts along dimension 0, may hold values from -0.7 to 0
- output_norm_gain: float32 [128], replicated, may hold values from 0.1 to 1.9
- retrieval_query_weight: bfloat16 [2048, 1024], P(None, 'tp'), may hold values from -0.125 to 0.125
- passage_key_weight: bfloat16 [2048, 1024], P(None, 'tp'), may hold values from -0.125 to 0.125
- passage_value_weight: bfloat16 [2048, 1024], P(None, 'tp'), may hold values from -0.125 to 0.125
- retrieval_gate_weight: bfloat16 [2048, 8], P(None, 'tp'), may hold values from -0.125 to 0.125
Outputs:
- mixed: bfloat16 [8192, 1024], P(('grp', 'st'), 'tp'), parts along dimension 0
The draws below stay inside these ranges and needn't reach their ends.
There are 2 independent parts, one for each index of `grp`. The reference program is written for one: setup_inputs(seed, part) draws one part's arguments, and reference() takes and returns one part's arrays. A program takes and returns all parts, laid end to end along the dimension named above; an argument that names none is the same for every part. Nothing has to cross between parts.
Inputs may be any that keep to these rules, and one draw needn't show every extreme that they name: `owners`: each row names 4 different values; the rows of one device name no value more than 8 times, a bound that some device reaches; every value is named by some row.
All inputs are finite; a program needn't handle non-finite values.
Results may differ from the reference program's by a relative error of at most 0.015.
The reference program's roundings to bfloat16 on the way count: a program that leaves them out, or rounds other values in their place, can miss the bound.
Values may be sent and summed in bfloat16 or wider, within the bound.
A program may use at most 128 MiB of HBM per device.

```python
import math
import jax
import jax.numpy as jnp
import numpy as np
from jax import lax

D = 2048
ATTENTION_GROUPS = 8
FEATURE_WIDTH = 128
STREAM_LENGTH = 512
PASS_DEV = 16
BLOCK_TOKENS = 64
PER_BLOCK = 4
PASS_LEN = 64
POSITIONS_ALL = 4096
BLK_DEV = 8
BLOCKS = 64
PASSAGES = 128
CAP = 8
N_ST = 8


def draw_store(key, part):
    base_key = jax.random.fold_in(key, 0)
    shape = (PASSAGES, PASS_LEN, D)
    values = jnp.clip(jax.random.normal(base_key, shape, jnp.float32), -6.0, 6.0)
    return values.astype(jnp.bfloat16)


def draw_extra_forgetting_exponent(key, part):
    where_key, depth_key = jax.random.split(key, 2)
    shape = (POSITIONS_ALL, ATTENTION_GROUPS)
    struck = jax.random.uniform(where_key, shape, jnp.float32) < 1.0 / 128.0
    depth = jnp.log(jax.random.uniform(depth_key, shape, jnp.float32, 0.5, 0.8))
    return jnp.where(struck, depth, 0.0).astype(jnp.float32)


def touch_ends(values, key, low, largest):
    longest = values.shape.index(max(values.shape))
    spots = []
    for shift in (0, 1):
        where = [jax.random.randint(jax.random.fold_in(key, axis), (), 0, length) for axis, length in enumerate(values.shape)]
        where[longest] = (where[longest] + shift) % values.shape[longest]
        spots.append(tuple(where))
    return values.at[spots[0]].set(low).at[spots[1]].set(largest)


def block_scale(rng, extent, cuts, least, top_value):
    loudness = 1.0
    for position, blocks in cuts:
        steps = jax.random.uniform(jax.random.fold_in(jax.random.fold_in(rng, 6), position), (blocks,), jnp.float32, least / len(cuts), top_value / len(cuts))
        loudness = loudness * jnp.repeat(jnp.exp(steps), extent[position] // blocks).reshape((-1,) + (1,) * (len(extent) - 1 - position))
    return loudness


def deal_out(key, own, number, rows, number_of, top, most, lean):
    sequence = jax.random.permutation(key, number_of)
    heavy_load, common = portions_of(number_of, rows * top, most, lean, True), portions_of(number_of, rows * top, most, lean, False)
    places = jnp.arange(number_of)

    def named(tallies, offset_by):
        used = int((tallies > 0).sum())
        fixed = max(1, used // 4)
        moved = fixed + (places - fixed + offset_by * (used - fixed)) % max(1, number_of - fixed)
        return jnp.zeros((number_of,), jnp.int32).at[sequence[jnp.where(places < fixed, places, moved)]].set(jnp.asarray(tallies, jnp.int32))

    tallies = jnp.where(number % 4 == 0, named(heavy_load, number // 4), named(common, number - number // 4 - 1))
    mixed = jax.random.permutation(jax.random.fold_in(own, 3), number_of)
    donor, taker = mixed[0:number_of // 2 * 2:2], mixed[1:number_of // 2 * 2:2]
    room = jnp.minimum(tallies[donor] - 1, most - tallies[taker]) // 2
    room = jnp.where((donor == sequence[0]) | (taker == sequence[0]) | (tallies[taker] == 0), 0, jnp.maximum(room, 0))
    moved = jax.random.randint(jax.random.fold_in(own, 4), (number_of // 2,), 0, 1 << 20) % (room + 1)
    tallies = tallies.at[donor].add(-moved).at[taker].add(moved)
    members = jnp.searchsorted(jnp.cumsum(tallies), jnp.arange(rows * top), side="right").astype(jnp.int32)
    listing = members.reshape(top, rows).T
    listing = listing[jax.random.permutation(jax.random.fold_in(own, 1), rows)]
    offset_by = jax.random.randint(jax.random.fold_in(own, 2), (rows, 1), 0, top)
    return jnp.take_along_axis(listing, (jnp.arange(top)[None, :] + offset_by) % top, axis=1)


def portions_of(number_of, total, bound, lean, full):
    loads = [(1 << 20) // math.isqrt(standing ** lean) + 1 for standing in range(1, number_of + 1)]
    largest = bound if full else min(bound, max(-(-total // number_of), total * loads[0] // sum(loads)))
    least = 1 if total - largest >= number_of - 1 else 0
    counts, rest = [largest] + [least] * (number_of - 1), total - largest - least * (number_of - 1)
    while rest > 0:
        candidates = [i for i in range(1, number_of) if counts[i] < largest] or [i for i in range(1, number_of) if counts[i] < bound]
        pool, remaining = sum([loads[i] for i in candidates]), rest
        for i in candidates:
            addition = min(bound - counts[i], max(1, remaining * loads[i] // pool), rest)
            counts[i] = counts[i] + addition
            rest = rest - addition
    return np.array(counts)


def scatter_about(stream_key, extent, deviation, reach, shards=(), kind=jnp.bfloat16):
    gain = block_scale(stream_key, extent, shards, -0.22, 0.18) if shards else 1.0
    values = jax.random.normal(stream_key, extent, jnp.float32) * deviation * gain
    return jnp.minimum(jnp.maximum(values, -reach), reach).astype(kind)


def setup_inputs(seed: int = 0, part: int = 0) -> dict:
    keys = jax.random.split(jax.random.key(seed), 17)
    own_keys = jax.random.split(jax.random.fold_in(keys[16], part), 17)
    tokens = scatter_about(own_keys[0], (POSITIONS_ALL, D), 1.0, 6.0, ((0, 8),))
    owners_keys = jax.random.split(jax.random.fold_in(own_keys[1], 1), BLOCKS // BLK_DEV)
    owners_turns = jax.random.permutation(jax.random.fold_in(own_keys[1], 3), BLOCKS // BLK_DEV)
    owners = jax.vmap(lambda own, number: deal_out(jax.random.fold_in(own_keys[1], 2), own, number, BLK_DEV, N_ST, PER_BLOCK, CAP, 2))(owners_keys, owners_turns).reshape((BLOCKS, PER_BLOCK))
    entries = touch_ends(jax.random.randint(own_keys[2], (BLOCKS, PER_BLOCK), 0, PASS_DEV), jax.random.fold_in(own_keys[2], 1), 0, PASS_DEV - 1).astype(jnp.int32)
    store = draw_store(jax.random.fold_in(jax.random.fold_in(keys[16], part), 71), part)
    mixer_query_weight = scatter_about(keys[4], (D, ATTENTION_GROUPS * FEATURE_WIDTH), D ** -0.5, 0.125, ((1, 2),))
    mixer_key_weight = scatter_about(keys[5], (D, ATTENTION_GROUPS * FEATURE_WIDTH), D ** -0.5, 0.125, ((1, 2),))
    mixer_value_weight = scatter_about(keys[6], (D, ATTENTION_GROUPS * FEATURE_WIDTH), D ** -0.5, 0.125, ((1, 2),))
    strength_weight = scatter_about(keys[7], (D, ATTENTION_GROUPS), D ** -0.5, 0.125, ((1, 2),))
    decay_weight = scatter_about(keys[8], (D, ATTENTION_GROUPS), D ** -0.5, 0.125, ((1, 2),))
    head_decay_rate = jnp.clip(jnp.exp(math.log(0.15) - 3.912023 * jax.random.uniform(keys[9], (ATTENTION_GROUPS,), jnp.float32) ** block_scale(keys[9], (ATTENTION_GROUPS,), ((0, 2),), -0.2, 0.2)), 0.003, 0.15)
    extra_forgetting_exponent = draw_extra_forgetting_exponent(jax.random.fold_in(jax.random.fold_in(keys[16], part), 71), part)
    output_norm_gain = jnp.clip(1.0 + 0.18 * jax.random.normal(keys[11], (FEATURE_WIDTH,), jnp.float32), 0.1, 1.9)
    retrieval_query_weight = scatter_about(keys[12], (D, ATTENTION_GROUPS * FEATURE_WIDTH), D ** -0.5, 0.125, ((1, 2),))
    passage_key_weight = scatter_about(keys[13], (D, ATTENTION_GROUPS * FEATURE_WIDTH), D ** -0.5, 0.125, ((1, 2),))
    passage_value_weight = scatter_about(keys[14], (D, ATTENTION_GROUPS * FEATURE_WIDTH), D ** -0.5, 0.125, ((1, 2),))
    retrieval_gate_weight = scatter_about(keys[15], (D, ATTENTION_GROUPS), D ** -0.5, 0.125, ((1, 2),))
    return {"tokens": tokens, "owners": owners, "entries": entries, "store": store, "mixer_query_weight": mixer_query_weight, "mixer_key_weight": mixer_key_weight, "mixer_value_weight": mixer_value_weight, "strength_weight": strength_weight, "decay_weight": decay_weight, "head_decay_rate": head_decay_rate, "extra_forgetting_exponent": extra_forgetting_exponent, "output_norm_gain": output_norm_gain, "retrieval_query_weight": retrieval_query_weight, "passage_key_weight": passage_key_weight, "passage_value_weight": passage_value_weight, "retrieval_gate_weight": retrieval_gate_weight}


eps = 1e-06

def matmul_high(left, right):
    return jnp.einsum('...ij,...jk->...ik', left, right, precision=lax.Precision.HIGHEST)

def unit_lower_inverse(strict_part):
    size = strict_part.shape[-1]
    ident = jnp.eye(size, dtype=jnp.float32)
    inverse = ident - strict_part
    power = strict_part
    for level in range(size.bit_length() - 2):
        power = matmul_high(power, power)
        inverse = matmul_high(inverse, ident + power)
    return inverse

def delta_rule(queries, keys_in, values_in, decay_logarithm, strength, block_slice):
    length, heads, width = queries.shape
    count = length // block_slice

    def split(array):
        return array.reshape(count, block_slice, heads, array.shape[-1]).transpose(0, 2, 1, 3)
    q_blk = split(queries)
    k_blk = split(keys_in)
    v_blk = split(values_in)
    decay_blk = decay_logarithm.reshape(count, block_slice, heads).transpose(0, 2, 1)
    beta_blk = strength.reshape(count, block_slice, heads).transpose(0, 2, 1)
    cumul = jnp.cumsum(decay_blk, axis=-1)
    lower = jnp.tril(jnp.ones((block_slice, block_slice), bool))
    strict = jnp.tril(jnp.ones((block_slice, block_slice), bool), -1)
    spread = cumul[..., :, None] - cumul[..., None, :]
    damping = jnp.where(lower, jnp.exp(jnp.where(lower, spread, 0.0)), 0.0)
    k_beta = k_blk * beta_blk[..., None]
    inner = jnp.where(strict, matmul_high(k_beta, jnp.swapaxes(k_blk, -1, -2)) * damping, 0.0)
    inverse = unit_lower_inverse(inner)
    fresh_base = matmul_high(inverse, v_blk * beta_blk[..., None])
    key_mix = matmul_high(inverse, k_beta * jnp.exp(cumul)[..., None])
    within = jnp.where(lower, matmul_high(q_blk, jnp.swapaxes(k_blk, -1, -2)) * damping, 0.0)
    q_decayed = q_blk * jnp.exp(cumul)[..., None]
    k_tail = k_blk * jnp.exp(cumul[..., -1:] - cumul)[..., None]
    carry_decay = jnp.exp(cumul[..., -1])

    def advance(state, pieces):
        q_part, k_part, base_part, mix_part, within_part, decay_part = pieces
        fresh = base_part - matmul_high(mix_part, state)
        result = matmul_high(q_part, state) + matmul_high(within_part, fresh)
        state = state * decay_part[:, None, None] + matmul_high(jnp.swapaxes(k_part, -1, -2), fresh)
        return (state, result)
    start = jnp.zeros((heads, width, values_in.shape[-1]), jnp.float32)
    final, outputs = lax.scan(advance, start, (q_decayed, k_tail, fresh_base, key_mix, within, carry_decay))
    return outputs.transpose(0, 2, 1, 3).reshape(length, heads, values_in.shape[-1])

def mixer_head_outputs(tokens, mixer_query_weight, mixer_key_weight, mixer_value_weight, strength_weight, decay_weight, head_decay_rate, extra_forgetting_exponent, output_norm_gain, block_slice):
    heads = head_decay_rate.shape[0]
    head_dim = output_norm_gain.shape[0]
    length = tokens.shape[0]

    def project(weight):
        rounded = jnp.dot(tokens, weight, preferred_element_type=jnp.float32).astype(jnp.bfloat16)
        return lax.optimization_barrier(rounded).astype(jnp.float32).reshape(length, heads, head_dim)

    def unit_rows(array):
        return array * lax.rsqrt(lax.optimization_barrier(jnp.sum(array * array, axis=-1, keepdims=True)) + eps)
    queries = unit_rows(project(mixer_query_weight)) * head_dim ** (-0.5)
    keys_in = unit_rows(project(mixer_key_weight))
    values_in = project(mixer_value_weight)
    strength = jax.nn.sigmoid(jnp.dot(tokens, strength_weight, preferred_element_type=jnp.float32))
    decay_logarithm = -head_decay_rate[None, :] * jax.nn.softplus(jnp.dot(tokens, decay_weight, preferred_element_type=jnp.float32)) + extra_forgetting_exponent
    recur = delta_rule(queries, keys_in, values_in, decay_logarithm, strength, block_slice)
    return recur * lax.rsqrt(lax.optimization_barrier(jnp.mean(recur * recur, axis=-1, keepdims=True)) + eps) * output_norm_gain

def reference(tokens, owners, entries, store, mixer_query_weight, mixer_key_weight, mixer_value_weight, strength_weight, decay_weight, head_decay_rate, extra_forgetting_exponent, output_norm_gain, retrieval_query_weight, passage_key_weight, passage_value_weight, retrieval_gate_weight):
    stream_group = tokens.reshape(N_ST, STREAM_LENGTH, D)
    forgetting_spikes = extra_forgetting_exponent.reshape(N_ST, STREAM_LENGTH, ATTENTION_GROUPS)

    def lone_stream(pair):
        return mixer_head_outputs(pair[0], mixer_query_weight, mixer_key_weight, mixer_value_weight, strength_weight, decay_weight, head_decay_rate, pair[1], output_norm_gain, BLOCK_TOKENS)
    rescaled_result = lax.map(lone_stream, (stream_group, forgetting_spikes)).reshape(POSITIONS_ALL, ATTENTION_GROUPS, FEATURE_WIDTH)
    flat_store = store.reshape(PASSAGES * PASS_LEN, D)
    pass_key = jnp.dot(flat_store, passage_key_weight, preferred_element_type=jnp.float32).astype(jnp.bfloat16).reshape(PASSAGES, PASS_LEN, ATTENTION_GROUPS * FEATURE_WIDTH)
    pass_value = jnp.dot(flat_store, passage_value_weight, preferred_element_type=jnp.float32).astype(jnp.bfloat16).reshape(PASSAGES, PASS_LEN, ATTENTION_GROUPS * FEATURE_WIDTH)
    passage = (owners.astype(jnp.int32) * PASS_DEV + entries.astype(jnp.int32)).astype(jnp.int32)
    keys_read = pass_key[passage].reshape(BLOCKS, PER_BLOCK * PASS_LEN, ATTENTION_GROUPS, FEATURE_WIDTH)
    values_read = pass_value[passage].reshape(BLOCKS, PER_BLOCK * PASS_LEN, ATTENTION_GROUPS, FEATURE_WIDTH)
    rquery = jnp.dot(tokens, retrieval_query_weight, preferred_element_type=jnp.float32).astype(jnp.bfloat16).reshape(BLOCKS, BLOCK_TOKENS, ATTENTION_GROUPS, FEATURE_WIDTH)
    scores = jnp.einsum('bqhd,bkhd->bhqk', rquery.astype(jnp.float32), keys_read.astype(jnp.float32)) * FEATURE_WIDTH ** (-0.5)
    peak = lax.optimization_barrier(jnp.max(scores, axis=-1, keepdims=True))
    expo = jnp.exp(scores - peak)
    weights = (expo / lax.optimization_barrier(jnp.sum(expo, axis=-1, keepdims=True))).astype(jnp.bfloat16)
    retrieved = jnp.einsum('bhqk,bkhd->bqhd', weights.astype(jnp.float32), values_read.astype(jnp.float32)).reshape(POSITIONS_ALL, ATTENTION_GROUPS, FEATURE_WIDTH)
    rgate = jax.nn.sigmoid(jnp.dot(tokens, retrieval_gate_weight, preferred_element_type=jnp.float32))
    mixed = rescaled_result + rgate[..., None] * retrieved
    return mixed.reshape(POSITIONS_ALL, ATTENTION_GROUPS * FEATURE_WIDTH).astype(jnp.bfloat16)
```

```python
import functools

import jax
import jax.numpy as jnp
from jax import lax
from jax.experimental import pallas as pl
from jax.experimental.pallas import tpu as pltpu
from jax.sharding import PartitionSpec as P

BLOCK = 64
EPS = 1e-06
MISSING = -1e30
F32 = jnp.float32
BF16 = jnp.bfloat16
SPAN = 128


def dot_nn(left, right):
    return jnp.dot(left, right, preferred_element_type=F32)


def dot_nt(left, right):
    return lax.dot_general(left, right, (((1,), (1,)), ((), ())), preferred_element_type=F32)


def dot_tn(left, right):
    return lax.dot_general(left, right, (((0,), (0,)), ((), ())), preferred_element_type=F32)


def attend_unit(q_ref, named, me, sibling, kv_own, kv_sib, o_ref, stat_ref, passage_rows, head_dim):
    length, half = q_ref.shape
    heads = half // head_dim
    blocks = length // BLOCK
    scale = head_dim ** (-0.5)
    nothing = jnp.zeros((BLOCK, head_dim), BF16)

    def find(pairs, device):
        hit = jnp.int32(0)
        for owner, entry in pairs:
            hit = hit + (owner == device).astype(jnp.int32) * (entry + 1)
        found = jnp.minimum(hit, 1)
        return hit - found, (1 - found).astype(F32) * MISSING

    places, scores = [], []
    for block in range(blocks):
        pairs = named(block)
        row_own, bias_own = find(pairs, me)
        row_sib, bias_sib = find(pairs, sibling)
        places.append((row_own, bias_own, row_sib, bias_sib))
        query = q_ref[block * BLOCK : (block + 1) * BLOCK, :]
        spread = jnp.concatenate(
            [
                jnp.concatenate(
                    [
                        query[:, head * head_dim : (head + 1) * head_dim] if head == place else nothing
                        for place in range(heads)
                    ],
                    axis=1,
                )
                for head in range(heads)
            ],
            axis=0,
        )
        keys = jnp.concatenate(
            [
                kv_own[row_own, :, :half],
                kv_sib[row_sib, :, :half],
            ],
            axis=0,
        )
        scores.append(dot_nt(keys, spread))
    weights, stats = [], []
    for block in range(blocks):
        _, bias_own, _, bias_sib = places[block]
        raw = scores[block]
        own = raw[:passage_rows] * scale + bias_own
        sib = raw[passage_rows:] * scale + bias_sib
        peak = jnp.max(jnp.maximum(own, sib), axis=0, keepdims=True)
        e_own = jnp.exp(own - peak)
        e_sib = jnp.exp(sib - peak)
        total = jnp.sum(e_own + e_sib, axis=0, keepdims=True)
        inv = 1.0 / total
        weights.append(jnp.concatenate([e_own * inv, e_sib * inv], axis=0).astype(BF16))
        stats.append(peak + jnp.log(total))
    for block in range(blocks):
        row_own, _, row_sib, _ = places[block]
        values = jnp.concatenate(
            [
                kv_own[row_own, :, half:],
                kv_sib[row_sib, :, half:],
            ],
            axis=0,
        )
        result = dot_tn(weights[block], values)
        for head in range(heads):
            cols = slice(head * head_dim, (head + 1) * head_dim)
            o_ref[block * BLOCK : (block + 1) * BLOCK, cols] = result[
                head * BLOCK : (head + 1) * BLOCK, cols
            ].astype(BF16)
    rows = jnp.concatenate(stats, axis=0)
    spare = stat_ref.shape[1] - rows.shape[1]
    if spare:
        rows = jnp.concatenate([rows, jnp.zeros((blocks, spare), F32)], axis=1)
    stat_ref[...] = rows


def gate_rows(gates, extra_ref, rate_ref):
    heads, length = extra_ref.shape
    rows = jnp.transpose(gates)
    beta = jax.nn.sigmoid(rows[:heads])
    raw = rows[heads : 2 * heads]
    softplus = jnp.maximum(raw, 0.0) + jnp.log1p(jnp.exp(-jnp.abs(raw)))
    which = lax.broadcasted_iota(jnp.int32, (heads, length), 0)
    rate = jnp.zeros((heads, length), F32)
    for head in range(heads):
        rate = jnp.where(which == head, rate_ref[head], rate)
    decay = -rate * softplus + extra_ref[...]
    rgate = jax.nn.sigmoid(rows[2 * heads : 3 * heads])
    tri = jnp.where(
        lax.broadcasted_iota(jnp.int32, (SPAN, SPAN), 0)
        <= lax.broadcasted_iota(jnp.int32, (SPAN, SPAN), 1),
        1.0,
        0.0,
    ).astype(F32)
    pad = jnp.zeros((8 - heads, SPAN), F32)
    spans = []
    for span in range(length // SPAN):
        at = slice(span * SPAN, (span + 1) * SPAN)
        cum = jnp.dot(
            jnp.concatenate([decay[:, at], pad], axis=0),
            tri,
            precision=lax.Precision.HIGHEST,
            preferred_element_type=F32,
        )[:heads]
        ends = cum[:, SPAN - 1 : SPAN]
        grow = jnp.exp(cum)
        cols = jnp.transpose(jnp.concatenate([cum, beta[:, at], grow, rgate[:, at]], axis=0))
        spans.append((cum, beta[:, at], beta[:, at] * grow, jnp.exp(ends - cum), jnp.exp(ends), cols))
    return spans


def delta_body(spans, read, gain, heads, store):
    head_dim = gain.shape[1]
    count = len(spans)
    half = SPAN // 2
    row = lax.broadcasted_iota(jnp.int32, (SPAN, SPAN), 0)
    col = lax.broadcasted_iota(jnp.int32, (SPAN, SPAN), 1)
    lower = row >= col
    strict = row > col
    prow = lax.broadcasted_iota(jnp.int32, (half, SPAN), 0)
    plane = lax.broadcasted_iota(jnp.int32, (half, SPAN), 1)
    pcol = plane % half
    is_left = plane < half
    left = jnp.where(is_left, 1.0, 0.0).astype(BF16)
    right = jnp.where(is_left, 0.0, 1.0).astype(BF16)
    eye = jnp.where(prow == pcol, 1.0, 0.0).astype(F32)
    sizes = []
    size = 2
    while size < half:
        sizes.append(size)
        size *= 2

    def cut_of(size):
        return ((prow // (2 * size)) == (pcol // (2 * size))) & ((prow // size) != (pcol // size))

    first = jnp.where(cut_of(1), 1.0, 0.0).astype(F32)
    cuts = []
    for size in sizes:
        cut = jnp.where(cut_of(size), 1.0, 0.0).astype(BF16)
        cuts.append((cut * left, cut * right))
    units = [(head, span) for head in range(heads) for span in range(count)]
    kb, kt, grams, mixes = {}, {}, {}, {}
    for unit in units:
        k32 = read("k", *unit).astype(F32)
        kn = k32 * lax.rsqrt(jnp.sum(k32 * k32, axis=1, keepdims=True) + EPS)
        kb[unit] = kn.astype(BF16)
        kt[unit] = jnp.transpose(kn)
    for unit in units:
        turned = kt[unit].astype(BF16)
        grams[unit] = dot_nn(kb[unit], turned)
        mixes[unit] = dot_nn(read("q", *unit), turned)
    within, packed, corner, inverse = {}, {}, {}, {}
    for unit in units:
        head, span = unit
        cum, _, _, _, _, cols = spans[span]
        spread = cols[:, head : head + 1] - cum[head : head + 1, :]
        damp = jnp.where(lower, jnp.exp(jnp.minimum(spread, 0.0)), 0.0)
        within[unit] = (mixes[unit] * damp).astype(BF16)
        inner = jnp.where(strict, grams[unit] * damp * cols[:, heads + head : heads + head + 1], 0.0)
        pack = jnp.where(is_left, inner[:half], inner[half:])
        packed[unit] = pack.astype(BF16)
        corner[unit] = jnp.where(is_left, inner[half:], 0.0).astype(BF16)
        inverse[unit] = eye - pack * first
    for cut_left, cut_right in cuts:
        parts = {}
        for unit in units:
            piece = packed[unit]
            parts[unit] = dot_nn(
                inverse[unit].astype(BF16),
                jnp.concatenate([piece * cut_left, piece * cut_right], axis=0),
            )
        for unit in units:
            now = inverse[unit].astype(BF16)
            inverse[unit] = inverse[unit] - dot_nn(
                parts[unit].astype(BF16), jnp.concatenate([now * left, now * right], axis=0)
            )
    parts = {}
    for unit in units:
        now = inverse[unit].astype(BF16)
        parts[unit] = dot_nn(corner[unit], jnp.concatenate([now * left, now * right], axis=0))
    zeros = jnp.zeros((half, SPAN), BF16)
    full = {}
    for unit in units:
        now = inverse[unit]
        link = dot_nn(
            now.astype(BF16) * right, jnp.concatenate([zeros, parts[unit].astype(BF16)], axis=0)
        )
        full[unit] = jnp.concatenate(
            [jnp.where(is_left, now, 0.0), jnp.where(is_left, -link, now)], axis=0
        )
    base, key_mix, tails = {}, {}, {}
    for unit in units:
        head, span = unit
        _, beta, beta_grow, tail, _, _ = spans[span]
        base[unit] = dot_nn((full[unit] * beta[head : head + 1, :]).astype(BF16), read("v", *unit))
        key_mix[unit] = dot_nn(
            (full[unit] * beta_grow[head : head + 1, :]).astype(BF16), kb[unit]
        ).astype(BF16)
        tails[unit] = (kt[unit] * tail[head : head + 1, :]).astype(BF16)
    state = [jnp.zeros((head_dim, head_dim), F32) for _ in range(heads)]
    for span in range(count):
        reads = [
            dot_nn(
                jnp.concatenate([key_mix[head, span], read("q", head, span)], axis=0),
                state[head].astype(BF16),
            )
            for head in range(heads)
        ]
        fresh = [(base[head, span] - reads[head][:SPAN]).astype(BF16) for head in range(heads)]
        carry = spans[span][4]
        state = [
            state[head] * carry[head : head + 1, :] + dot_nn(tails[head, span], fresh[head])
            for head in range(heads)
        ]
        for head in range(heads):
            cols = spans[span][5]
            grow = cols[:, 2 * heads + head : 2 * heads + head + 1]
            result = reads[head][SPAN:] * grow + dot_nn(within[head, span], fresh[head])
            q32 = read("q", head, span).astype(F32)
            square = jnp.sum(q32 * q32, axis=1, keepdims=True)
            norm = lax.rsqrt(
                jnp.mean(result * result, axis=1, keepdims=True)
                + EPS * head_dim * (square + EPS)
            )
            store(head, span, result * norm * gain)


def whole_kernel(
    chips,
    head_dim,
    passage_rows,
    owners_ref,
    entries_ref,
    extra_ref,
    small_refs,
    gain_ref,
    rate_ref,
    tokens_hbm,
    store_hbm,
    weights_hbm,
    o_ref,
    tok,
    sto,
    wts,
    rq,
    qkv,
    kv_own,
    kv_sib,
    kv_out,
    qbuf,
    obuf,
    sbuf,
    part,
    pstat,
    normed,
    want_mine,
    want_all,
    want_smem,
    load_sem,
    want_sem,
    kv_sem,
    send_q,
    recv_q,
    send_r,
    recv_r,
    send_s,
    recv_s,
    send_w,
    recv_w,
):
    devices = 2 * chips
    reach = chips // 2
    me = lax.axis_index("st")
    core, chip = lax.rem(me, 2), me // 2
    other = 1 - core
    sibling = chip * 2 + other
    length, width = normed.shape
    half = width // 2
    heads = width // head_dim

    def device(dz, which):
        return lax.rem(chip + dz, chips) * 2 + which

    def rcopy(src, dst, ssem, rsem, target):
        return pltpu.make_async_remote_copy(
            src_ref=src,
            dst_ref=dst,
            send_sem=ssem,
            recv_sem=rsem,
            device_id={"st": target},
            device_id_type=pl.DeviceIdType.MESH,
        )

    barrier = pltpu.get_barrier_semaphore()

    @pl.loop(1, devices)
    def _(off):
        pl.semaphore_signal(
            barrier,
            inc=1,
            device_id={"st": lax.rem(me + off, devices)},
            device_id_type=pl.DeviceIdType.MESH,
        )

    rq_w, pk_w, pv_w, q_w = 0, 1, 2, 3
    loads = [pltpu.make_async_copy(tokens_hbm, tok, load_sem.at[0])]
    loads += [
        pltpu.make_async_copy(weights_hbm[i], wts.at[i], load_sem.at[1 + i]) for i in range(6)
    ]
    loads.append(pltpu.make_async_copy(store_hbm, sto, load_sem.at[7]))
    loads[0].start()
    loads[1].start()

    want_mine[...] = jnp.zeros_like(want_mine)
    per = owners_ref.shape[0]
    blocks = owners_ref.shape[1]
    want_mine[:per, :blocks] = owners_ref[...]
    want_mine[per : 2 * per, :blocks] = entries_ref[...]
    want_all[me] = want_mine[...]

    loads[0].wait()
    loads[1].wait()
    loads[7].start()
    loads[1 + pk_w].start()
    loads[1 + pv_w].start()

    @pl.loop(0, 2)
    def _(side):
        cols = pl.ds(pl.multiple_of(side * half, half), half)
        rq[side] = dot_nn(tok[...], wts[rq_w, :, cols]).astype(BF16)

    pl.semaphore_wait(barrier, devices - 1)

    def slot(dz, which):
        return (dz % chips) * 2 + which

    hop1 = []
    for count, (dz, which) in enumerate(
        [(1, core), (chips - 1, other), (1, other), (chips - 1, core)]
    ):
        there = slot(chips - dz, core)
        hop1.append(
            rcopy(
                rq.at[which], qbuf.at[there], send_q.at[count], recv_q.at[there], device(dz, which)
            )
        )
    hop1.append(
        rcopy(rq.at[other], qbuf.at[core], send_q.at[4], recv_q.at[core], sibling)
    )
    for copy in hop1:
        copy.start()

    def want_copy(off):
        return rcopy(
            want_mine,
            want_all.at[me],
            send_w.at[off - 1],
            recv_w.at[me],
            lax.rem(me + off, devices),
        )

    @pl.loop(1, devices)
    def _(off):
        want_copy(off).start()

    qbuf[core] = rq[core]

    loads[7].wait()
    loads[1 + pk_w].wait()
    for i in range(3):
        loads[1 + q_w + i].start()

    rows = sto.shape[0]
    tile = min(512, rows)

    def project_store(which, weight, dst, place):
        cols = pl.ds(pl.multiple_of(which * half, half), half)

        @pl.loop(0, rows // tile)
        def _(m):
            at = pl.ds(pl.multiple_of(m * tile, tile), tile)
            held = dot_nn(sto[at, :], wts[weight, :, cols]).astype(BF16)
            count = tile // passage_rows
            dst[pl.ds(m * count, count), :, place * half : (place + 1) * half] = held.reshape(
                count, passage_rows, half
            )

    project_store(other, pk_w, kv_out, 0)
    loads[1 + pv_w].wait()
    project_store(other, pv_w, kv_out, 1)
    project_store(core, pk_w, kv_own, 0)
    swap = rcopy(kv_out, kv_sib, kv_sem.at[0], kv_sem.at[1], sibling)
    swap.start()
    project_store(core, pv_w, kv_own, 1)

    for i in range(3):
        loads[1 + q_w + i].wait()

    @pl.loop(0, 6)
    def _(step):
        i, side = step // 2, lax.rem(step, 2)
        cols = pl.ds(pl.multiple_of(side * half, half), half)
        qkv[i, :, cols] = dot_nn(tok[...], wts[q_w + i, :, cols]).astype(BF16)

    small = jnp.concatenate(
        [ref[...] for ref in small_refs] + [jnp.zeros((16 - 3 * heads, tok.shape[1]), BF16)], axis=0
    )
    gates = dot_nt(tok[...], small)
    spans = gate_rows(gates, extra_ref, rate_ref)

    @pl.loop(1, devices)
    def _(off):
        source = lax.rem(me + off, devices)
        rcopy(want_mine, want_all.at[source], send_w.at[0], recv_w.at[source], source).wait_recv()

    fetch = pltpu.make_async_copy(want_all, want_smem, want_sem)
    fetch.start()
    fetch.wait()
    swap.wait()

    def await_query(at):
        rcopy(rq.at[0], qbuf.at[at], send_q.at[0], recv_q.at[at], sibling).wait_recv()

    def attend(dz, which):
        at = slot(dz, which)
        source = device(dz, which)

        def named(block):
            return [
                (want_smem[source, place, block], want_smem[source, per + place, block])
                for place in range(per)
            ]

        attend_unit(
            qbuf.at[at],
            named,
            me,
            sibling,
            kv_own,
            kv_sib,
            obuf.at[at],
            sbuf.at[at],
            passage_rows,
            head_dim,
        )

    def reply(dz, which):
        at = slot(dz, which)
        back = (chips - dz) % chips
        target = device(dz, which)
        return (
            rcopy(
                obuf.at[at], part.at[back, core], send_r.at[at], recv_r.at[back, core], target
            ),
            rcopy(
                sbuf.at[at], pstat.at[back, core], send_s.at[at], recv_s.at[back, core], target
            ),
        )

    relays = []

    def relay(src, dst, count, target):
        copy = rcopy(qbuf.at[src], qbuf.at[dst], send_q.at[count], recv_q.at[dst], target)
        copy.start()
        relays.append(copy)

    count = 5
    await_query(other)

    @pl.loop(0, 2)
    def _(which):
        attend(0, which)

    part[0, core] = obuf[core]
    pstat[0, core] = sbuf[core]
    for copy in reply(0, other):
        copy.start()

    for hop in range(1, reach):
        back = chips - hop
        if hop < reach - 1:
            for which in range(2):
                await_query(slot(back, which))
                relay(slot(back, which), slot(back - 1, which), count, device(1, core))
                await_query(slot(hop, which))
                relay(slot(hop, which), slot(hop + 1, which), count + 1, device(chips - 1, core))
                count += 2
        else:
            await_query(slot(back, core))
            relay(slot(back, core), slot(reach, core), count, device(1, core))
            await_query(slot(hop, other))
            relay(slot(hop, other), slot(reach, other), count + 1, device(chips - 1, core))
            count += 2
            await_query(slot(back, other))
            await_query(slot(hop, core))
        for dz in (back, hop):

            @pl.loop(0, 2)
            def _(which):
                attend(dz, which)
                for copy in reply(dz, which):
                    copy.start()

    await_query(slot(reach, 0))
    await_query(slot(reach, 1))

    @pl.loop(0, 2)
    def _(which):
        attend(reach, which)
        for copy in reply(reach, which):
            copy.start()

    def read(name, head, span):
        return qkv[
            "qkv".index(name),
            span * SPAN : (span + 1) * SPAN,
            head * head_dim : (head + 1) * head_dim,
        ]

    def keep(head, span, value):
        normed[span * SPAN : (span + 1) * SPAN, head * head_dim : (head + 1) * head_dim] = value

    delta_body(spans, read, gain_ref[...], heads, keep)

    def await_part(back, side):
        rcopy(
            obuf.at[0], part.at[back, side], send_r.at[0], recv_r.at[back, side], sibling
        ).wait_recv()
        rcopy(
            sbuf.at[0], pstat.at[back, side], send_s.at[0], recv_s.at[back, side], sibling
        ).wait_recv()

    await_part(0, other)
    for back in range(1, chips):
        for side in range(2):
            await_part(back, side)

    here = heads // 2
    for side in range(2):
        stats = [pstat[back, side] for back in range(chips)]
        peak = functools.reduce(jnp.maximum, stats)
        expo = [jnp.exp(stat - peak) for stat in stats]
        inv = 1.0 / functools.reduce(jnp.add, expo)
        shares = [jnp.transpose(e * inv) for e in expo]
        for block in range(blocks):
            at = slice(block * BLOCK, (block + 1) * BLOCK)
            span, inside = divmod(block * BLOCK, SPAN)
            for local in range(here):
                cols = slice(local * head_dim, (local + 1) * head_dim)
                head = side * here + local
                where = slice(head * head_dim, (head + 1) * head_dim)
                value = functools.reduce(
                    jnp.add,
                    [
                        part[back, side, at, cols].astype(F32)
                        * shares[back][local * BLOCK : (local + 1) * BLOCK, block : block + 1]
                        for back in range(chips)
                    ],
                )
                rgate = spans[span][5][
                    inside : inside + BLOCK, 3 * heads + head : 3 * heads + head + 1
                ]
                o_ref[at, where] = (normed[at, where] + rgate * value).astype(BF16)

    for copy in hop1 + relays:
        copy.wait_send()

    @pl.loop(1, devices)
    def _(off):
        want_copy(off).wait_send()

    for copy in reply(0, other):
        copy.wait_send()
    for dz in range(1, chips):
        for which in range(2):
            for copy in reply(dz, which):
                copy.wait_send()


def per_device(
    chips,
    tokens,
    owners,
    entries,
    store,
    mixer_query_weight,
    mixer_key_weight,
    mixer_value_weight,
    strength_weight,
    decay_weight,
    head_decay_rate,
    extra_forgetting_exponent,
    output_norm_gain,
    retrieval_query_weight,
    passage_key_weight,
    passage_value_weight,
    retrieval_gate_weight,
):
    heads = head_decay_rate.shape[0]
    head_dim = output_norm_gain.shape[0]
    length, depth = tokens.shape
    passage_rows = store.shape[1]
    rows = store.shape[0] * passage_rows
    width = heads * head_dim
    half = width // 2
    devices = 2 * chips
    blocks = owners.shape[0]
    vmem = pl.BlockSpec(memory_space=pltpu.VMEM)
    anywhere = pl.BlockSpec(memory_space=pl.ANY)
    weights = [
        retrieval_query_weight,
        passage_key_weight,
        passage_value_weight,
        mixer_query_weight,
        mixer_key_weight,
        mixer_value_weight,
    ]

    def body(owners_ref, entries_ref, extra_ref, s1, s2, s3, gain_ref, rate_ref, tok, sto, *rest):
        whole_kernel(
            chips, head_dim, passage_rows, owners_ref, entries_ref, extra_ref, (s1, s2, s3),
            gain_ref, rate_ref, tok, sto, rest[:6], *rest[6:],
        )

    dma = pltpu.SemaphoreType.DMA
    return pl.pallas_call(
        body,
        out_shape=jax.ShapeDtypeStruct((length, width), BF16),
        in_specs=[vmem] * 7 + [pl.BlockSpec(memory_space=pltpu.SMEM)] + [anywhere] * 8,
        out_specs=vmem,
        scratch_shapes=[
            pltpu.VMEM((length, depth), BF16),
            pltpu.VMEM((rows, depth), BF16),
            pltpu.VMEM((6, depth, width), BF16),
            pltpu.VMEM((2, length, half), BF16),
            pltpu.VMEM((3, length, width), BF16),
            pltpu.VMEM((store.shape[0], passage_rows, width), BF16),
            pltpu.VMEM((store.shape[0], passage_rows, width), BF16),
            pltpu.VMEM((store.shape[0], passage_rows, width), BF16),
            pltpu.VMEM((devices, length, half), BF16),
            pltpu.VMEM((devices, length, half), BF16),
            pltpu.VMEM((devices, blocks, 2 * BLOCK), F32),
            pltpu.VMEM((chips, 2, length, half), BF16),
            pltpu.VMEM((chips, 2, blocks, 2 * BLOCK), F32),
            pltpu.VMEM((length, width), F32),
            pltpu.VMEM((8, 128), jnp.int32),
            pltpu.VMEM((devices, 8, 128), jnp.int32),
            pltpu.SMEM((devices, 8, 128), jnp.int32),
            dma((8,)),
            dma,
            dma((2,)),
            dma((5 + 2 * devices,)),
            dma((devices,)),
            dma((devices,)),
            dma((chips, 2)),
            dma((devices,)),
            dma((chips, 2)),
            dma((devices,)),
            dma((devices,)),
        ],
        compiler_params=pltpu.CompilerParams(
            collective_id=0, has_side_effects=True, vmem_limit_bytes=60 * 1024 * 1024
        ),
        cost_estimate=pl.CostEstimate(
            flops=12_000_000_000, bytes_accessed=20_000_000, transcendentals=0
        ),
        name="whole",
    )(
        owners.T,
        entries.T,
        extra_forgetting_exponent.T,
        strength_weight.T,
        decay_weight.T,
        retrieval_gate_weight.T,
        output_norm_gain[None, :],
        head_decay_rate,
        tokens,
        store.reshape(rows, depth),
        *weights,
    )


def solution(mesh):
    rows = ("grp", "st")
    return jax.shard_map(
        functools.partial(per_device, mesh.shape["st"] // 2),
        mesh=mesh,
        in_specs=(
            P(rows, None),
            P(rows, None),
            P(rows, None),
            P(rows, None, None),
            P(None, "tp"),
            P(None, "tp"),
            P(None, "tp"),
            P(None, "tp"),
            P(None, "tp"),
            P("tp"),
            P(rows, "tp"),
            P(),
            P(None, "tp"),
            P(None, "tp"),
            P(None, "tp"),
            P(None, "tp"),
        ),
        out_specs=P(rows, "tp"),
        check_vma=False,
    )
```

```python
import functools

import jax
import jax.numpy as jnp
from jax import lax
from jax.experimental import pallas as pl
from jax.experimental.pallas import tpu as pltpu
from jax.sharding import PartitionSpec as P

BLOCK = 64
EPS = 1e-06
MISSING = -1e30
F32 = jnp.float32
BF16 = jnp.bfloat16
SPAN = 128


def dot_nn(left, right):
    return jnp.dot(left, right, preferred_element_type=F32)


def dot_nt(left, right):
    return lax.dot_general(left, right, (((1,), (1,)), ((), ())), preferred_element_type=F32)


def dot_tn(left, right):
    return lax.dot_general(left, right, (((0,), (0,)), ((), ())), preferred_element_type=F32)


def attend_jobs(jobs, me, sibling, kv_own, kv_sib, head_dim):
    passage_rows, half = kv_own.shape[1], kv_own.shape[2] // 2
    heads = half // head_dim
    scale = head_dim ** (-0.5)
    nothing = jnp.zeros((BLOCK, head_dim), BF16)

    def find(pairs, device):
        hit = jnp.int32(0)
        for owner, entry in pairs:
            hit = hit + (owner == device).astype(jnp.int32) * (entry + 1)
        found = jnp.minimum(hit, 1)
        return hit - found, (1 - found).astype(F32) * MISSING

    work = []
    for q_ref, named, o_ref, stat_ref in jobs:
        for block in range(q_ref.shape[0] // BLOCK):
            pairs = named(block)
            work.append((q_ref, o_ref, block, find(pairs, me), find(pairs, sibling)))
    scores = []
    for q_ref, _, block, (row_own, _), (row_sib, _) in work:
        query = q_ref[block * BLOCK : (block + 1) * BLOCK, :]
        spread = jnp.concatenate(
            [
                jnp.concatenate(
                    [
                        query[:, head * head_dim : (head + 1) * head_dim] if head == place else nothing
                        for place in range(heads)
                    ],
                    axis=1,
                )
                for head in range(heads)
            ],
            axis=0,
        )
        keys = jnp.concatenate([kv_own[row_own, :, :half], kv_sib[row_sib, :, :half]], axis=0)
        scores.append(dot_nt(keys, spread))
    weights, stats = [], []
    for (_, _, _, (_, bias_own), (_, bias_sib)), raw in zip(work, scores):
        own = raw[:passage_rows] * scale + bias_own
        sib = raw[passage_rows:] * scale + bias_sib
        peak = jnp.max(jnp.maximum(own, sib), axis=0, keepdims=True)
        e_own = jnp.exp(own - peak)
        e_sib = jnp.exp(sib - peak)
        total = jnp.sum(e_own + e_sib, axis=0, keepdims=True)
        inv = 1.0 / total
        weights.append(jnp.concatenate([e_own * inv, e_sib * inv], axis=0).astype(BF16))
        stats.append(peak + jnp.log(total))
    for (_, o_ref, block, (row_own, _), (row_sib, _)), weight in zip(work, weights):
        values = jnp.concatenate([kv_own[row_own, :, half:], kv_sib[row_sib, :, half:]], axis=0)
        result = dot_tn(weight, values)
        for head in range(heads):
            cols = slice(head * head_dim, (head + 1) * head_dim)
            o_ref[block * BLOCK : (block + 1) * BLOCK, cols] = result[
                head * BLOCK : (head + 1) * BLOCK, cols
            ].astype(BF16)
    done = 0
    for q_ref, _, _, stat_ref in jobs:
        blocks = q_ref.shape[0] // BLOCK
        rows = jnp.concatenate(stats[done : done + blocks], axis=0)
        done += blocks
        spare = stat_ref.shape[1] - rows.shape[1]
        if spare:
            rows = jnp.concatenate([rows, jnp.zeros((blocks, spare), F32)], axis=1)
        stat_ref[...] = rows


def shares_of(stats):
    peak = functools.reduce(jnp.maximum, stats)
    expo = [jnp.exp(stat - peak) for stat in stats]
    total = functools.reduce(jnp.add, expo)
    inv = 1.0 / total
    pad = (-peak.shape[0]) % 8
    rows = [e * inv for e in expo]
    if pad:
        rows = [jnp.concatenate([r, jnp.zeros((pad, r.shape[1]), F32)], axis=0) for r in rows]
    return [jnp.transpose(r) for r in rows], peak + jnp.log(total)


def blend(refs, shares, block, local, head_dim):
    at = slice(block * BLOCK, (block + 1) * BLOCK)
    cols = slice(local * head_dim, (local + 1) * head_dim)
    return functools.reduce(
        jnp.add,
        [
            ref[at, cols].astype(F32) * share[local * BLOCK : (local + 1) * BLOCK, block : block + 1]
            for ref, share in zip(refs, shares)
        ],
    )


def gate_rows(gates, extra_ref, rate_ref):
    heads, length = extra_ref.shape
    rows = jnp.transpose(gates)
    beta = jax.nn.sigmoid(rows[:heads])
    raw = rows[heads : 2 * heads]
    softplus = jnp.maximum(raw, 0.0) + jnp.log1p(jnp.exp(-jnp.abs(raw)))
    which = lax.broadcasted_iota(jnp.int32, (heads, length), 0)
    rate = jnp.zeros((heads, length), F32)
    for head in range(heads):
        rate = jnp.where(which == head, rate_ref[head], rate)
    decay = -rate * softplus + extra_ref[...]
    rgate = jax.nn.sigmoid(rows[2 * heads : 3 * heads])
    tri = jnp.where(
        lax.broadcasted_iota(jnp.int32, (SPAN, SPAN), 0)
        <= lax.broadcasted_iota(jnp.int32, (SPAN, SPAN), 1),
        1.0,
        0.0,
    ).astype(F32)
    pad = jnp.zeros((8 - heads, SPAN), F32)
    spans = []
    for span in range(length // SPAN):
        at = slice(span * SPAN, (span + 1) * SPAN)
        cum = jnp.dot(
            jnp.concatenate([decay[:, at], pad], axis=0),
            tri,
            precision=lax.Precision.HIGHEST,
            preferred_element_type=F32,
        )[:heads]
        ends = cum[:, SPAN - 1 : SPAN]
        grow = jnp.exp(cum)
        cols = jnp.transpose(jnp.concatenate([cum, beta[:, at], grow, rgate[:, at]], axis=0))
        spans.append((cum, beta[:, at], beta[:, at] * grow, jnp.exp(ends - cum), jnp.exp(ends), cols, rgate[:, at]))
    return spans


def delta_body(spans, read, gain, heads, store):
    head_dim = gain.shape[1]
    count = len(spans)
    half = SPAN // 2
    row = lax.broadcasted_iota(jnp.int32, (SPAN, SPAN), 0)
    col = lax.broadcasted_iota(jnp.int32, (SPAN, SPAN), 1)
    lower = row >= col
    strict = row > col
    prow = lax.broadcasted_iota(jnp.int32, (half, SPAN), 0)
    plane = lax.broadcasted_iota(jnp.int32, (half, SPAN), 1)
    pcol = plane % half
    is_left = plane < half
    left = jnp.where(is_left, 1.0, 0.0).astype(BF16)
    right = jnp.where(is_left, 0.0, 1.0).astype(BF16)
    eye = jnp.where(prow == pcol, 1.0, 0.0).astype(F32)
    sizes = []
    size = 2
    while size < half:
        sizes.append(size)
        size *= 2

    def cut_of(size):
        return ((prow // (2 * size)) == (pcol // (2 * size))) & ((prow // size) != (pcol // size))

    first = jnp.where(cut_of(1), 1.0, 0.0).astype(F32)
    cuts = []
    for size in sizes:
        cut = jnp.where(cut_of(size), 1.0, 0.0).astype(BF16)
        cuts.append((cut * left, cut * right))
    units = [(head, span) for head in range(heads) for span in range(count)]
    kb, kt, grams, mixes = {}, {}, {}, {}
    for unit in units:
        k32 = read("k", *unit).astype(F32)
        kn = k32 * lax.rsqrt(jnp.sum(k32 * k32, axis=1, keepdims=True) + EPS)
        kb[unit] = kn.astype(BF16)
        kt[unit] = jnp.transpose(kn)
    for unit in units:
        turned = kt[unit].astype(BF16)
        grams[unit] = dot_nn(kb[unit], turned)
        mixes[unit] = dot_nn(read("q", *unit), turned)
    within, packed, corner, inverse = {}, {}, {}, {}
    for unit in units:
        head, span = unit
        cum, _, _, _, _, cols, _ = spans[span]
        spread = cols[:, head : head + 1] - cum[head : head + 1, :]
        damp = jnp.where(lower, jnp.exp(jnp.minimum(spread, 0.0)), 0.0)
        within[unit] = (mixes[unit] * damp).astype(BF16)
        inner = jnp.where(strict, grams[unit] * damp * cols[:, heads + head : heads + head + 1], 0.0)
        pack = jnp.where(is_left, inner[:half], inner[half:])
        packed[unit] = pack.astype(BF16)
        corner[unit] = jnp.where(is_left, inner[half:], 0.0).astype(BF16)
        inverse[unit] = eye - pack * first
    for cut_left, cut_right in cuts:
        parts = {}
        for unit in units:
            piece = packed[unit]
            parts[unit] = dot_nn(
                inverse[unit].astype(BF16),
                jnp.concatenate([piece * cut_left, piece * cut_right], axis=0),
            )
        for unit in units:
            now = inverse[unit].astype(BF16)
            inverse[unit] = inverse[unit] - dot_nn(
                parts[unit].astype(BF16), jnp.concatenate([now * left, now * right], axis=0)
            )
    parts = {}
    for unit in units:
        now = inverse[unit].astype(BF16)
        parts[unit] = dot_nn(corner[unit], jnp.concatenate([now * left, now * right], axis=0))
    zeros = jnp.zeros((half, SPAN), BF16)
    full = {}
    for unit in units:
        now = inverse[unit]
        link = dot_nn(
            now.astype(BF16) * right, jnp.concatenate([zeros, parts[unit].astype(BF16)], axis=0)
        )
        full[unit] = jnp.concatenate(
            [jnp.where(is_left, now, 0.0), jnp.where(is_left, -link, now)], axis=0
        )
    base, key_mix, tails = {}, {}, {}
    for unit in units:
        head, span = unit
        _, beta, beta_grow, tail, _, _, _ = spans[span]
        base[unit] = dot_nn((full[unit] * beta[head : head + 1, :]).astype(BF16), read("v", *unit))
        key_mix[unit] = dot_nn(
            (full[unit] * beta_grow[head : head + 1, :]).astype(BF16), kb[unit]
        ).astype(BF16)
        tails[unit] = (kt[unit] * tail[head : head + 1, :]).astype(BF16)
    state = [jnp.zeros((head_dim, head_dim), F32) for _ in range(heads)]
    for span in range(count):
        reads = [
            dot_nn(
                jnp.concatenate([key_mix[head, span], read("q", head, span)], axis=0),
                state[head].astype(BF16),
            )
            for head in range(heads)
        ]
        fresh = [(base[head, span] - reads[head][:SPAN]).astype(BF16) for head in range(heads)]
        carry = spans[span][4]
        state = [
            state[head] * carry[head : head + 1, :] + dot_nn(tails[head, span], fresh[head])
            for head in range(heads)
        ]
        for head in range(heads):
            cols = spans[span][5]
            grow = cols[:, 2 * heads + head : 2 * heads + head + 1]
            result = reads[head][SPAN:] * grow + dot_nn(within[head, span], fresh[head])
            q32 = read("q", head, span).astype(F32)
            square = jnp.sum(q32 * q32, axis=1, keepdims=True)
            norm = lax.rsqrt(
                jnp.mean(result * result, axis=1, keepdims=True)
                + EPS * head_dim * (square + EPS)
            )
            store(head, span, result * norm * gain)


def whole_kernel(
    chips,
    head_dim,
    passage_rows,
    lesser,
    tokens_hbm,
    store_hbm,
    weights_hbm,
    o_ref,
    owners_ref,
    entries_ref,
    extra_ref,
    small_a,
    small_b,
    small_c,
    gain_ref,
    rate_ref,
    gate_ref,
    tok,
    sto,
    wts,
    rq,
    qkv,
    kv_own,
    kv_sib,
    kv_out,
    qbuf,
    obuf,
    sbuf,
    rbuf,
    rstat,
    fin,
    fstat,
    normed,
    gsel,
    want_mine,
    want_all,
    want_smem,
    load_sem,
    want_sem,
    kv_sem,
    send_q,
    recv_q,
    send_r,
    send_s,
    recv_r,
    recv_s,
    recv_f,
    recv_g,
    send_w,
    recv_w,
    send_h,
):
    devices = 2 * chips
    reach = chips // 2
    me = lax.axis_index("st")
    core, chip = lax.rem(me, 2), me // 2
    other = 1 - core
    sibling = chip * 2 + other
    length, width = normed.shape
    half = width // 2
    heads = width // head_dim
    here = heads // 2
    pieces = rq.shape[1]
    piece_rows = length // pieces
    piece_blocks = piece_rows // BLOCK
    per = owners_ref.shape[0]
    blocks = owners_ref.shape[1]

    def rcopy(src, dst, ssem, rsem, target):
        return pltpu.make_async_remote_copy(
            src_ref=src,
            dst_ref=dst,
            send_sem=ssem,
            recv_sem=rsem,
            device_id={"st": target},
            device_id_type=pl.DeviceIdType.MESH,
        )

    barrier = pltpu.get_barrier_semaphore()

    @pl.loop(1, devices)
    def _(off):
        pl.semaphore_signal(
            barrier,
            inc=1,
            device_id={"st": lax.rem(me + off, devices)},
            device_id_type=pl.DeviceIdType.MESH,
        )

    rq_w, pk_w, pv_w, q_w = 0, 1, 2, 3

    def token_rows(piece):
        at = pl.ds(piece * piece_rows, piece_rows)
        return pltpu.make_async_copy(tokens_hbm.at[at], tok.at[at], load_sem.at[8 + piece])

    def query_weight(which, index):
        at = pl.ds(pl.multiple_of(which * half, half), half)
        return pltpu.make_async_copy(
            weights_hbm[rq_w].at[:, at], wts.at[rq_w, :, at], load_sem.at[index]
        )

    loads = [None, None]
    loads += [
        pltpu.make_async_copy(weights_hbm[i], wts.at[i], load_sem.at[1 + i]) for i in range(1, 6)
    ]
    loads.append(pltpu.make_async_copy(store_hbm, sto, load_sem.at[7]))
    first_loads = [token_rows(0), query_weight(core, 0)]
    second_loads = [token_rows(piece) for piece in range(1, pieces)] + [query_weight(other, 1)]
    small_refs = (small_a, small_b, small_c)
    lesser_loads = [
        pltpu.make_async_copy(src, dst, load_sem.at[8 + pieces + i])
        for i, (src, dst) in enumerate(
            zip(lesser, (owners_ref, entries_ref, extra_ref) + small_refs + (gain_ref, rate_ref))
        )
    ]
    for copy in first_loads + lesser_loads[:2] + second_loads:
        copy.start()
    lesser_loads[0].wait()
    lesser_loads[1].wait()

    want_mine[...] = jnp.zeros_like(want_mine)
    want_mine[:per, :blocks] = owners_ref[...]
    want_mine[per : 2 * per, :blocks] = entries_ref[...]
    want_all[me] = want_mine[...]

    with jax.named_scope("wait_tok"):
        for copy in first_loads:
            copy.wait()
    loads[7].start()
    loads[1 + pk_w].start()

    def project_query(side, piece):
        at = pl.ds(piece * piece_rows, piece_rows)
        cols = pl.ds(pl.multiple_of(side * half, half), half)
        rq[side, piece] = dot_nn(tok[at, :], wts[rq_w, :, cols]).astype(BF16)

    def want_copy(off):
        return rcopy(
            want_mine,
            want_all.at[me],
            send_w.at[off - 1],
            recv_w.at[me],
            lax.rem(me + off, devices),
        )

    def own_query(there, side, piece, way):
        return rcopy(
            rq.at[side, piece],
            qbuf.at[me, piece],
            send_q.at[way, chip * 2 + side, piece],
            recv_q.at[me, piece],
            there * 2 + side,
        )

    def pass_query(source, piece, there, way):
        return rcopy(
            qbuf.at[source, piece],
            qbuf.at[source, piece],
            send_q.at[way, source, piece],
            recv_q.at[source, piece],
            there * 2 + core,
        )

    def await_query(source, piece):
        pass_query(source, piece, sibling // 2, 0).wait_recv()

    def result_to(source, piece, dst, dstat, rsem, gsem, target):
        return (
            rcopy(obuf.at[source, piece], dst, send_r.at[source, piece], rsem, target),
            rcopy(sbuf.at[source, piece], dstat, send_s.at[source, piece], gsem, target),
        )

    def pass_result(source, piece, there):
        return result_to(
            source,
            piece,
            rbuf.at[source, piece],
            rstat.at[source, piece],
            recv_r.at[source, piece],
            recv_s.at[source, piece],
            there * 2 + core,
        )

    def give_result(source, piece, side):
        return result_to(
            source,
            piece,
            fin.at[side, core, piece],
            fstat.at[side, core, piece],
            recv_f.at[side, core, piece],
            recv_g.at[side, core, piece],
            source,
        )

    def await_result(source, piece):
        for copy in pass_result(source, piece, sibling // 2):
            copy.wait_recv()

    def await_final(side, which, piece):
        copies = result_to(
            me,
            piece,
            fin.at[side, which, piece],
            fstat.at[side, which, piece],
            recv_f.at[side, which, piece],
            recv_g.at[side, which, piece],
            sibling,
        )
        for copy in copies:
            copy.wait_recv()

    def begin(copies):
        for copy in copies if isinstance(copies, tuple) else (copies,):
            copy.start()

    def job(source, piece, own=False):
        def named(block):
            at = piece * piece_blocks + block
            return [
                (want_smem[source, place, at], want_smem[source, per + place, at])
                for place in range(per)
            ]

        if own:
            return (
                rq.at[core, piece], named, fin.at[2, core, piece], fstat.at[2, core, piece]
            )
        return (qbuf.at[source, piece], named, obuf.at[source, piece], sbuf.at[source, piece])

    def attend(*jobs):
        attend_jobs(jobs, me, sibling, kv_own, kv_sib, head_dim)

    def attend_here():
        @pl.loop(0, pieces)
        def _(piece):
            await_query(sibling, piece)
            attend(job(me, piece, own=True), job(sibling, piece))
            begin(give_result(sibling, piece, 2))

    def merge(source, piece):
        await_result(source, piece)
        refs = [obuf.at[source, piece], rbuf.at[source, piece]]
        shares, stat = shares_of([sbuf[source, piece], rstat[source, piece]])
        for block in range(piece_blocks):
            for local in range(here):
                value = blend(refs, shares, block, local, head_dim)
                obuf[
                    source,
                    piece,
                    block * BLOCK : (block + 1) * BLOCK,
                    local * head_dim : (local + 1) * head_dim,
                ] = value.astype(BF16)
        sbuf[source, piece] = stat

    inner = jnp.logical_and(chip > 0, chip < chips - 1)
    end = jnp.logical_or(chip == 0, chip == chips - 1)
    near = 2 * (chip // reach) - 1
    far = -near
    near_side, far_side = (1 - near) // 2, (1 - far) // 2

    def own_first(piece):
        @pl.when(inner)
        def _():
            own_query(chip + near, core, piece, 0).start()
            own_query(chip + far, core, piece, 1).start()

        @pl.when(end)
        def _():
            own_query(chip + far, core, piece, 1).start()

    with jax.named_scope("rq0"):
        project_query(core, 0)
    with jax.named_scope("barrier_wait"):
        pl.semaphore_wait(barrier, devices - 1)
    with jax.named_scope("rq1"):

        @pl.loop(1, devices)
        def _(off):
            want_copy(off).start()

        own_first(0)
        for copy in second_loads:
            copy.wait()
        for copy in lesser_loads[2:]:
            copy.start()
        loads[1 + pv_w].start()
        for piece in range(1, pieces):
            project_query(core, piece)
            own_first(piece)
        for piece in range(pieces):
            project_query(other, piece)

    @pl.when(end)
    def _():
        for piece in range(pieces):
            own_query(chip + far, other, piece, 1).start()

    def sib_copy(piece):
        return rcopy(
            rq.at[other, piece], qbuf.at[me, piece], send_h.at[piece], recv_q.at[me, piece], sibling
        )

    rows = sto.shape[0]
    tile = min(512, rows)

    def project_store(which, weight, dst, place, m):
        cols = pl.ds(pl.multiple_of(which * half, half), half)
        at = pl.ds(pl.multiple_of(m * tile, tile), tile)
        held = dot_nn(sto[at, :], wts[weight, :, cols]).astype(BF16)
        count = tile // passage_rows
        dst[pl.ds(m * count, count), :, place * half : (place + 1) * half] = held.reshape(
            count, passage_rows, half
        )

    def relay_first(piece):
        edge, peer = chip + near, chip + far

        @pl.when(inner)
        def _():
            await_query(edge * 2 + core, piece)
            pass_query(edge * 2 + core, piece, peer, 1).start()
            await_query(peer * 2 + core, piece)
            pass_query(peer * 2 + core, piece, edge, 0).start()

    tiles = rows // tile
    with jax.named_scope("kv"):
        loads[7].wait()
        loads[1 + pk_w].wait()
        for i in range(3):
            loads[1 + q_w + i].start()

        @pl.loop(0, tiles)
        def _(m):
            project_store(other, pk_w, kv_out, 0, m)

        loads[1 + pv_w].wait()

        @pl.loop(0, tiles)
        def _(m):
            project_store(other, pv_w, kv_out, 1, m)

        swap = rcopy(kv_out, kv_sib, kv_sem.at[0], kv_sem.at[1], sibling)
        swap.start()
        for piece in range(pieces):
            sib_copy(piece).start()

        @pl.loop(0, tiles)
        def _(m):
            project_store(core, pk_w, kv_own, 0, m)

    with jax.named_scope("relay0"):
        relay_first(0)
    with jax.named_scope("kv2"):

        @pl.loop(0, tiles)
        def _(m):
            project_store(core, pv_w, kv_own, 1, m)

    with jax.named_scope("relay1"):
        for piece in range(1, pieces):
            relay_first(piece)

    def project_mixer(step):
        i, side = step // 2, lax.rem(step, 2)
        cols = pl.ds(pl.multiple_of(side * half, half), half)
        qkv[i, :, cols] = dot_nn(tok[...], wts[q_w + i, :, cols]).astype(BF16)

    def project_gates():
        small = jnp.concatenate(
            [ref[...] for ref in small_refs]
            + [jnp.zeros((16 - 3 * heads, tok.shape[1]), BF16)],
            axis=0,
        )
        gate_ref[...] = dot_nt(tok[...], small)

    with jax.named_scope("wants"):

        @pl.loop(1, devices)
        def _(off):
            source = lax.rem(me + off, devices)
            rcopy(want_mine, want_all.at[source], send_w.at[0], recv_w.at[source], source).wait_recv()

        fetch = pltpu.make_async_copy(want_all, want_smem, want_sem)
        fetch.start()
        fetch.wait()
        swap.wait()
        for i in range(3):
            loads[1 + q_w + i].wait()
        for copy in lesser_loads[2:]:
            copy.wait()

    @pl.when(inner)
    def _():
        edge, peer, beyond = chip + near, chip + far, chip + 2 * far

        def at(where, which):
            return where * 2 + which

        with jax.named_scope("in01"):

            @pl.loop(0, pieces)
            def _(piece):
                attend(job(at(edge, core), piece), job(at(peer, core), piece))

        with jax.named_scope("in_here"):
            attend_here()
        with jax.named_scope("in23"):

            @pl.loop(0, pieces)
            def _(piece):
                await_query(at(edge, other), piece)
                pass_query(at(edge, other), piece, peer, 1).start()
                await_query(at(beyond, core), piece)
                pass_query(at(beyond, core), piece, edge, 0).start()
                attend(job(at(edge, other), piece), job(at(beyond, core), piece))

                @pl.loop(2 * piece, 2 * piece + 2)
                def _(step):
                    project_mixer(step)


        for piece in range(pieces):
            own_query(peer, other, piece, 1).start()
        with jax.named_scope("in45"):

            @pl.loop(0, pieces)
            def _(piece):
                await_query(at(beyond, other), piece)
                pass_query(at(beyond, other), piece, edge, 0).start()
                attend(job(at(beyond, other), piece))
                project_mixer(2 * pieces + piece)

        project_gates()
        with jax.named_scope("in67"):

            @pl.loop(0, pieces)
            def _(piece):
                await_query(at(peer, other), piece)
                pass_query(at(peer, other), piece, edge, 0).start()
                merge(at(beyond, core), piece)
                begin(pass_result(at(beyond, core), piece, peer))
                attend(job(at(peer, other), piece))

        for piece in range(pieces):
            own_query(edge, other, piece, 0).start()
        with jax.named_scope("in89"):

            @pl.loop(0, pieces)
            def _(piece):
                merge(at(beyond, other), piece)
                begin(pass_result(at(beyond, other), piece, peer))
                merge(at(edge, core), piece)
                begin(give_result(at(edge, core), piece, near_side))

        with jax.named_scope("in1011"):

            @pl.loop(0, pieces)
            def _(piece):
                merge(at(peer, core), piece)
                begin(give_result(at(peer, core), piece, far_side))
                merge(at(edge, other), piece)
                begin(give_result(at(edge, other), piece, near_side))

        with jax.named_scope("in12"):

            @pl.loop(0, pieces)
            def _(piece):
                merge(at(peer, other), piece)
                begin(give_result(at(peer, other), piece, far_side))

    @pl.when(end)
    def _():
        def at(distance, which):
            return (chip + far * distance) * 2 + which

        def handle(distance, which, send, fill=None):
            @pl.loop(0, pieces)
            def _(piece):
                await_query(at(distance, which), piece)
                attend(job(at(distance, which), piece))
                if send:
                    if distance == 1:
                        begin(give_result(at(distance, which), piece, far_side))
                    else:
                        begin(pass_result(at(distance, which), piece, chip + far))
                if fill is not None:
                    fill(piece)

        def fill_two(piece):
            @pl.loop(2 * piece, 2 * piece + 2)
            def _(step):
                project_mixer(step)

        def fill_one(piece):
            project_mixer(2 * pieces + piece)

        with jax.named_scope("end01"):
            handle(1, core, False)
        with jax.named_scope("end_here"):
            attend_here()
        with jax.named_scope("end23"):
            handle(2, core, True, fill_two)
        with jax.named_scope("end45"):
            handle(3, core, True, fill_one)
        project_gates()
        with jax.named_scope("end67"):
            handle(3, other, True)
        with jax.named_scope("end89"):
            handle(2, other, True)
        for piece in range(pieces):
            begin(give_result(at(1, core), piece, far_side))
        with jax.named_scope("end1011"):
            handle(1, other, True)

    with jax.named_scope("gates"):
        spans = gate_rows(gate_ref[...], extra_ref, rate_ref)
        for span, held in enumerate(spans):
            for side in range(2):
                rgate = held[6][side * here : (side + 1) * here]
                gsel[side, span * SPAN : (span + 1) * SPAN, :8] = jnp.transpose(
                    jnp.concatenate([rgate, jnp.zeros((8 - here, SPAN), F32)], axis=0)
                )

    def read(name, head, span):
        return qkv[
            "qkv".index(name),
            span * SPAN : (span + 1) * SPAN,
            head * head_dim : (head + 1) * head_dim,
        ]

    def keep(head, span, value):
        normed[span * SPAN : (span + 1) * SPAN, head * head_dim : (head + 1) * head_dim] = value

    with jax.named_scope("delta"):
        delta_body(spans, read, gain_ref[...], heads, keep)

    def finish(which, piece, sides):
        @pl.when(which == other)
        def _():
            await_final(2, which, piece)

        for side in sides[:-1]:
            await_final(side, which, piece)
        refs = [fin.at[side, which, piece] for side in sides]
        shares, _ = shares_of([fstat[side, which, piece] for side in sides])
        for block in range(piece_blocks):
            at = pl.ds(pl.multiple_of(piece * piece_rows + block * BLOCK, BLOCK), BLOCK)
            for local in range(here):
                cols = pl.ds(
                    pl.multiple_of(which * half + local * head_dim, head_dim), head_dim
                )
                value = blend(refs, shares, block, local, head_dim)
                rgate = gsel[which, at, local : local + 1]
                o_ref[at, cols] = (normed[at, cols] + rgate * value).astype(BF16)

    def finish_all(sides):
        @pl.loop(0, 2 * pieces)
        def _(step):
            finish(lax.rem(core + step // pieces, 2), lax.rem(step, pieces), sides)

    with jax.named_scope("finish"):

        @pl.when(inner)
        def _():
            finish_all((0, 1, 2))

        @pl.when(end)
        def _():
            finish_all((1 - far_side, 2))

    @pl.loop(1, devices)
    def _(off):
        want_copy(off).wait_send()

    @pl.loop(0, pieces)
    def _(piece):
        sib_copy(piece).wait_send()
        for copy in give_result(sibling, piece, 2):
            copy.wait_send()

    @pl.loop(0, 2 * pieces)
    def _(step):
        piece, which = lax.rem(step, pieces), step // pieces

        @pl.when(inner)
        def _():
            edge, peer, beyond = chip + near, chip + far, chip + 2 * far
            own_query(edge, which, piece, 0).wait_send()
            own_query(peer, which, piece, 1).wait_send()
            pass_query(edge * 2 + which, piece, peer, 1).wait_send()
            pass_query(peer * 2 + which, piece, edge, 0).wait_send()
            pass_query(beyond * 2 + which, piece, edge, 0).wait_send()
            for where in (edge, peer, beyond):
                for copy in give_result(where * 2 + which, piece, 0):
                    copy.wait_send()

        @pl.when(end)
        def _():
            own_query(chip + far, which, piece, 1).wait_send()
            for distance in range(1, chips):
                for copy in give_result((chip + far * distance) * 2 + which, piece, 0):
                    copy.wait_send()


def line_device(
    chips,
    tokens,
    owners,
    entries,
    store,
    mixer_query_weight,
    mixer_key_weight,
    mixer_value_weight,
    strength_weight,
    decay_weight,
    head_decay_rate,
    extra_forgetting_exponent,
    output_norm_gain,
    retrieval_query_weight,
    passage_key_weight,
    passage_value_weight,
    retrieval_gate_weight,
):
    heads = head_decay_rate.shape[0]
    head_dim = output_norm_gain.shape[0]
    length, depth = tokens.shape
    passage_rows = store.shape[1]
    rows = store.shape[0] * passage_rows
    width = heads * head_dim
    half = width // 2
    devices = 2 * chips
    blocks = owners.shape[0]
    pieces = 2
    piece_rows, piece_blocks = length // pieces, blocks // pieces
    lanes = 2 * BLOCK
    vmem = pl.BlockSpec(memory_space=pltpu.VMEM)
    anywhere = pl.BlockSpec(memory_space=pl.ANY)
    weights = [
        retrieval_query_weight,
        passage_key_weight,
        passage_value_weight,
        mixer_query_weight,
        mixer_key_weight,
        mixer_value_weight,
    ]

    def body(*refs):
        whole_kernel(
            chips, head_dim, passage_rows, refs[:8], refs[8], refs[9], refs[10:16], *refs[16:]
        )

    dma = pltpu.SemaphoreType.DMA
    return pl.pallas_call(
        body,
        out_shape=jax.ShapeDtypeStruct((length, width), BF16),
        in_specs=[anywhere] * 16,
        out_specs=vmem,
        scratch_shapes=[
            pltpu.VMEM(owners.shape[::-1], jnp.int32),
            pltpu.VMEM(owners.shape[::-1], jnp.int32),
            pltpu.VMEM((heads, length), F32),
            pltpu.VMEM((heads, depth), BF16),
            pltpu.VMEM((heads, depth), BF16),
            pltpu.VMEM((heads, depth), BF16),
            pltpu.VMEM((1, head_dim), F32),
            pltpu.SMEM((heads,), F32),
            pltpu.VMEM((length, 16), F32),
            pltpu.VMEM((length, depth), BF16),
            pltpu.VMEM((rows, depth), BF16),
            pltpu.VMEM((6, depth, width), BF16),
            pltpu.VMEM((2, pieces, piece_rows, half), BF16),
            pltpu.VMEM((3, length, width), BF16),
            pltpu.VMEM((store.shape[0], passage_rows, width), BF16),
            pltpu.VMEM((store.shape[0], passage_rows, width), BF16),
            pltpu.VMEM((store.shape[0], passage_rows, width), BF16),
            pltpu.VMEM((devices, pieces, piece_rows, half), BF16),
            pltpu.VMEM((devices, pieces, piece_rows, half), BF16),
            pltpu.VMEM((devices, pieces, piece_blocks, lanes), F32),
            pltpu.VMEM((devices, pieces, piece_rows, half), BF16),
            pltpu.VMEM((devices, pieces, piece_blocks, lanes), F32),
            pltpu.VMEM((3, 2, pieces, piece_rows, half), BF16),
            pltpu.VMEM((3, 2, pieces, piece_blocks, lanes), F32),
            pltpu.VMEM((length, width), F32),
            pltpu.VMEM((2, length, 128), F32),
            pltpu.VMEM((8, 128), jnp.int32),
            pltpu.VMEM((devices, 8, 128), jnp.int32),
            pltpu.SMEM((devices, 8, 128), jnp.int32),
            dma((8 + pieces + 8,)),
            dma,
            dma((2,)),
            dma((2, devices, pieces)),
            dma((devices, pieces)),
            dma((devices, pieces)),
            dma((devices, pieces)),
            dma((devices, pieces)),
            dma((devices, pieces)),
            dma((3, 2, pieces)),
            dma((3, 2, pieces)),
            dma((devices,)),
            dma((devices,)),
            dma((pieces,)),
        ],
        compiler_params=pltpu.CompilerParams(
            collective_id=0, has_side_effects=True, vmem_limit_bytes=60 * 1024 * 1024
        ),
        cost_estimate=pl.CostEstimate(
            flops=12_000_000_000, bytes_accessed=20_000_000, transcendentals=0
        ),
        name="whole",
    )(
        owners.T,
        entries.T,
        extra_forgetting_exponent.T,
        strength_weight.T,
        decay_weight.T,
        retrieval_gate_weight.T,
        output_norm_gain[None, :],
        head_decay_rate,
        tokens,
        store.reshape(rows, depth),
        *weights,
    )


def ring_attend(q_ref, named, me, sibling, kv_own, kv_sib, o_ref, stat_ref, passage_rows, head_dim):
    length, half = q_ref.shape
    heads = half // head_dim
    blocks = length // BLOCK
    scale = head_dim ** (-0.5)
    nothing = jnp.zeros((BLOCK, head_dim), BF16)

    def find(pairs, device):
        hit = jnp.int32(0)
        for owner, entry in pairs:
            hit = hit + (owner == device).astype(jnp.int32) * (entry + 1)
        found = jnp.minimum(hit, 1)
        return hit - found, (1 - found).astype(F32) * MISSING

    places, scores = [], []
    for block in range(blocks):
        pairs = named(block)
        row_own, bias_own = find(pairs, me)
        row_sib, bias_sib = find(pairs, sibling)
        places.append((row_own, bias_own, row_sib, bias_sib))
        query = q_ref[block * BLOCK : (block + 1) * BLOCK, :]
        spread = jnp.concatenate(
            [
                jnp.concatenate(
                    [
                        query[:, head * head_dim : (head + 1) * head_dim] if head == place else nothing
                        for place in range(heads)
                    ],
                    axis=1,
                )
                for head in range(heads)
            ],
            axis=0,
        )
        keys = jnp.concatenate(
            [
                kv_own[row_own, :, :half],
                kv_sib[row_sib, :, :half],
            ],
            axis=0,
        )
        scores.append(dot_nt(keys, spread))
    weights, stats = [], []
    for block in range(blocks):
        _, bias_own, _, bias_sib = places[block]
        raw = scores[block]
        own = raw[:passage_rows] * scale + bias_own
        sib = raw[passage_rows:] * scale + bias_sib
        peak = jnp.max(jnp.maximum(own, sib), axis=0, keepdims=True)
        e_own = jnp.exp(own - peak)
        e_sib = jnp.exp(sib - peak)
        total = jnp.sum(e_own + e_sib, axis=0, keepdims=True)
        inv = 1.0 / total
        weights.append(jnp.concatenate([e_own * inv, e_sib * inv], axis=0).astype(BF16))
        stats.append(peak + jnp.log(total))
    for block in range(blocks):
        row_own, _, row_sib, _ = places[block]
        values = jnp.concatenate(
            [
                kv_own[row_own, :, half:],
                kv_sib[row_sib, :, half:],
            ],
            axis=0,
        )
        result = dot_tn(weights[block], values)
        for head in range(heads):
            cols = slice(head * head_dim, (head + 1) * head_dim)
            o_ref[block * BLOCK : (block + 1) * BLOCK, cols] = result[
                head * BLOCK : (head + 1) * BLOCK, cols
            ].astype(BF16)
    rows = jnp.concatenate(stats, axis=0)
    spare = stat_ref.shape[1] - rows.shape[1]
    if spare:
        rows = jnp.concatenate([rows, jnp.zeros((blocks, spare), F32)], axis=1)
    stat_ref[...] = rows


def ring_kernel(
    chips,
    head_dim,
    passage_rows,
    owners_ref,
    entries_ref,
    extra_ref,
    small_refs,
    gain_ref,
    rate_ref,
    tokens_hbm,
    store_hbm,
    weights_hbm,
    o_ref,
    tok,
    sto,
    wts,
    rq,
    qkv,
    kv_own,
    kv_sib,
    kv_out,
    qbuf,
    obuf,
    sbuf,
    part,
    pstat,
    normed,
    want_mine,
    want_all,
    want_smem,
    load_sem,
    want_sem,
    kv_sem,
    send_q,
    recv_q,
    send_r,
    recv_r,
    send_s,
    recv_s,
    send_w,
    recv_w,
):
    devices = 2 * chips
    reach = chips // 2
    me = lax.axis_index("st")
    core, chip = lax.rem(me, 2), me // 2
    other = 1 - core
    sibling = chip * 2 + other
    length, width = normed.shape
    half = width // 2
    heads = width // head_dim

    def device(dz, which):
        return lax.rem(chip + dz, chips) * 2 + which

    def rcopy(src, dst, ssem, rsem, target):
        return pltpu.make_async_remote_copy(
            src_ref=src,
            dst_ref=dst,
            send_sem=ssem,
            recv_sem=rsem,
            device_id={"st": target},
            device_id_type=pl.DeviceIdType.MESH,
        )

    barrier = pltpu.get_barrier_semaphore()

    @pl.loop(1, devices)
    def _(off):
        pl.semaphore_signal(
            barrier,
            inc=1,
            device_id={"st": lax.rem(me + off, devices)},
            device_id_type=pl.DeviceIdType.MESH,
        )

    rq_w, pk_w, pv_w, q_w = 0, 1, 2, 3
    loads = [pltpu.make_async_copy(tokens_hbm, tok, load_sem.at[0])]
    loads += [
        pltpu.make_async_copy(weights_hbm[i], wts.at[i], load_sem.at[1 + i]) for i in range(6)
    ]
    loads.append(pltpu.make_async_copy(store_hbm, sto, load_sem.at[7]))
    loads[0].start()
    loads[1].start()

    want_mine[...] = jnp.zeros_like(want_mine)
    per = owners_ref.shape[0]
    blocks = owners_ref.shape[1]
    want_mine[:per, :blocks] = owners_ref[...]
    want_mine[per : 2 * per, :blocks] = entries_ref[...]
    want_all[me] = want_mine[...]

    loads[0].wait()
    loads[1].wait()
    loads[7].start()
    loads[1 + pk_w].start()
    loads[1 + pv_w].start()

    @pl.loop(0, 2)
    def _(side):
        cols = pl.ds(pl.multiple_of(side * half, half), half)
        rq[side] = dot_nn(tok[...], wts[rq_w, :, cols]).astype(BF16)

    pl.semaphore_wait(barrier, devices - 1)

    def slot(dz, which):
        return (dz % chips) * 2 + which

    hop1 = []
    for count, (dz, which) in enumerate(
        [(1, core), (chips - 1, other), (1, other), (chips - 1, core)]
    ):
        there = slot(chips - dz, core)
        hop1.append(
            rcopy(
                rq.at[which], qbuf.at[there], send_q.at[count], recv_q.at[there], device(dz, which)
            )
        )
    hop1.append(
        rcopy(rq.at[other], qbuf.at[core], send_q.at[4], recv_q.at[core], sibling)
    )
    for copy in hop1:
        copy.start()

    def want_copy(off):
        return rcopy(
            want_mine,
            want_all.at[me],
            send_w.at[off - 1],
            recv_w.at[me],
            lax.rem(me + off, devices),
        )

    @pl.loop(1, devices)
    def _(off):
        want_copy(off).start()

    qbuf[core] = rq[core]

    loads[7].wait()
    loads[1 + pk_w].wait()
    for i in range(3):
        loads[1 + q_w + i].start()

    rows = sto.shape[0]
    tile = min(512, rows)

    def project_store(which, weight, dst, place):
        cols = pl.ds(pl.multiple_of(which * half, half), half)

        @pl.loop(0, rows // tile)
        def _(m):
            at = pl.ds(pl.multiple_of(m * tile, tile), tile)
            held = dot_nn(sto[at, :], wts[weight, :, cols]).astype(BF16)
            count = tile // passage_rows
            dst[pl.ds(m * count, count), :, place * half : (place + 1) * half] = held.reshape(
                count, passage_rows, half
            )

    project_store(other, pk_w, kv_out, 0)
    loads[1 + pv_w].wait()
    project_store(other, pv_w, kv_out, 1)
    project_store(core, pk_w, kv_own, 0)
    swap = rcopy(kv_out, kv_sib, kv_sem.at[0], kv_sem.at[1], sibling)
    swap.start()
    project_store(core, pv_w, kv_own, 1)

    for i in range(3):
        loads[1 + q_w + i].wait()

    @pl.loop(0, 6)
    def _(step):
        i, side = step // 2, lax.rem(step, 2)
        cols = pl.ds(pl.multiple_of(side * half, half), half)
        qkv[i, :, cols] = dot_nn(tok[...], wts[q_w + i, :, cols]).astype(BF16)

    small = jnp.concatenate(
        [ref[...] for ref in small_refs] + [jnp.zeros((16 - 3 * heads, tok.shape[1]), BF16)], axis=0
    )
    gates = dot_nt(tok[...], small)
    spans = gate_rows(gates, extra_ref, rate_ref)

    @pl.loop(1, devices)
    def _(off):
        source = lax.rem(me + off, devices)
        rcopy(want_mine, want_all.at[source], send_w.at[0], recv_w.at[source], source).wait_recv()

    fetch = pltpu.make_async_copy(want_all, want_smem, want_sem)
    fetch.start()
    fetch.wait()
    swap.wait()

    def await_query(at):
        rcopy(rq.at[0], qbuf.at[at], send_q.at[0], recv_q.at[at], sibling).wait_recv()

    def attend(dz, which):
        at = slot(dz, which)
        source = device(dz, which)

        def named(block):
            return [
                (want_smem[source, place, block], want_smem[source, per + place, block])
                for place in range(per)
            ]

        ring_attend(
            qbuf.at[at],
            named,
            me,
            sibling,
            kv_own,
            kv_sib,
            obuf.at[at],
            sbuf.at[at],
            passage_rows,
            head_dim,
        )

    def reply(dz, which):
        at = slot(dz, which)
        back = (chips - dz) % chips
        target = device(dz, which)
        return (
            rcopy(
                obuf.at[at], part.at[back, core], send_r.at[at], recv_r.at[back, core], target
            ),
            rcopy(
                sbuf.at[at], pstat.at[back, core], send_s.at[at], recv_s.at[back, core], target
            ),
        )

    relays = []

    def relay(src, dst, count, target):
        copy = rcopy(qbuf.at[src], qbuf.at[dst], send_q.at[count], recv_q.at[dst], target)
        copy.start()
        relays.append(copy)

    count = 5
    await_query(other)

    @pl.loop(0, 2)
    def _(which):
        attend(0, which)

    part[0, core] = obuf[core]
    pstat[0, core] = sbuf[core]
    for copy in reply(0, other):
        copy.start()

    for hop in range(1, reach):
        back = chips - hop
        if hop < reach - 1:
            for which in range(2):
                await_query(slot(back, which))
                relay(slot(back, which), slot(back - 1, which), count, device(1, core))
                await_query(slot(hop, which))
                relay(slot(hop, which), slot(hop + 1, which), count + 1, device(chips - 1, core))
                count += 2
        else:
            await_query(slot(back, core))
            relay(slot(back, core), slot(reach, core), count, device(1, core))
            await_query(slot(hop, other))
            relay(slot(hop, other), slot(reach, other), count + 1, device(chips - 1, core))
            count += 2
            await_query(slot(back, other))
            await_query(slot(hop, core))
        for dz in (back, hop):

            @pl.loop(0, 2)
            def _(which):
                attend(dz, which)
                for copy in reply(dz, which):
                    copy.start()

    await_query(slot(reach, 0))
    await_query(slot(reach, 1))

    @pl.loop(0, 2)
    def _(which):
        attend(reach, which)
        for copy in reply(reach, which):
            copy.start()

    def read(name, head, span):
        return qkv[
            "qkv".index(name),
            span * SPAN : (span + 1) * SPAN,
            head * head_dim : (head + 1) * head_dim,
        ]

    def keep(head, span, value):
        normed[span * SPAN : (span + 1) * SPAN, head * head_dim : (head + 1) * head_dim] = value

    delta_body(spans, read, gain_ref[...], heads, keep)

    def await_part(back, side):
        rcopy(
            obuf.at[0], part.at[back, side], send_r.at[0], recv_r.at[back, side], sibling
        ).wait_recv()
        rcopy(
            sbuf.at[0], pstat.at[back, side], send_s.at[0], recv_s.at[back, side], sibling
        ).wait_recv()

    await_part(0, other)
    for back in range(1, chips):
        for side in range(2):
            await_part(back, side)

    here = heads // 2
    for side in range(2):
        stats = [pstat[back, side] for back in range(chips)]
        peak = functools.reduce(jnp.maximum, stats)
        expo = [jnp.exp(stat - peak) for stat in stats]
        inv = 1.0 / functools.reduce(jnp.add, expo)
        shares = [jnp.transpose(e * inv) for e in expo]
        for block in range(blocks):
            at = slice(block * BLOCK, (block + 1) * BLOCK)
            span, inside = divmod(block * BLOCK, SPAN)
            for local in range(here):
                cols = slice(local * head_dim, (local + 1) * head_dim)
                head = side * here + local
                where = slice(head * head_dim, (head + 1) * head_dim)
                value = functools.reduce(
                    jnp.add,
                    [
                        part[back, side, at, cols].astype(F32)
                        * shares[back][local * BLOCK : (local + 1) * BLOCK, block : block + 1]
                        for back in range(chips)
                    ],
                )
                rgate = spans[span][5][
                    inside : inside + BLOCK, 3 * heads + head : 3 * heads + head + 1
                ]
                o_ref[at, where] = (normed[at, where] + rgate * value).astype(BF16)

    for copy in hop1 + relays:
        copy.wait_send()

    @pl.loop(1, devices)
    def _(off):
        want_copy(off).wait_send()

    for copy in reply(0, other):
        copy.wait_send()
    for dz in range(1, chips):
        for which in range(2):
            for copy in reply(dz, which):
                copy.wait_send()


def ring_device(
    chips,
    tokens,
    owners,
    entries,
    store,
    mixer_query_weight,
    mixer_key_weight,
    mixer_value_weight,
    strength_weight,
    decay_weight,
    head_decay_rate,
    extra_forgetting_exponent,
    output_norm_gain,
    retrieval_query_weight,
    passage_key_weight,
    passage_value_weight,
    retrieval_gate_weight,
):
    heads = head_decay_rate.shape[0]
    head_dim = output_norm_gain.shape[0]
    length, depth = tokens.shape
    passage_rows = store.shape[1]
    rows = store.shape[0] * passage_rows
    width = heads * head_dim
    half = width // 2
    devices = 2 * chips
    blocks = owners.shape[0]
    vmem = pl.BlockSpec(memory_space=pltpu.VMEM)
    anywhere = pl.BlockSpec(memory_space=pl.ANY)
    weights = [
        retrieval_query_weight,
        passage_key_weight,
        passage_value_weight,
        mixer_query_weight,
        mixer_key_weight,
        mixer_value_weight,
    ]

    def body(owners_ref, entries_ref, extra_ref, s1, s2, s3, gain_ref, rate_ref, tok, sto, *rest):
        ring_kernel(
            chips, head_dim, passage_rows, owners_ref, entries_ref, extra_ref, (s1, s2, s3),
            gain_ref, rate_ref, tok, sto, rest[:6], *rest[6:],
        )

    dma = pltpu.SemaphoreType.DMA
    return pl.pallas_call(
        body,
        out_shape=jax.ShapeDtypeStruct((length, width), BF16),
        in_specs=[vmem] * 7 + [pl.BlockSpec(memory_space=pltpu.SMEM)] + [anywhere] * 8,
        out_specs=vmem,
        scratch_shapes=[
            pltpu.VMEM((length, depth), BF16),
            pltpu.VMEM((rows, depth), BF16),
            pltpu.VMEM((6, depth, width), BF16),
            pltpu.VMEM((2, length, half), BF16),
            pltpu.VMEM((3, length, width), BF16),
            pltpu.VMEM((store.shape[0], passage_rows, width), BF16),
            pltpu.VMEM((store.shape[0], passage_rows, width), BF16),
            pltpu.VMEM((store.shape[0], passage_rows, width), BF16),
            pltpu.VMEM((devices, length, half), BF16),
            pltpu.VMEM((devices, length, half), BF16),
            pltpu.VMEM((devices, blocks, 2 * BLOCK), F32),
            pltpu.VMEM((chips, 2, length, half), BF16),
            pltpu.VMEM((chips, 2, blocks, 2 * BLOCK), F32),
            pltpu.VMEM((length, width), F32),
            pltpu.VMEM((8, 128), jnp.int32),
            pltpu.VMEM((devices, 8, 128), jnp.int32),
            pltpu.SMEM((devices, 8, 128), jnp.int32),
            dma((8,)),
            dma,
            dma((2,)),
            dma((5 + 2 * devices,)),
            dma((devices,)),
            dma((devices,)),
            dma((chips, 2)),
            dma((devices,)),
            dma((chips, 2)),
            dma((devices,)),
            dma((devices,)),
        ],
        compiler_params=pltpu.CompilerParams(
            collective_id=0, has_side_effects=True, vmem_limit_bytes=60 * 1024 * 1024
        ),
        cost_estimate=pl.CostEstimate(
            flops=12_000_000_000, bytes_accessed=20_000_000, transcendentals=0
        ),
        name="ring",
    )(
        owners.T,
        entries.T,
        extra_forgetting_exponent.T,
        strength_weight.T,
        decay_weight.T,
        retrieval_gate_weight.T,
        output_norm_gain[None, :],
        head_decay_rate,
        tokens,
        store.reshape(rows, depth),
        *weights,
    )


def solution(mesh):
    rows = ("grp", "st")
    chips = mesh.shape["st"] // 2
    return jax.shard_map(
        functools.partial(line_device if chips // 2 == 2 else ring_device, chips),
        mesh=mesh,
        in_specs=(
            P(rows, None),
            P(rows, None),
            P(rows, None),
            P(rows, None, None),
            P(None, "tp"),
            P(None, "tp"),
            P(None, "tp"),
            P(None, "tp"),
            P(None, "tp"),
            P("tp"),
            P(rows, "tp"),
            P(),
            P(None, "tp"),
            P(None, "tp"),
            P(None, "tp"),
            P(None, "tp"),
        ),
        out_specs=P(rows, "tp"),
        check_vma=False,
    )
```

```python
import functools

import jax
import jax.numpy as jnp
from jax import lax
from jax.experimental import pallas as pl
from jax.experimental.pallas import tpu as pltpu
from jax.sharding import PartitionSpec as P

BLOCK = 64
EPS = 1e-06
MISSING = -1e30
F32 = jnp.float32
BF16 = jnp.bfloat16
SPAN = 128


def dot_nn(left, right):
    return jnp.dot(left, right, preferred_element_type=F32)


def dot_nt(left, right):
    return lax.dot_general(left, right, (((1,), (1,)), ((), ())), preferred_element_type=F32)


def dot_tn(left, right):
    return lax.dot_general(left, right, (((0,), (0,)), ((), ())), preferred_element_type=F32)


def attend_jobs(jobs, me, sibling, kv_own, kv_sib, head_dim):
    passage_rows, half = kv_own.shape[1], kv_own.shape[2] // 2
    heads = half // head_dim
    scale = head_dim ** (-0.5)
    nothing = jnp.zeros((BLOCK, head_dim), BF16)

    def find(pairs, device):
        hit = jnp.int32(0)
        for owner, entry in pairs:
            hit = hit + (owner == device).astype(jnp.int32) * (entry + 1)
        found = jnp.minimum(hit, 1)
        return hit - found, (1 - found).astype(F32) * MISSING

    work = []
    for q_ref, named, o_ref, stat_ref in jobs:
        for block in range(q_ref.shape[0] // BLOCK):
            pairs = named(block)
            work.append((q_ref, o_ref, block, find(pairs, me), find(pairs, sibling)))
    scores = []
    for q_ref, _, block, (row_own, _), (row_sib, _) in work:
        query = q_ref[block * BLOCK : (block + 1) * BLOCK, :]
        spread = jnp.concatenate(
            [
                jnp.concatenate(
                    [
                        query[:, head * head_dim : (head + 1) * head_dim] if head == place else nothing
                        for place in range(heads)
                    ],
                    axis=1,
                )
                for head in range(heads)
            ],
            axis=0,
        )
        keys = jnp.concatenate([kv_own[row_own, :, :half], kv_sib[row_sib, :, :half]], axis=0)
        scores.append(dot_nt(keys, spread))
    weights, stats = [], []
    for (_, _, _, (_, bias_own), (_, bias_sib)), raw in zip(work, scores):
        own = raw[:passage_rows] * scale + bias_own
        sib = raw[passage_rows:] * scale + bias_sib
        peak = jnp.max(jnp.maximum(own, sib), axis=0, keepdims=True)
        e_own = jnp.exp(own - peak)
        e_sib = jnp.exp(sib - peak)
        total = jnp.sum(e_own + e_sib, axis=0, keepdims=True)
        inv = 1.0 / total
        weights.append(jnp.concatenate([e_own * inv, e_sib * inv], axis=0).astype(BF16))
        stats.append(peak + jnp.log(total))
    for (_, o_ref, block, (row_own, _), (row_sib, _)), weight in zip(work, weights):
        values = jnp.concatenate([kv_own[row_own, :, half:], kv_sib[row_sib, :, half:]], axis=0)
        result = dot_tn(weight, values)
        for head in range(heads):
            cols = slice(head * head_dim, (head + 1) * head_dim)
            o_ref[block * BLOCK : (block + 1) * BLOCK, cols] = result[
                head * BLOCK : (head + 1) * BLOCK, cols
            ].astype(BF16)
    done = 0
    for q_ref, _, _, stat_ref in jobs:
        blocks = q_ref.shape[0] // BLOCK
        rows = jnp.concatenate(stats[done : done + blocks], axis=0)
        done += blocks
        spare = stat_ref.shape[1] - rows.shape[1]
        if spare:
            rows = jnp.concatenate([rows, jnp.zeros((blocks, spare), F32)], axis=1)
        stat_ref[...] = rows


def shares_of(stats):
    peak = functools.reduce(jnp.maximum, stats)
    expo = [jnp.exp(stat - peak) for stat in stats]
    total = functools.reduce(jnp.add, expo)
    inv = 1.0 / total
    pad = (-peak.shape[0]) % 8
    rows = [e * inv for e in expo]
    if pad:
        rows = [jnp.concatenate([r, jnp.zeros((pad, r.shape[1]), F32)], axis=0) for r in rows]
    return [jnp.transpose(r) for r in rows], peak + jnp.log(total)


def blend(refs, shares, block, local, head_dim):
    at = slice(block * BLOCK, (block + 1) * BLOCK)
    cols = slice(local * head_dim, (local + 1) * head_dim)
    return functools.reduce(
        jnp.add,
        [
            ref[at, cols].astype(F32) * share[local * BLOCK : (local + 1) * BLOCK, block : block + 1]
            for ref, share in zip(refs, shares)
        ],
    )


def gate_rows(gates, extra_ref, rate_ref):
    heads, length = extra_ref.shape
    rows = jnp.transpose(gates)
    beta = jax.nn.sigmoid(rows[:heads])
    raw = rows[heads : 2 * heads]
    softplus = jnp.maximum(raw, 0.0) + jnp.log1p(jnp.exp(-jnp.abs(raw)))
    which = lax.broadcasted_iota(jnp.int32, (heads, length), 0)
    rate = jnp.zeros((heads, length), F32)
    for head in range(heads):
        rate = jnp.where(which == head, rate_ref[:, head : head + 1], rate)
    decay = -rate * softplus + extra_ref[...]
    rgate = jax.nn.sigmoid(rows[2 * heads : 3 * heads])
    tri = jnp.where(
        lax.broadcasted_iota(jnp.int32, (SPAN, SPAN), 0)
        <= lax.broadcasted_iota(jnp.int32, (SPAN, SPAN), 1),
        1.0,
        0.0,
    ).astype(F32)
    pad = jnp.zeros((8 - heads, SPAN), F32)
    spans = []
    for span in range(length // SPAN):
        at = slice(span * SPAN, (span + 1) * SPAN)
        cum = jnp.dot(
            jnp.concatenate([decay[:, at], pad], axis=0),
            tri,
            precision=lax.Precision.HIGHEST,
            preferred_element_type=F32,
        )[:heads]
        ends = cum[:, SPAN - 1 : SPAN]
        grow = jnp.exp(cum)
        cols = jnp.transpose(jnp.concatenate([cum, beta[:, at], grow, rgate[:, at]], axis=0))
        spans.append((cum, beta[:, at], beta[:, at] * grow, jnp.exp(ends - cum), jnp.exp(ends), cols, rgate[:, at]))
    return spans


def delta_body(spans, read, gain, heads, store):
    head_dim = gain.shape[1]
    count = len(spans)
    half = SPAN // 2
    row = lax.broadcasted_iota(jnp.int32, (SPAN, SPAN), 0)
    col = lax.broadcasted_iota(jnp.int32, (SPAN, SPAN), 1)
    lower = row >= col
    strict = row > col
    prow = lax.broadcasted_iota(jnp.int32, (half, SPAN), 0)
    plane = lax.broadcasted_iota(jnp.int32, (half, SPAN), 1)
    pcol = plane % half
    is_left = plane < half
    left = jnp.where(is_left, 1.0, 0.0).astype(BF16)
    right = jnp.where(is_left, 0.0, 1.0).astype(BF16)
    eye = jnp.where(prow == pcol, 1.0, 0.0).astype(F32)
    sizes = []
    size = 2
    while size < half:
        sizes.append(size)
        size *= 2

    def cut_of(size):
        return ((prow // (2 * size)) == (pcol // (2 * size))) & ((prow // size) != (pcol // size))

    first = jnp.where(cut_of(1), 1.0, 0.0).astype(F32)
    cuts = []
    for size in sizes:
        cut = jnp.where(cut_of(size), 1.0, 0.0).astype(BF16)
        cuts.append((cut * left, cut * right))
    units = [(head, span) for head in range(heads) for span in range(count)]
    kb, kt, grams, mixes = {}, {}, {}, {}
    for unit in units:
        k32 = read("k", *unit).astype(F32)
        kn = k32 * lax.rsqrt(jnp.sum(k32 * k32, axis=1, keepdims=True) + EPS)
        kb[unit] = kn.astype(BF16)
        kt[unit] = jnp.transpose(kn)
    for unit in units:
        turned = kt[unit].astype(BF16)
        grams[unit] = dot_nn(kb[unit], turned)
        mixes[unit] = dot_nn(read("q", *unit), turned)
    within, packed, corner, inverse = {}, {}, {}, {}
    for unit in units:
        head, span = unit
        cum, _, _, _, _, cols, _ = spans[span]
        spread = cols[:, head : head + 1] - cum[head : head + 1, :]
        damp = jnp.where(lower, jnp.exp(jnp.minimum(spread, 0.0)), 0.0)
        within[unit] = (mixes[unit] * damp).astype(BF16)
        inner = jnp.where(strict, grams[unit] * damp * cols[:, heads + head : heads + head + 1], 0.0)
        pack = jnp.where(is_left, inner[:half], inner[half:])
        packed[unit] = pack.astype(BF16)
        corner[unit] = jnp.where(is_left, inner[half:], 0.0).astype(BF16)
        inverse[unit] = eye - pack * first
    for cut_left, cut_right in cuts:
        parts = {}
        for unit in units:
            piece = packed[unit]
            parts[unit] = dot_nn(
                inverse[unit].astype(BF16),
                jnp.concatenate([piece * cut_left, piece * cut_right], axis=0),
            )
        for unit in units:
            now = inverse[unit].astype(BF16)
            inverse[unit] = inverse[unit] - dot_nn(
                parts[unit].astype(BF16), jnp.concatenate([now * left, now * right], axis=0)
            )
    parts = {}
    for unit in units:
        now = inverse[unit].astype(BF16)
        parts[unit] = dot_nn(corner[unit], jnp.concatenate([now * left, now * right], axis=0))
    zeros = jnp.zeros((half, SPAN), BF16)
    full = {}
    for unit in units:
        now = inverse[unit]
        link = dot_nn(
            now.astype(BF16) * right, jnp.concatenate([zeros, parts[unit].astype(BF16)], axis=0)
        )
        full[unit] = jnp.concatenate(
            [jnp.where(is_left, now, 0.0), jnp.where(is_left, -link, now)], axis=0
        )
    base, key_mix, tails = {}, {}, {}
    for unit in units:
        head, span = unit
        _, beta, beta_grow, tail, _, _, _ = spans[span]
        base[unit] = dot_nn((full[unit] * beta[head : head + 1, :]).astype(BF16), read("v", *unit))
        key_mix[unit] = dot_nn(
            (full[unit] * beta_grow[head : head + 1, :]).astype(BF16), kb[unit]
        ).astype(BF16)
        tails[unit] = (kt[unit] * tail[head : head + 1, :]).astype(BF16)
    state = [jnp.zeros((head_dim, head_dim), F32) for _ in range(heads)]
    for span in range(count):
        reads = [
            dot_nn(
                jnp.concatenate([key_mix[head, span], read("q", head, span)], axis=0),
                state[head].astype(BF16),
            )
            for head in range(heads)
        ]
        fresh = [(base[head, span] - reads[head][:SPAN]).astype(BF16) for head in range(heads)]
        carry = spans[span][4]
        state = [
            state[head] * carry[head : head + 1, :] + dot_nn(tails[head, span], fresh[head])
            for head in range(heads)
        ]
        for head in range(heads):
            cols = spans[span][5]
            grow = cols[:, 2 * heads + head : 2 * heads + head + 1]
            result = reads[head][SPAN:] * grow + dot_nn(within[head, span], fresh[head])
            q32 = read("q", head, span).astype(F32)
            square = jnp.sum(q32 * q32, axis=1, keepdims=True)
            norm = lax.rsqrt(
                jnp.mean(result * result, axis=1, keepdims=True)
                + EPS * head_dim * (square + EPS)
            )
            store(head, span, result * norm * gain)


def whole_kernel(
    chips,
    head_dim,
    passage_rows,
    lesser,
    tokens_hbm,
    store_hbm,
    weights_hbm,
    o_ref,
    owners_ref,
    entries_ref,
    extra_ref,
    small_a,
    small_b,
    small_c,
    gain_ref,
    rate_ref,
    gate_ref,
    tok,
    sto,
    wts,
    rq,
    qkv,
    kv_own,
    kv_sib,
    kv_out,
    qbuf,
    obuf,
    sbuf,
    rbuf,
    rstat,
    fin,
    fstat,
    normed,
    gsel,
    want_mine,
    want_all,
    want_smem,
    load_sem,
    want_sem,
    kv_sem,
    send_q,
    recv_q,
    send_r,
    send_s,
    recv_s,
    recv_f,
    recv_g,
    send_w,
    recv_w,
    send_h,
):
    devices = 2 * chips
    reach = chips // 2
    me = lax.axis_index("st")
    core, chip = lax.rem(me, 2), me // 2
    other = 1 - core
    sibling = chip * 2 + other
    length, width = normed.shape
    half = width // 2
    heads = width // head_dim
    here = heads // 2
    pieces = rq.shape[1]
    piece_rows = length // pieces
    piece_blocks = piece_rows // BLOCK
    per = owners_ref.shape[0]
    blocks = owners_ref.shape[1]

    def rcopy(src, dst, ssem, rsem, target):
        return pltpu.make_async_remote_copy(
            src_ref=src,
            dst_ref=dst,
            send_sem=ssem,
            recv_sem=rsem,
            device_id={"st": target},
            device_id_type=pl.DeviceIdType.MESH,
        )

    rq_w, pk_w, pv_w, q_w = 0, 1, 2, 3

    def token_rows(piece):
        at = pl.ds(piece * piece_rows, piece_rows)
        return pltpu.make_async_copy(tokens_hbm.at[at], tok.at[at], load_sem.at[6 + piece])

    def query_weight(which, index):
        at = pl.ds(pl.multiple_of(which * half, half), half)
        return pltpu.make_async_copy(
            weights_hbm[rq_w].at[:, at], wts.at[rq_w, :, at], load_sem.at[index]
        )

    loads = [None, None]
    loads += [
        pltpu.make_async_copy(weights_hbm[i], wts.at[i], load_sem.at[min(1 + i, 4)])
        for i in range(1, 6)
    ]
    loads.append(pltpu.make_async_copy(store_hbm, sto, load_sem.at[5]))
    first_loads = [token_rows(0), query_weight(core, 0)]
    second_loads = [token_rows(piece) for piece in range(1, pieces)] + [query_weight(other, 1)]
    small_refs = (small_a, small_b, small_c)
    lesser_loads = [
        pltpu.make_async_copy(src, dst, load_sem.at[6 + pieces + i])
        for i, (src, dst) in enumerate(
            zip(lesser, (owners_ref, entries_ref, extra_ref) + small_refs + (gain_ref, rate_ref))
        )
    ]
    for copy in first_loads + second_loads + lesser_loads[:2]:
        copy.start()
    barrier = pltpu.get_barrier_semaphore()

    @pl.loop(1, devices)
    def _(off):
        pl.semaphore_signal(
            barrier,
            inc=1,
            device_id={"st": lax.rem(me + off, devices)},
            device_id_type=pl.DeviceIdType.MESH,
        )

    with jax.named_scope("wait_tok"):
        for copy in first_loads:
            copy.wait()
    loads[7].start()
    loads[1 + pk_w].start()

    def project_query(side, piece):
        at = pl.ds(piece * piece_rows, piece_rows)
        cols = pl.ds(pl.multiple_of(side * half, half), half)
        rq[side, piece] = dot_nn(tok[at, :], wts[rq_w, :, cols]).astype(BF16)

    def all_of(shaped, sem):
        return pltpu.make_async_copy(shaped, shaped, sem)

    def want_copy(off):
        return rcopy(
            want_mine,
            want_all.at[me],
            send_w,
            recv_w,
            lax.rem(me + off, devices),
        )

    def own_query(there, side, piece, way):
        return rcopy(
            rq.at[side, piece],
            qbuf.at[me, piece],
            send_q.at[way],
            recv_q.at[me, piece],
            there * 2 + side,
        )

    def pass_query(source, piece, there, way):
        return rcopy(
            qbuf.at[source, piece],
            qbuf.at[source, piece],
            send_q.at[way],
            recv_q.at[source, piece],
            there * 2 + core,
        )

    def await_query(source, piece):
        pass_query(source, piece, sibling // 2, 0).wait_recv()

    def result_to(source, piece, dst, dstat, rsem, gsem, target):
        return (
            rcopy(obuf.at[source, piece], dst, send_r, rsem, target),
            rcopy(sbuf.at[source, piece], dstat, send_s, gsem, target),
        )

    def pass_result(source, piece, there):
        return result_to(
            source,
            piece,
            rbuf.at[source, piece],
            rstat.at[source, piece],
            recv_q.at[source, piece],
            recv_s.at[source, piece],
            there * 2 + core,
        )

    def give_result(source, piece, side):
        return result_to(
            source,
            piece,
            fin.at[side, core, piece],
            fstat.at[side, core, piece],
            recv_f.at[side, core, piece],
            recv_g.at[side, core, piece],
            source,
        )

    def await_result(source, piece):
        for copy in pass_result(source, piece, sibling // 2):
            copy.wait_recv()

    def await_final(side, which, piece):
        copies = result_to(
            me,
            piece,
            fin.at[side, which, piece],
            fstat.at[side, which, piece],
            recv_f.at[side, which, piece],
            recv_g.at[side, which, piece],
            sibling,
        )
        for copy in copies:
            copy.wait_recv()

    def begin(copies):
        for copy in copies if isinstance(copies, tuple) else (copies,):
            copy.start()

    def job(source, piece, own=False):
        def named(block):
            at = piece * piece_blocks + block
            return [
                (
                    want_smem[source, 0, place * blocks + at],
                    want_smem[source, 0, (per + place) * blocks + at],
                )
                for place in range(per)
            ]

        if own:
            return (
                rq.at[core, piece], named, fin.at[2, core, piece], fstat.at[2, core, piece]
            )
        return (qbuf.at[source, piece], named, obuf.at[source, piece], sbuf.at[source, piece])

    def attend(*jobs):
        attend_jobs(jobs, me, sibling, kv_own, kv_sib, head_dim)

    def attend_here():
        @pl.loop(0, pieces)
        def _(piece):
            await_query(sibling, piece)
            attend(job(me, piece, own=True), job(sibling, piece))
            begin(give_result(sibling, piece, 2))

    def merge(source, piece):
        await_result(source, piece)
        refs = [obuf.at[source, piece], rbuf.at[source, piece]]
        shares, stat = shares_of([sbuf[source, piece], rstat[source, piece]])
        for block in range(piece_blocks):
            for local in range(here):
                value = blend(refs, shares, block, local, head_dim)
                obuf[
                    source,
                    piece,
                    block * BLOCK : (block + 1) * BLOCK,
                    local * head_dim : (local + 1) * head_dim,
                ] = value.astype(BF16)
        sbuf[source, piece] = stat

    inner = jnp.logical_and(chip > 0, chip < chips - 1)
    end = jnp.logical_or(chip == 0, chip == chips - 1)
    near = 2 * (chip // reach) - 1
    far = -near
    near_side, far_side = (1 - near) // 2, (1 - far) // 2

    def own_first(piece):
        @pl.when(inner)
        def _():
            own_query(chip + near, core, piece, 0).start()
            own_query(chip + far, core, piece, 1).start()

        @pl.when(end)
        def _():
            own_query(chip + far, core, piece, 1).start()

    with jax.named_scope("rq0"):
        project_query(core, 0)
    with jax.named_scope("barrier_wait"):
        pl.semaphore_wait(barrier, devices - 1)
    with jax.named_scope("rq1"):

        own_first(0)
        lesser_loads[0].wait()
        lesser_loads[1].wait()
        named_rows = [
            ref[place : place + 1, :] for ref in (owners_ref, entries_ref) for place in range(per)
        ]
        want = jnp.concatenate(
            named_rows + [jnp.zeros((1, want_mine.shape[1] - 2 * per * blocks), jnp.int32)], axis=1
        )
        want_mine[...] = want
        want_all[me] = want
        for copy in second_loads:
            copy.wait()
        loads[1 + pv_w].start()
        for piece in range(1, pieces):
            project_query(core, piece)
            own_first(piece)

        @pl.loop(1, devices)
        def _(off):
            want_copy(off).start()

        for copy in lesser_loads[2:]:
            copy.start()
        for piece in range(pieces):
            project_query(other, piece)

    @pl.when(end)
    def _():
        for piece in range(pieces):
            own_query(chip + far, other, piece, 1).start()

    def sib_copy(piece):
        return rcopy(
            rq.at[other, piece], qbuf.at[me, piece], send_h, recv_q.at[me, piece], sibling
        )

    rows = sto.shape[0]
    tile = min(512, rows)

    def project_store(which, weight, dst, place, m):
        cols = pl.ds(pl.multiple_of(which * half, half), half)
        at = pl.ds(pl.multiple_of(m * tile, tile), tile)
        held = dot_nn(sto[at, :], wts[weight, :, cols]).astype(BF16)
        count = tile // passage_rows
        dst[pl.ds(m * count, count), :, place * half : (place + 1) * half] = held.reshape(
            count, passage_rows, half
        )

    def relay_first(piece):
        edge, peer = chip + near, chip + far

        @pl.when(inner)
        def _():
            await_query(edge * 2 + core, piece)
            pass_query(edge * 2 + core, piece, peer, 1).start()
            await_query(peer * 2 + core, piece)
            pass_query(peer * 2 + core, piece, edge, 0).start()

    tiles = rows // tile
    with jax.named_scope("kv"):
        loads[7].wait()
        loads[1 + pk_w].wait()
        for i in range(3):
            loads[1 + q_w + i].start()

        @pl.loop(0, tiles)
        def _(m):
            project_store(other, pk_w, kv_out, 0, m)

        loads[1 + pv_w].wait()

        @pl.loop(0, tiles)
        def _(m):
            project_store(other, pv_w, kv_out, 1, m)

        swap = rcopy(kv_out, kv_sib, kv_sem.at[0], kv_sem.at[1], sibling)
        swap.start()
        for piece in range(pieces):
            sib_copy(piece).start()

        @pl.loop(0, tiles)
        def _(m):
            project_store(core, pk_w, kv_own, 0, m)

    with jax.named_scope("relay0"):
        relay_first(0)
    with jax.named_scope("kv2"):

        @pl.loop(0, tiles)
        def _(m):
            project_store(core, pv_w, kv_own, 1, m)

    with jax.named_scope("relay1"):
        for piece in range(1, pieces):
            relay_first(piece)

    def project_mixer(step):
        i, side = step // 2, lax.rem(step, 2)
        cols = pl.ds(pl.multiple_of(side * half, half), half)
        qkv[i, :, cols] = dot_nn(tok[...], wts[q_w + i, :, cols]).astype(BF16)

    def project_gates():
        small = jnp.concatenate(
            [ref[...] for ref in small_refs]
            + [jnp.zeros((16 - 3 * heads, tok.shape[1]), BF16)],
            axis=0,
        )
        gate_ref[...] = dot_nt(tok[...], small)

    with jax.named_scope("wants"):

        all_of(want_all.at[pl.ds(0, devices - 1)], recv_w).wait()
        fetch = pltpu.make_async_copy(want_all, want_smem, want_sem)
        fetch.start()
        fetch.wait()
        swap.wait()
        for copy in lesser_loads[2:]:
            copy.wait()
        all_of(wts.at[pl.ds(q_w, 3)], load_sem.at[4]).wait()

    @pl.when(inner)
    def _():
        edge, peer, beyond = chip + near, chip + far, chip + 2 * far

        def at(where, which):
            return where * 2 + which

        with jax.named_scope("in01"):

            @pl.loop(0, pieces)
            def _(piece):
                attend(job(at(edge, core), piece), job(at(peer, core), piece))

        with jax.named_scope("in_here"):
            attend_here()
        with jax.named_scope("in23"):

            @pl.loop(0, pieces)
            def _(piece):
                await_query(at(edge, other), piece)
                pass_query(at(edge, other), piece, peer, 1).start()
                await_query(at(beyond, core), piece)
                pass_query(at(beyond, core), piece, edge, 0).start()
                attend(job(at(edge, other), piece), job(at(beyond, core), piece))

                @pl.loop(2 * piece, 2 * piece + 2)
                def _(step):
                    project_mixer(step)


        for piece in range(pieces):
            own_query(peer, other, piece, 1).start()
        with jax.named_scope("in45"):

            @pl.loop(0, pieces)
            def _(piece):
                await_query(at(beyond, other), piece)
                pass_query(at(beyond, other), piece, edge, 0).start()
                attend(job(at(beyond, other), piece))
                project_mixer(2 * pieces + piece)

        project_gates()
        with jax.named_scope("in67"):

            @pl.loop(0, pieces)
            def _(piece):
                await_query(at(peer, other), piece)
                pass_query(at(peer, other), piece, edge, 0).start()
                merge(at(beyond, core), piece)
                begin(pass_result(at(beyond, core), piece, peer))
                attend(job(at(peer, other), piece))

        for piece in range(pieces):
            own_query(edge, other, piece, 0).start()
        with jax.named_scope("in89"):

            @pl.loop(0, pieces)
            def _(piece):
                merge(at(beyond, other), piece)
                begin(pass_result(at(beyond, other), piece, peer))
                merge(at(edge, core), piece)
                begin(give_result(at(edge, core), piece, near_side))

        with jax.named_scope("in1011"):

            @pl.loop(0, pieces)
            def _(piece):
                merge(at(peer, core), piece)
                begin(give_result(at(peer, core), piece, far_side))
                merge(at(edge, other), piece)
                begin(give_result(at(edge, other), piece, near_side))

        with jax.named_scope("in12"):

            @pl.loop(0, pieces)
            def _(piece):
                merge(at(peer, other), piece)
                begin(give_result(at(peer, other), piece, far_side))

    @pl.when(end)
    def _():
        def at(distance, which):
            return (chip + far * distance) * 2 + which

        def handle(distance, which, send, fill=None):
            @pl.loop(0, pieces)
            def _(piece):
                await_query(at(distance, which), piece)
                attend(job(at(distance, which), piece))
                if send:
                    if distance == 1:
                        begin(give_result(at(distance, which), piece, far_side))
                    else:
                        begin(pass_result(at(distance, which), piece, chip + far))
                if fill is not None:
                    fill(piece)

        def fill_two(piece):
            @pl.loop(2 * piece, 2 * piece + 2)
            def _(step):
                project_mixer(step)

        def fill_one(piece):
            project_mixer(2 * pieces + piece)

        with jax.named_scope("end01"):
            handle(1, core, False)
        with jax.named_scope("end_here"):
            attend_here()
        with jax.named_scope("end23"):
            handle(2, core, True, fill_two)
        with jax.named_scope("end45"):
            handle(3, core, True, fill_one)
        project_gates()
        with jax.named_scope("end67"):
            handle(3, other, True)
        with jax.named_scope("end89"):
            handle(2, other, True)
        for piece in range(pieces):
            begin(give_result(at(1, core), piece, far_side))
        with jax.named_scope("end1011"):
            handle(1, other, True)

    with jax.named_scope("gates"):
        spans = gate_rows(gate_ref[...], extra_ref, rate_ref)
        for span, held in enumerate(spans):
            for side in range(2):
                rgate = held[6][side * here : (side + 1) * here]
                gsel[side, span * SPAN : (span + 1) * SPAN, :8] = jnp.transpose(
                    jnp.concatenate([rgate, jnp.zeros((8 - here, SPAN), F32)], axis=0)
                )

    def read(name, head, span):
        return qkv[
            "qkv".index(name),
            span * SPAN : (span + 1) * SPAN,
            head * head_dim : (head + 1) * head_dim,
        ]

    def keep(head, span, value):
        normed[span * SPAN : (span + 1) * SPAN, head * head_dim : (head + 1) * head_dim] = value

    with jax.named_scope("delta"):
        delta_body(spans, read, gain_ref[...], heads, keep)

    def finish(which, piece, sides):
        @pl.when(which == other)
        def _():
            await_final(2, which, piece)

        for side in sides[:-1]:
            await_final(side, which, piece)
        refs = [fin.at[side, which, piece] for side in sides]
        shares, _ = shares_of([fstat[side, which, piece] for side in sides])
        for block in range(piece_blocks):
            at = pl.ds(pl.multiple_of(piece * piece_rows + block * BLOCK, BLOCK), BLOCK)
            for local in range(here):
                cols = pl.ds(
                    pl.multiple_of(which * half + local * head_dim, head_dim), head_dim
                )
                value = blend(refs, shares, block, local, head_dim)
                rgate = gsel[which, at, local : local + 1]
                o_ref[at, cols] = (normed[at, cols] + rgate * value).astype(BF16)

    def finish_all(sides):
        @pl.loop(0, 2 * pieces)
        def _(step):
            finish(lax.rem(core + step // pieces, 2), lax.rem(step, pieces), sides)

    with jax.named_scope("finish"):

        @pl.when(inner)
        def _():
            finish_all((0, 1, 2))

        @pl.when(end)
        def _():
            finish_all((1 - far_side, 2))

    all_of(want_all.at[pl.ds(0, devices - 1)], send_w).wait()
    all_of(qbuf.at[0], send_h).wait()
    all_of(obuf.at[pl.ds(0, devices - 1)], send_r).wait()
    all_of(sbuf.at[pl.ds(0, devices - 1)], send_s).wait()

    @pl.when(inner)
    def _():
        all_of(qbuf.at[pl.ds(0, 6)], send_q.at[0]).wait()
        all_of(qbuf.at[pl.ds(0, 4)], send_q.at[1]).wait()

    @pl.when(end)
    def _():
        all_of(qbuf.at[pl.ds(0, 2)], send_q.at[1]).wait()


def line_device(
    chips,
    tokens,
    owners,
    entries,
    store,
    mixer_query_weight,
    mixer_key_weight,
    mixer_value_weight,
    strength_weight,
    decay_weight,
    head_decay_rate,
    extra_forgetting_exponent,
    output_norm_gain,
    retrieval_query_weight,
    passage_key_weight,
    passage_value_weight,
    retrieval_gate_weight,
):
    heads = head_decay_rate.shape[0]
    head_dim = output_norm_gain.shape[0]
    length, depth = tokens.shape
    passage_rows = store.shape[1]
    rows = store.shape[0] * passage_rows
    width = heads * head_dim
    half = width // 2
    devices = 2 * chips
    blocks = owners.shape[0]
    pieces = 2
    piece_rows, piece_blocks = length // pieces, blocks // pieces
    lanes = 2 * BLOCK
    vmem = pl.BlockSpec(memory_space=pltpu.VMEM)
    anywhere = pl.BlockSpec(memory_space=pltpu.HBM)
    weights = [
        retrieval_query_weight,
        passage_key_weight,
        passage_value_weight,
        mixer_query_weight,
        mixer_key_weight,
        mixer_value_weight,
    ]

    def body(*refs):
        whole_kernel(
            chips, head_dim, passage_rows, refs[:8], refs[8], refs[9], refs[10:16], *refs[16:]
        )

    dma = pltpu.SemaphoreType.DMA
    call = pl.pallas_call(
        body,
        out_shape=jax.ShapeDtypeStruct((length, width), BF16),
        in_specs=[anywhere] * 16,
        out_specs=vmem,
        scratch_shapes=[
            pltpu.VMEM(owners.shape[::-1], jnp.int32),
            pltpu.VMEM(owners.shape[::-1], jnp.int32),
            pltpu.VMEM((heads, length), F32),
            pltpu.VMEM((heads, depth), BF16),
            pltpu.VMEM((heads, depth), BF16),
            pltpu.VMEM((heads, depth), BF16),
            pltpu.VMEM((1, head_dim), F32),
            pltpu.VMEM((1, heads), F32),
            pltpu.VMEM((length, 16), F32),
            pltpu.VMEM((length, depth), BF16),
            pltpu.VMEM((rows, depth), BF16),
            pltpu.VMEM((6, depth, width), BF16),
            pltpu.VMEM((2, pieces, piece_rows, half), BF16),
            pltpu.VMEM((3, length, width), BF16),
            pltpu.VMEM((store.shape[0], passage_rows, width), BF16),
            pltpu.VMEM((store.shape[0], passage_rows, width), BF16),
            pltpu.VMEM((store.shape[0], passage_rows, width), BF16),
            pltpu.VMEM((devices, pieces, piece_rows, half), BF16),
            pltpu.VMEM((devices, pieces, piece_rows, half), BF16),
            pltpu.VMEM((devices, pieces, piece_blocks, lanes), F32),
            pltpu.VMEM((devices, pieces, piece_rows, half), BF16),
            pltpu.VMEM((devices, pieces, piece_blocks, lanes), F32),
            pltpu.VMEM((3, 2, pieces, piece_rows, half), BF16),
            pltpu.VMEM((3, 2, pieces, piece_blocks, lanes), F32),
            pltpu.VMEM((length, width), F32),
            pltpu.VMEM((2, length, 128), F32),
            pltpu.VMEM((1, 128), jnp.int32),
            pltpu.VMEM((devices, 1, 128), jnp.int32),
            pltpu.SMEM((devices, 1, 128), jnp.int32),
            dma((6 + pieces + 8,)),
            dma,
            dma((2,)),
            dma((2,)),
            dma((devices, pieces)),
            dma,
            dma,
            dma((devices, pieces)),
            dma((3, 2, pieces)),
            dma((3, 2, pieces)),
            dma,
            dma,
            dma,
        ],
        compiler_params=pltpu.CompilerParams(
            collective_id=0, has_side_effects=True, vmem_limit_bytes=54000 * 1024
        ),
        cost_estimate=pl.CostEstimate(
            flops=12_000_000_000, bytes_accessed=20_000_000, transcendentals=0
        ),
        name="whole",
    )
    operands = (
        owners.T,
        entries.T,
        extra_forgetting_exponent.T,
        strength_weight.T,
        decay_weight.T,
        retrieval_gate_weight.T,
        output_norm_gain[None, :],
        head_decay_rate[None, :],
        tokens,
        store.reshape(rows, depth),
        *weights,
    )
    return call(*[pltpu.with_memory_space_constraint(array, pltpu.HBM) for array in operands])


def ring_attend(q_ref, named, me, sibling, kv_own, kv_sib, o_ref, stat_ref, passage_rows, head_dim):
    length, half = q_ref.shape
    heads = half // head_dim
    blocks = length // BLOCK
    scale = head_dim ** (-0.5)
    nothing = jnp.zeros((BLOCK, head_dim), BF16)

    def find(pairs, device):
        hit = jnp.int32(0)
        for owner, entry in pairs:
            hit = hit + (owner == device).astype(jnp.int32) * (entry + 1)
        found = jnp.minimum(hit, 1)
        return hit - found, (1 - found).astype(F32) * MISSING

    places, scores = [], []
    for block in range(blocks):
        pairs = named(block)
        row_own, bias_own = find(pairs, me)
        row_sib, bias_sib = find(pairs, sibling)
        places.append((row_own, bias_own, row_sib, bias_sib))
        query = q_ref[block * BLOCK : (block + 1) * BLOCK, :]
        spread = jnp.concatenate(
            [
                jnp.concatenate(
                    [
                        query[:, head * head_dim : (head + 1) * head_dim] if head == place else nothing
                        for place in range(heads)
                    ],
                    axis=1,
                )
                for head in range(heads)
            ],
            axis=0,
        )
        keys = jnp.concatenate(
            [
                kv_own[row_own, :, :half],
                kv_sib[row_sib, :, :half],
            ],
            axis=0,
        )
        scores.append(dot_nt(keys, spread))
    weights, stats = [], []
    for block in range(blocks):
        _, bias_own, _, bias_sib = places[block]
        raw = scores[block]
        own = raw[:passage_rows] * scale + bias_own
        sib = raw[passage_rows:] * scale + bias_sib
        peak = jnp.max(jnp.maximum(own, sib), axis=0, keepdims=True)
        e_own = jnp.exp(own - peak)
        e_sib = jnp.exp(sib - peak)
        total = jnp.sum(e_own + e_sib, axis=0, keepdims=True)
        inv = 1.0 / total
        weights.append(jnp.concatenate([e_own * inv, e_sib * inv], axis=0).astype(BF16))
        stats.append(peak + jnp.log(total))
    for block in range(blocks):
        row_own, _, row_sib, _ = places[block]
        values = jnp.concatenate(
            [
                kv_own[row_own, :, half:],
                kv_sib[row_sib, :, half:],
            ],
            axis=0,
        )
        result = dot_tn(weights[block], values)
        for head in range(heads):
            cols = slice(head * head_dim, (head + 1) * head_dim)
            o_ref[block * BLOCK : (block + 1) * BLOCK, cols] = result[
                head * BLOCK : (head + 1) * BLOCK, cols
            ].astype(BF16)
    rows = jnp.concatenate(stats, axis=0)
    spare = stat_ref.shape[1] - rows.shape[1]
    if spare:
        rows = jnp.concatenate([rows, jnp.zeros((blocks, spare), F32)], axis=1)
    stat_ref[...] = rows


def ring_kernel(
    chips,
    head_dim,
    passage_rows,
    owners_ref,
    entries_ref,
    extra_ref,
    small_refs,
    gain_ref,
    rate_ref,
    tokens_hbm,
    store_hbm,
    weights_hbm,
    o_ref,
    tok,
    sto,
    wts,
    rq,
    qkv,
    kv_own,
    kv_sib,
    kv_out,
    qbuf,
    obuf,
    sbuf,
    part,
    pstat,
    normed,
    want_mine,
    want_all,
    want_smem,
    load_sem,
    want_sem,
    kv_sem,
    send_q,
    recv_q,
    send_r,
    recv_r,
    send_s,
    recv_s,
    send_w,
    recv_w,
):
    devices = 2 * chips
    reach = chips // 2
    me = lax.axis_index("st")
    core, chip = lax.rem(me, 2), me // 2
    other = 1 - core
    sibling = chip * 2 + other
    length, width = normed.shape
    half = width // 2
    heads = width // head_dim

    def device(dz, which):
        return lax.rem(chip + dz, chips) * 2 + which

    def rcopy(src, dst, ssem, rsem, target):
        return pltpu.make_async_remote_copy(
            src_ref=src,
            dst_ref=dst,
            send_sem=ssem,
            recv_sem=rsem,
            device_id={"st": target},
            device_id_type=pl.DeviceIdType.MESH,
        )

    barrier = pltpu.get_barrier_semaphore()

    @pl.loop(1, devices)
    def _(off):
        pl.semaphore_signal(
            barrier,
            inc=1,
            device_id={"st": lax.rem(me + off, devices)},
            device_id_type=pl.DeviceIdType.MESH,
        )

    rq_w, pk_w, pv_w, q_w = 0, 1, 2, 3
    loads = [pltpu.make_async_copy(tokens_hbm, tok, load_sem.at[0])]
    loads += [
        pltpu.make_async_copy(weights_hbm[i], wts.at[i], load_sem.at[1 + i]) for i in range(6)
    ]
    loads.append(pltpu.make_async_copy(store_hbm, sto, load_sem.at[7]))
    loads[0].start()
    loads[1].start()

    want_mine[...] = jnp.zeros_like(want_mine)
    per = owners_ref.shape[0]
    blocks = owners_ref.shape[1]
    want_mine[:per, :blocks] = owners_ref[...]
    want_mine[per : 2 * per, :blocks] = entries_ref[...]
    want_all[me] = want_mine[...]

    loads[0].wait()
    loads[1].wait()
    loads[7].start()
    loads[1 + pk_w].start()
    loads[1 + pv_w].start()

    @pl.loop(0, 2)
    def _(side):
        cols = pl.ds(pl.multiple_of(side * half, half), half)
        rq[side] = dot_nn(tok[...], wts[rq_w, :, cols]).astype(BF16)

    pl.semaphore_wait(barrier, devices - 1)

    def slot(dz, which):
        return (dz % chips) * 2 + which

    hop1 = []
    for count, (dz, which) in enumerate(
        [(1, core), (chips - 1, other), (1, other), (chips - 1, core)]
    ):
        there = slot(chips - dz, core)
        hop1.append(
            rcopy(
                rq.at[which], qbuf.at[there], send_q.at[count], recv_q.at[there], device(dz, which)
            )
        )
    hop1.append(
        rcopy(rq.at[other], qbuf.at[core], send_q.at[4], recv_q.at[core], sibling)
    )
    for copy in hop1:
        copy.start()

    def want_copy(off):
        return rcopy(
            want_mine,
            want_all.at[me],
            send_w.at[off - 1],
            recv_w.at[me],
            lax.rem(me + off, devices),
        )

    @pl.loop(1, devices)
    def _(off):
        want_copy(off).start()

    qbuf[core] = rq[core]

    loads[7].wait()
    loads[1 + pk_w].wait()
    for i in range(3):
        loads[1 + q_w + i].start()

    rows = sto.shape[0]
    tile = min(512, rows)

    def project_store(which, weight, dst, place):
        cols = pl.ds(pl.multiple_of(which * half, half), half)

        @pl.loop(0, rows // tile)
        def _(m):
            at = pl.ds(pl.multiple_of(m * tile, tile), tile)
            held = dot_nn(sto[at, :], wts[weight, :, cols]).astype(BF16)
            count = tile // passage_rows
            dst[pl.ds(m * count, count), :, place * half : (place + 1) * half] = held.reshape(
                count, passage_rows, half
            )

    project_store(other, pk_w, kv_out, 0)
    loads[1 + pv_w].wait()
    project_store(other, pv_w, kv_out, 1)
    project_store(core, pk_w, kv_own, 0)
    swap = rcopy(kv_out, kv_sib, kv_sem.at[0], kv_sem.at[1], sibling)
    swap.start()
    project_store(core, pv_w, kv_own, 1)

    for i in range(3):
        loads[1 + q_w + i].wait()

    @pl.loop(0, 6)
    def _(step):
        i, side = step // 2, lax.rem(step, 2)
        cols = pl.ds(pl.multiple_of(side * half, half), half)
        qkv[i, :, cols] = dot_nn(tok[...], wts[q_w + i, :, cols]).astype(BF16)

    small = jnp.concatenate(
        [ref[...] for ref in small_refs] + [jnp.zeros((16 - 3 * heads, tok.shape[1]), BF16)], axis=0
    )
    gates = dot_nt(tok[...], small)
    spans = gate_rows(gates, extra_ref, rate_ref)

    @pl.loop(1, devices)
    def _(off):
        source = lax.rem(me + off, devices)
        rcopy(want_mine, want_all.at[source], send_w.at[0], recv_w.at[source], source).wait_recv()

    fetch = pltpu.make_async_copy(want_all, want_smem, want_sem)
    fetch.start()
    fetch.wait()
    swap.wait()

    def await_query(at):
        rcopy(rq.at[0], qbuf.at[at], send_q.at[0], recv_q.at[at], sibling).wait_recv()

    def attend(dz, which):
        at = slot(dz, which)
        source = device(dz, which)

        def named(block):
            return [
                (want_smem[source, place, block], want_smem[source, per + place, block])
                for place in range(per)
            ]

        ring_attend(
            qbuf.at[at],
            named,
            me,
            sibling,
            kv_own,
            kv_sib,
            obuf.at[at],
            sbuf.at[at],
            passage_rows,
            head_dim,
        )

    def reply(dz, which):
        at = slot(dz, which)
        back = (chips - dz) % chips
        target = device(dz, which)
        return (
            rcopy(
                obuf.at[at], part.at[back, core], send_r.at[at], recv_r.at[back, core], target
            ),
            rcopy(
                sbuf.at[at], pstat.at[back, core], send_s.at[at], recv_s.at[back, core], target
            ),
        )

    relays = []

    def relay(src, dst, count, target):
        copy = rcopy(qbuf.at[src], qbuf.at[dst], send_q.at[count], recv_q.at[dst], target)
        copy.start()
        relays.append(copy)

    count = 5
    await_query(other)

    @pl.loop(0, 2)
    def _(which):
        attend(0, which)

    part[0, core] = obuf[core]
    pstat[0, core] = sbuf[core]
    for copy in reply(0, other):
        copy.start()

    for hop in range(1, reach):
        back = chips - hop
        if hop < reach - 1:
            for which in range(2):
                await_query(slot(back, which))
                relay(slot(back, which), slot(back - 1, which), count, device(1, core))
                await_query(slot(hop, which))
                relay(slot(hop, which), slot(hop + 1, which), count + 1, device(chips - 1, core))
                count += 2
        else:
            await_query(slot(back, core))
            relay(slot(back, core), slot(reach, core), count, device(1, core))
            await_query(slot(hop, other))
            relay(slot(hop, other), slot(reach, other), count + 1, device(chips - 1, core))
            count += 2
            await_query(slot(back, other))
            await_query(slot(hop, core))
        for dz in (back, hop):

            @pl.loop(0, 2)
            def _(which):
                attend(dz, which)
                for copy in reply(dz, which):
                    copy.start()

    await_query(slot(reach, 0))
    await_query(slot(reach, 1))

    @pl.loop(0, 2)
    def _(which):
        attend(reach, which)
        for copy in reply(reach, which):
            copy.start()

    def read(name, head, span):
        return qkv[
            "qkv".index(name),
            span * SPAN : (span + 1) * SPAN,
            head * head_dim : (head + 1) * head_dim,
        ]

    def keep(head, span, value):
        normed[span * SPAN : (span + 1) * SPAN, head * head_dim : (head + 1) * head_dim] = value

    delta_body(spans, read, gain_ref[...], heads, keep)

    def await_part(back, side):
        rcopy(
            obuf.at[0], part.at[back, side], send_r.at[0], recv_r.at[back, side], sibling
        ).wait_recv()
        rcopy(
            sbuf.at[0], pstat.at[back, side], send_s.at[0], recv_s.at[back, side], sibling
        ).wait_recv()

    await_part(0, other)
    for back in range(1, chips):
        for side in range(2):
            await_part(back, side)

    here = heads // 2
    for side in range(2):
        stats = [pstat[back, side] for back in range(chips)]
        peak = functools.reduce(jnp.maximum, stats)
        expo = [jnp.exp(stat - peak) for stat in stats]
        inv = 1.0 / functools.reduce(jnp.add, expo)
        shares = [jnp.transpose(e * inv) for e in expo]
        for block in range(blocks):
            at = slice(block * BLOCK, (block + 1) * BLOCK)
            span, inside = divmod(block * BLOCK, SPAN)
            for local in range(here):
                cols = slice(local * head_dim, (local + 1) * head_dim)
                head = side * here + local
                where = slice(head * head_dim, (head + 1) * head_dim)
                value = functools.reduce(
                    jnp.add,
                    [
                        part[back, side, at, cols].astype(F32)
                        * shares[back][local * BLOCK : (local + 1) * BLOCK, block : block + 1]
                        for back in range(chips)
                    ],
                )
                rgate = spans[span][5][
                    inside : inside + BLOCK, 3 * heads + head : 3 * heads + head + 1
                ]
                o_ref[at, where] = (normed[at, where] + rgate * value).astype(BF16)

    for copy in hop1 + relays:
        copy.wait_send()

    @pl.loop(1, devices)
    def _(off):
        want_copy(off).wait_send()

    for copy in reply(0, other):
        copy.wait_send()
    for dz in range(1, chips):
        for which in range(2):
            for copy in reply(dz, which):
                copy.wait_send()


def ring_device(
    chips,
    tokens,
    owners,
    entries,
    store,
    mixer_query_weight,
    mixer_key_weight,
    mixer_value_weight,
    strength_weight,
    decay_weight,
    head_decay_rate,
    extra_forgetting_exponent,
    output_norm_gain,
    retrieval_query_weight,
    passage_key_weight,
    passage_value_weight,
    retrieval_gate_weight,
):
    heads = head_decay_rate.shape[0]
    head_dim = output_norm_gain.shape[0]
    length, depth = tokens.shape
    passage_rows = store.shape[1]
    rows = store.shape[0] * passage_rows
    width = heads * head_dim
    half = width // 2
    devices = 2 * chips
    blocks = owners.shape[0]
    vmem = pl.BlockSpec(memory_space=pltpu.VMEM)
    anywhere = pl.BlockSpec(memory_space=pl.ANY)
    weights = [
        retrieval_query_weight,
        passage_key_weight,
        passage_value_weight,
        mixer_query_weight,
        mixer_key_weight,
        mixer_value_weight,
    ]

    def body(owners_ref, entries_ref, extra_ref, s1, s2, s3, gain_ref, rate_ref, tok, sto, *rest):
        ring_kernel(
            chips, head_dim, passage_rows, owners_ref, entries_ref, extra_ref, (s1, s2, s3),
            gain_ref, rate_ref, tok, sto, rest[:6], *rest[6:],
        )

    dma = pltpu.SemaphoreType.DMA
    return pl.pallas_call(
        body,
        out_shape=jax.ShapeDtypeStruct((length, width), BF16),
        in_specs=[vmem] * 8 + [anywhere] * 8,
        out_specs=vmem,
        scratch_shapes=[
            pltpu.VMEM((length, depth), BF16),
            pltpu.VMEM((rows, depth), BF16),
            pltpu.VMEM((6, depth, width), BF16),
            pltpu.VMEM((2, length, half), BF16),
            pltpu.VMEM((3, length, width), BF16),
            pltpu.VMEM((store.shape[0], passage_rows, width), BF16),
            pltpu.VMEM((store.shape[0], passage_rows, width), BF16),
            pltpu.VMEM((store.shape[0], passage_rows, width), BF16),
            pltpu.VMEM((devices, length, half), BF16),
            pltpu.VMEM((devices, length, half), BF16),
            pltpu.VMEM((devices, blocks, 2 * BLOCK), F32),
            pltpu.VMEM((chips, 2, length, half), BF16),
            pltpu.VMEM((chips, 2, blocks, 2 * BLOCK), F32),
            pltpu.VMEM((length, width), F32),
            pltpu.VMEM((8, 128), jnp.int32),
            pltpu.VMEM((devices, 8, 128), jnp.int32),
            pltpu.SMEM((devices, 8, 128), jnp.int32),
            dma((8,)),
            dma,
            dma((2,)),
            dma((5 + 2 * devices,)),
            dma((devices,)),
            dma((devices,)),
            dma((chips, 2)),
            dma((devices,)),
            dma((chips, 2)),
            dma((devices,)),
            dma((devices,)),
        ],
        compiler_params=pltpu.CompilerParams(
            collective_id=0, has_side_effects=True, vmem_limit_bytes=60 * 1024 * 1024
        ),
        cost_estimate=pl.CostEstimate(
            flops=12_000_000_000, bytes_accessed=20_000_000, transcendentals=0
        ),
        name="ring",
    )(
        owners.T,
        entries.T,
        extra_forgetting_exponent.T,
        strength_weight.T,
        decay_weight.T,
        retrieval_gate_weight.T,
        output_norm_gain[None, :],
        head_decay_rate[None, :],
        tokens,
        store.reshape(rows, depth),
        *weights,
    )


def solution(mesh):
    rows = ("grp", "st")
    chips = mesh.shape["st"] // 2
    return jax.shard_map(
        functools.partial(line_device if chips // 2 == 2 else ring_device, chips),
        mesh=mesh,
        in_specs=(
            P(rows, None),
            P(rows, None),
            P(rows, None),
            P(rows, None, None),
            P(None, "tp"),
            P(None, "tp"),
            P(None, "tp"),
            P(None, "tp"),
            P(None, "tp"),
            P("tp"),
            P(rows, "tp"),
            P(),
            P(None, "tp"),
            P(None, "tp"),
            P(None, "tp"),
            P(None, "tp"),
        ),
        out_specs=P(rows, "tp"),
        check_vma=False,
    )
```

```python
import functools

import jax
import jax.numpy as jnp
from jax import lax
from jax.experimental import pallas as pl
from jax.experimental.pallas import tpu as pltpu
from jax.sharding import PartitionSpec as P

BLOCK = 64
EPS = 1e-06
MISSING = -1e30
F32 = jnp.float32
BF16 = jnp.bfloat16
SPAN = 128


def dot_nn(left, right):
    return jnp.dot(left, right, preferred_element_type=F32)


def dot_nt(left, right):
    return lax.dot_general(left, right, (((1,), (1,)), ((), ())), preferred_element_type=F32)


def dot_tn(left, right):
    return lax.dot_general(left, right, (((0,), (0,)), ((), ())), preferred_element_type=F32)


def attend_jobs(jobs, me, sibling, kv_own, kv_sib, head_dim):
    passage_rows, half = kv_own.shape[1], kv_own.shape[2] // 2
    heads = half // head_dim
    scale = head_dim ** (-0.5)
    nothing = jnp.zeros((BLOCK, head_dim), BF16)

    def find(pairs, device):
        hit = jnp.int32(0)
        for owner, entry in pairs:
            hit = hit + (owner == device).astype(jnp.int32) * (entry + 1)
        found = jnp.minimum(hit, 1)
        return hit - found, (1 - found).astype(F32) * MISSING

    work = []
    for q_ref, named, o_ref, stat_ref in jobs:
        for block in range(q_ref.shape[0] // BLOCK):
            pairs = named(block)
            work.append((q_ref, o_ref, block, find(pairs, me), find(pairs, sibling)))
    scores = []
    for q_ref, _, block, (row_own, _), (row_sib, _) in work:
        query = q_ref[block * BLOCK : (block + 1) * BLOCK, :]
        spread = jnp.concatenate(
            [
                jnp.concatenate(
                    [
                        query[:, head * head_dim : (head + 1) * head_dim] if head == place else nothing
                        for place in range(heads)
                    ],
                    axis=1,
                )
                for head in range(heads)
            ],
            axis=0,
        )
        keys = jnp.concatenate([kv_own[row_own, :, :half], kv_sib[row_sib, :, :half]], axis=0)
        scores.append(dot_nt(keys, spread))
    weights, stats = [], []
    for (_, _, _, (_, bias_own), (_, bias_sib)), raw in zip(work, scores):
        own = raw[:passage_rows] * scale + bias_own
        sib = raw[passage_rows:] * scale + bias_sib
        peak = jnp.max(jnp.maximum(own, sib), axis=0, keepdims=True)
        e_own = jnp.exp(own - peak)
        e_sib = jnp.exp(sib - peak)
        total = jnp.sum(e_own + e_sib, axis=0, keepdims=True)
        inv = 1.0 / total
        weights.append(jnp.concatenate([e_own * inv, e_sib * inv], axis=0).astype(BF16))
        stats.append(peak + jnp.log(total))
    for (_, o_ref, block, (row_own, _), (row_sib, _)), weight in zip(work, weights):
        values = jnp.concatenate([kv_own[row_own, :, half:], kv_sib[row_sib, :, half:]], axis=0)
        result = dot_tn(weight, values)
        for head in range(heads):
            cols = slice(head * head_dim, (head + 1) * head_dim)
            o_ref[block * BLOCK : (block + 1) * BLOCK, cols] = result[
                head * BLOCK : (head + 1) * BLOCK, cols
            ].astype(BF16)
    done = 0
    for q_ref, _, _, stat_ref in jobs:
        blocks = q_ref.shape[0] // BLOCK
        rows = jnp.concatenate(stats[done : done + blocks], axis=0)
        done += blocks
        spare = stat_ref.shape[1] - rows.shape[1]
        if spare:
            rows = jnp.concatenate([rows, jnp.zeros((blocks, spare), F32)], axis=1)
        stat_ref[...] = rows


def shares_of(stats):
    peak = functools.reduce(jnp.maximum, stats)
    expo = [jnp.exp(stat - peak) for stat in stats]
    total = functools.reduce(jnp.add, expo)
    inv = 1.0 / total
    pad = (-peak.shape[0]) % 8
    rows = [e * inv for e in expo]
    if pad:
        rows = [jnp.concatenate([r, jnp.zeros((pad, r.shape[1]), F32)], axis=0) for r in rows]
    return [jnp.transpose(r) for r in rows], peak + jnp.log(total)


def blend(refs, shares, block, local, head_dim):
    at = slice(block * BLOCK, (block + 1) * BLOCK)
    cols = slice(local * head_dim, (local + 1) * head_dim)
    return functools.reduce(
        jnp.add,
        [
            ref[at, cols].astype(F32) * share[local * BLOCK : (local + 1) * BLOCK, block : block + 1]
            for ref, share in zip(refs, shares)
        ],
    )


def gate_rows(gates, extra_ref, rate_ref):
    heads, length = extra_ref.shape
    rows = jnp.transpose(gates)
    beta = jax.nn.sigmoid(rows[:heads])
    raw = rows[heads : 2 * heads]
    softplus = jnp.maximum(raw, 0.0) + jnp.log1p(jnp.exp(-jnp.abs(raw)))
    which = lax.broadcasted_iota(jnp.int32, (heads, length), 0)
    rate = jnp.zeros((heads, length), F32)
    for head in range(heads):
        rate = jnp.where(which == head, rate_ref[:, head : head + 1], rate)
    decay = -rate * softplus + extra_ref[...]
    rgate = jax.nn.sigmoid(rows[2 * heads : 3 * heads])
    tri = jnp.where(
        lax.broadcasted_iota(jnp.int32, (SPAN, SPAN), 0)
        <= lax.broadcasted_iota(jnp.int32, (SPAN, SPAN), 1),
        1.0,
        0.0,
    ).astype(F32)
    pad = jnp.zeros((8 - heads, SPAN), F32)
    spans = []
    for span in range(length // SPAN):
        at = slice(span * SPAN, (span + 1) * SPAN)
        cum = jnp.dot(
            jnp.concatenate([decay[:, at], pad], axis=0),
            tri,
            precision=lax.Precision.HIGHEST,
            preferred_element_type=F32,
        )[:heads]
        ends = cum[:, SPAN - 1 : SPAN]
        grow = jnp.exp(cum)
        cols = jnp.transpose(jnp.concatenate([cum, beta[:, at], grow, rgate[:, at]], axis=0))
        spans.append((cum, beta[:, at], beta[:, at] * grow, jnp.exp(ends - cum), jnp.exp(ends), cols, rgate[:, at]))
    return spans


def delta_body(spans, read, gain, heads, store):
    head_dim = gain.shape[1]
    count = len(spans)
    half = SPAN // 2
    row = lax.broadcasted_iota(jnp.int32, (SPAN, SPAN), 0)
    col = lax.broadcasted_iota(jnp.int32, (SPAN, SPAN), 1)
    lower = row >= col
    strict = row > col
    prow = lax.broadcasted_iota(jnp.int32, (half, SPAN), 0)
    plane = lax.broadcasted_iota(jnp.int32, (half, SPAN), 1)
    pcol = plane % half
    is_left = plane < half
    left = jnp.where(is_left, 1.0, 0.0).astype(BF16)
    right = jnp.where(is_left, 0.0, 1.0).astype(BF16)
    eye = jnp.where(prow == pcol, 1.0, 0.0).astype(F32)
    sizes = []
    size = 2
    while size < half:
        sizes.append(size)
        size *= 2

    def cut_of(size):
        return ((prow // (2 * size)) == (pcol // (2 * size))) & ((prow // size) != (pcol // size))

    first = jnp.where(cut_of(1), 1.0, 0.0).astype(F32)
    cuts = []
    for size in sizes:
        cut = jnp.where(cut_of(size), 1.0, 0.0).astype(BF16)
        cuts.append((cut * left, cut * right))
    units = [(head, span) for head in range(heads) for span in range(count)]
    kb, kt, grams, mixes = {}, {}, {}, {}
    for unit in units:
        k32 = read("k", *unit).astype(F32)
        kn = k32 * lax.rsqrt(jnp.sum(k32 * k32, axis=1, keepdims=True) + EPS)
        kb[unit] = kn.astype(BF16)
        kt[unit] = jnp.transpose(kn)
    for unit in units:
        turned = kt[unit].astype(BF16)
        grams[unit] = dot_nn(kb[unit], turned)
        mixes[unit] = dot_nn(read("q", *unit), turned)
    within, packed, corner, inverse = {}, {}, {}, {}
    for unit in units:
        head, span = unit
        cum, _, _, _, _, cols, _ = spans[span]
        spread = cols[:, head : head + 1] - cum[head : head + 1, :]
        damp = jnp.where(lower, jnp.exp(jnp.minimum(spread, 0.0)), 0.0)
        within[unit] = (mixes[unit] * damp).astype(BF16)
        inner = jnp.where(strict, grams[unit] * damp * cols[:, heads + head : heads + head + 1], 0.0)
        pack = jnp.where(is_left, inner[:half], inner[half:])
        packed[unit] = pack.astype(BF16)
        corner[unit] = jnp.where(is_left, inner[half:], 0.0).astype(BF16)
        inverse[unit] = eye - pack * first
    for cut_left, cut_right in cuts:
        parts = {}
        for unit in units:
            piece = packed[unit]
            parts[unit] = dot_nn(
                inverse[unit].astype(BF16),
                jnp.concatenate([piece * cut_left, piece * cut_right], axis=0),
            )
        for unit in units:
            now = inverse[unit].astype(BF16)
            inverse[unit] = inverse[unit] - dot_nn(
                parts[unit].astype(BF16), jnp.concatenate([now * left, now * right], axis=0)
            )
    parts = {}
    for unit in units:
        now = inverse[unit].astype(BF16)
        parts[unit] = dot_nn(corner[unit], jnp.concatenate([now * left, now * right], axis=0))
    zeros = jnp.zeros((half, SPAN), BF16)
    full = {}
    for unit in units:
        now = inverse[unit]
        link = dot_nn(
            now.astype(BF16) * right, jnp.concatenate([zeros, parts[unit].astype(BF16)], axis=0)
        )
        full[unit] = jnp.concatenate(
            [jnp.where(is_left, now, 0.0), jnp.where(is_left, -link, now)], axis=0
        )
    base, key_mix, tails = {}, {}, {}
    for unit in units:
        head, span = unit
        _, beta, beta_grow, tail, _, _, _ = spans[span]
        base[unit] = dot_nn((full[unit] * beta[head : head + 1, :]).astype(BF16), read("v", *unit))
        key_mix[unit] = dot_nn(
            (full[unit] * beta_grow[head : head + 1, :]).astype(BF16), kb[unit]
        ).astype(BF16)
        tails[unit] = (kt[unit] * tail[head : head + 1, :]).astype(BF16)
    state = [jnp.zeros((head_dim, head_dim), F32) for _ in range(heads)]
    for span in range(count):
        reads = [
            dot_nn(
                jnp.concatenate([key_mix[head, span], read("q", head, span)], axis=0),
                state[head].astype(BF16),
            )
            for head in range(heads)
        ]
        fresh = [(base[head, span] - reads[head][:SPAN]).astype(BF16) for head in range(heads)]
        carry = spans[span][4]
        state = [
            state[head] * carry[head : head + 1, :] + dot_nn(tails[head, span], fresh[head])
            for head in range(heads)
        ]
        for head in range(heads):
            cols = spans[span][5]
            grow = cols[:, 2 * heads + head : 2 * heads + head + 1]
            result = reads[head][SPAN:] * grow + dot_nn(within[head, span], fresh[head])
            q32 = read("q", head, span).astype(F32)
            square = jnp.sum(q32 * q32, axis=1, keepdims=True)
            norm = lax.rsqrt(
                jnp.mean(result * result, axis=1, keepdims=True)
                + EPS * head_dim * (square + EPS)
            )
            store(head, span, result * norm * gain)


def whole_kernel(
    chips,
    head_dim,
    passage_rows,
    lesser,
    tokens_hbm,
    store_hbm,
    weights_hbm,
    o_ref,
    owners_ref,
    entries_ref,
    extra_ref,
    small_a,
    small_b,
    small_c,
    gain_ref,
    rate_ref,
    gate_ref,
    tok,
    sto,
    wts,
    rq,
    qkv,
    kv_own,
    kv_sib,
    kv_out,
    qbuf,
    obuf,
    sbuf,
    rbuf,
    rstat,
    fin,
    fstat,
    normed,
    gsel,
    want_mine,
    want_all,
    want_smem,
    load_sem,
    want_sem,
    kv_sem,
    send_q,
    recv_q,
    send_r,
    send_s,
    recv_s,
    recv_f,
    recv_g,
    send_w,
    recv_w,
    send_h,
):
    devices = 2 * chips
    reach = chips // 2
    me = lax.axis_index("st")
    core, chip = lax.rem(me, 2), me // 2
    other = 1 - core
    sibling = chip * 2 + other
    length, width = normed.shape
    half = width // 2
    heads = width // head_dim
    here = heads // 2
    pieces = rq.shape[1]
    piece_rows = length // pieces
    piece_blocks = piece_rows // BLOCK
    per = owners_ref.shape[0]
    blocks = owners_ref.shape[1]

    def rcopy(src, dst, ssem, rsem, target):
        return pltpu.make_async_remote_copy(
            src_ref=src,
            dst_ref=dst,
            send_sem=ssem,
            recv_sem=rsem,
            device_id={"st": target},
            device_id_type=pl.DeviceIdType.MESH,
        )

    rq_w, pk_w, pv_w, q_w = 0, 1, 2, 3

    def token_rows(piece):
        at = pl.ds(piece * piece_rows, piece_rows)
        return pltpu.make_async_copy(tokens_hbm.at[at], tok.at[at], load_sem.at[6 + piece])

    def query_weight(which, index):
        at = pl.ds(pl.multiple_of(which * half, half), half)
        return pltpu.make_async_copy(
            weights_hbm[rq_w].at[:, at], wts.at[rq_w, :, at], load_sem.at[index]
        )

    loads = [None, None]
    loads += [
        pltpu.make_async_copy(weights_hbm[i], wts.at[i], load_sem.at[min(1 + i, 4)])
        for i in range(1, 6)
    ]
    loads.append(pltpu.make_async_copy(store_hbm, sto, load_sem.at[5]))
    first_loads = [token_rows(0), query_weight(core, 0)]
    second_loads = [token_rows(piece) for piece in range(1, pieces)] + [query_weight(other, 1)]
    small_refs = (small_a, small_b, small_c)
    lesser_loads = [
        pltpu.make_async_copy(src, dst, load_sem.at[6 + pieces + i])
        for i, (src, dst) in enumerate(
            zip(lesser, (owners_ref, entries_ref, extra_ref) + small_refs + (gain_ref, rate_ref))
        )
    ]
    for copy in lesser_loads[:2] + first_loads + second_loads:
        copy.start()
    barrier = pltpu.get_barrier_semaphore()

    @pl.loop(1, devices)
    def _(off):
        pl.semaphore_signal(
            barrier,
            inc=1,
            device_id={"st": lax.rem(me + off, devices)},
            device_id_type=pl.DeviceIdType.MESH,
        )

    lesser_loads[0].wait()
    lesser_loads[1].wait()
    named_rows = [
        ref[place : place + 1, :] for ref in (owners_ref, entries_ref) for place in range(per)
    ]
    want = jnp.concatenate(
        named_rows + [jnp.zeros((1, want_mine.shape[1] - 2 * per * blocks), jnp.int32)], axis=1
    )
    want_mine[...] = want
    want_all[me] = want

    with jax.named_scope("wait_tok"):
        for copy in first_loads:
            copy.wait()
    loads[7].start()
    loads[1 + pk_w].start()

    def project_query(side, piece):
        at = pl.ds(piece * piece_rows, piece_rows)
        cols = pl.ds(pl.multiple_of(side * half, half), half)
        rq[side, piece] = dot_nn(tok[at, :], wts[rq_w, :, cols]).astype(BF16)

    def all_of(shaped, sem):
        return pltpu.make_async_copy(shaped, shaped, sem)

    def want_copy(off):
        return rcopy(
            want_mine,
            want_all.at[me],
            send_w,
            recv_w,
            lax.rem(me + off, devices),
        )

    def own_query(there, side, piece, way):
        return rcopy(
            rq.at[side, piece],
            qbuf.at[me, piece],
            send_q.at[way],
            recv_q.at[me, piece],
            there * 2 + side,
        )

    def pass_query(source, piece, there, way):
        return rcopy(
            qbuf.at[source, piece],
            qbuf.at[source, piece],
            send_q.at[way],
            recv_q.at[source, piece],
            there * 2 + core,
        )

    def await_query(source, piece):
        pass_query(source, piece, sibling // 2, 0).wait_recv()

    def result_to(source, piece, dst, dstat, rsem, gsem, target):
        return (
            rcopy(obuf.at[source, piece], dst, send_r, rsem, target),
            rcopy(sbuf.at[source, piece], dstat, send_s, gsem, target),
        )

    def pass_result(source, piece, there):
        return result_to(
            source,
            piece,
            rbuf.at[source, piece],
            rstat.at[source, piece],
            recv_q.at[source, piece],
            recv_s.at[source, piece],
            there * 2 + core,
        )

    def give_result(source, piece, side):
        return result_to(
            source,
            piece,
            fin.at[side, core, piece],
            fstat.at[side, core, piece],
            recv_f.at[side, core, piece],
            recv_g.at[side, core, piece],
            source,
        )

    def await_result(source, piece):
        for copy in pass_result(source, piece, sibling // 2):
            copy.wait_recv()

    def await_final(side, which, piece):
        copies = result_to(
            me,
            piece,
            fin.at[side, which, piece],
            fstat.at[side, which, piece],
            recv_f.at[side, which, piece],
            recv_g.at[side, which, piece],
            sibling,
        )
        for copy in copies:
            copy.wait_recv()

    def begin(copies):
        for copy in copies if isinstance(copies, tuple) else (copies,):
            copy.start()

    def job(source, piece, own=False):
        def named(block):
            at = piece * piece_blocks + block
            return [
                (
                    want_smem[source, 0, place * blocks + at],
                    want_smem[source, 0, (per + place) * blocks + at],
                )
                for place in range(per)
            ]

        if own:
            return (
                rq.at[core, piece], named, fin.at[2, core, piece], fstat.at[2, core, piece]
            )
        return (qbuf.at[source, piece], named, obuf.at[source, piece], sbuf.at[source, piece])

    def attend(*jobs):
        attend_jobs(jobs, me, sibling, kv_own, kv_sib, head_dim)

    def attend_here():
        @pl.loop(0, pieces)
        def _(piece):
            await_query(sibling, piece)
            attend(job(me, piece, own=True), job(sibling, piece))
            begin(give_result(sibling, piece, 2))

    def merge(source, piece):
        await_result(source, piece)
        refs = [obuf.at[source, piece], rbuf.at[source, piece]]
        shares, stat = shares_of([sbuf[source, piece], rstat[source, piece]])
        for block in range(piece_blocks):
            for local in range(here):
                value = blend(refs, shares, block, local, head_dim)
                obuf[
                    source,
                    piece,
                    block * BLOCK : (block + 1) * BLOCK,
                    local * head_dim : (local + 1) * head_dim,
                ] = value.astype(BF16)
        sbuf[source, piece] = stat

    inner = jnp.logical_and(chip > 0, chip < chips - 1)
    end = jnp.logical_or(chip == 0, chip == chips - 1)
    near = 2 * (chip // reach) - 1
    far = -near
    near_side, far_side = (1 - near) // 2, (1 - far) // 2

    def own_first(piece):
        @pl.when(inner)
        def _():
            own_query(chip + near, core, piece, 0).start()
            own_query(chip + far, core, piece, 1).start()

        @pl.when(end)
        def _():
            own_query(chip + far, core, piece, 1).start()

    with jax.named_scope("rq0"):
        project_query(core, 0)
    with jax.named_scope("barrier_wait"):
        pl.semaphore_wait(barrier, devices - 1)
    with jax.named_scope("rq1"):

        @pl.loop(1, devices)
        def _(off):
            want_copy(off).start()

        own_first(0)
        for copy in second_loads:
            copy.wait()
        loads[1 + pv_w].start()
        for piece in range(1, pieces):
            project_query(core, piece)
            own_first(piece)
        for copy in lesser_loads[2:]:
            copy.start()
        for piece in range(pieces):
            project_query(other, piece)

    @pl.when(end)
    def _():
        for piece in range(pieces):
            own_query(chip + far, other, piece, 1).start()

    def sib_copy(piece):
        return rcopy(
            rq.at[other, piece], qbuf.at[me, piece], send_h, recv_q.at[me, piece], sibling
        )

    rows = sto.shape[0]
    tile = min(512, rows)

    def project_store(which, weight, dst, place, m):
        cols = pl.ds(pl.multiple_of(which * half, half), half)
        at = pl.ds(pl.multiple_of(m * tile, tile), tile)
        held = dot_nn(sto[at, :], wts[weight, :, cols]).astype(BF16)
        count = tile // passage_rows
        dst[pl.ds(m * count, count), :, place * half : (place + 1) * half] = held.reshape(
            count, passage_rows, half
        )

    def relay_first(piece):
        edge, peer = chip + near, chip + far

        @pl.when(inner)
        def _():
            await_query(edge * 2 + core, piece)
            pass_query(edge * 2 + core, piece, peer, 1).start()
            await_query(peer * 2 + core, piece)
            pass_query(peer * 2 + core, piece, edge, 0).start()

    tiles = rows // tile
    with jax.named_scope("kv"):
        loads[7].wait()
        loads[1 + pk_w].wait()
        for i in range(3):
            loads[1 + q_w + i].start()

        @pl.loop(0, tiles)
        def _(m):
            project_store(other, pk_w, kv_out, 0, m)

        loads[1 + pv_w].wait()

        @pl.loop(0, tiles)
        def _(m):
            project_store(other, pv_w, kv_out, 1, m)

        swap = rcopy(kv_out, kv_sib, kv_sem.at[0], kv_sem.at[1], sibling)
        swap.start()
        for piece in range(pieces):
            sib_copy(piece).start()

        project_store(core, pk_w, kv_own, 0, 0)
    with jax.named_scope("relay0"):
        relay_first(0)
    with jax.named_scope("kv2"):

        @pl.loop(1, tiles)
        def _(m):
            project_store(core, pk_w, kv_own, 0, m)

        all_of(want_all.at[pl.ds(0, devices - 1)], recv_w).wait()
        fetch = pltpu.make_async_copy(want_all, want_smem, want_sem)
        fetch.start()

        @pl.loop(0, tiles)
        def _(m):
            project_store(core, pv_w, kv_own, 1, m)

    with jax.named_scope("relay1"):
        for piece in range(1, pieces):
            relay_first(piece)

    def project_mixer(step):
        i, side = step // 2, lax.rem(step, 2)
        cols = pl.ds(pl.multiple_of(side * half, half), half)
        qkv[i, :, cols] = dot_nn(tok[...], wts[q_w + i, :, cols]).astype(BF16)

    def project_gates():
        small = jnp.concatenate(
            [ref[...] for ref in small_refs]
            + [jnp.zeros((16 - 3 * heads, tok.shape[1]), BF16)],
            axis=0,
        )
        gate_ref[...] = dot_nt(tok[...], small)

    with jax.named_scope("wants"):

        fetch.wait()
        swap.wait()
        for copy in lesser_loads[2:]:
            copy.wait()
        all_of(wts.at[pl.ds(q_w, 3)], load_sem.at[4]).wait()

    @pl.when(inner)
    def _():
        edge, peer, beyond = chip + near, chip + far, chip + 2 * far

        def at(where, which):
            return where * 2 + which

        with jax.named_scope("in01"):

            @pl.loop(0, pieces)
            def _(piece):
                attend(job(at(edge, core), piece), job(at(peer, core), piece))

        with jax.named_scope("in23"):

            @pl.loop(0, pieces)
            def _(piece):
                await_query(at(edge, other), piece)
                pass_query(at(edge, other), piece, peer, 1).start()
                await_query(at(beyond, core), piece)
                pass_query(at(beyond, core), piece, edge, 0).start()
                attend(job(at(edge, other), piece), job(at(beyond, core), piece))

                @pl.loop(2 * piece, 2 * piece + 2)
                def _(step):
                    project_mixer(step)


        for piece in range(pieces):
            own_query(peer, other, piece, 1).start()
        with jax.named_scope("in45"):

            @pl.loop(0, pieces)
            def _(piece):
                await_query(at(beyond, other), piece)
                pass_query(at(beyond, other), piece, edge, 0).start()
                attend(job(at(beyond, other), piece))
                project_mixer(2 * pieces + piece)

        with jax.named_scope("in_here"):
            attend_here()
        with jax.named_scope("in67"):

            @pl.loop(0, pieces)
            def _(piece):
                await_query(at(peer, other), piece)
                pass_query(at(peer, other), piece, edge, 0).start()
                merge(at(beyond, core), piece)
                begin(pass_result(at(beyond, core), piece, peer))
                attend(job(at(peer, other), piece))

        for piece in range(pieces):
            own_query(edge, other, piece, 0).start()
        with jax.named_scope("in89"):

            @pl.loop(0, pieces)
            def _(piece):
                merge(at(beyond, other), piece)
                begin(pass_result(at(beyond, other), piece, peer))
                merge(at(edge, core), piece)
                begin(give_result(at(edge, core), piece, near_side))

        project_gates()
        with jax.named_scope("in1011"):

            @pl.loop(0, pieces)
            def _(piece):
                merge(at(peer, core), piece)
                begin(give_result(at(peer, core), piece, far_side))
                merge(at(edge, other), piece)
                begin(give_result(at(edge, other), piece, near_side))

        with jax.named_scope("in12"):

            @pl.loop(0, pieces)
            def _(piece):
                merge(at(peer, other), piece)
                begin(give_result(at(peer, other), piece, far_side))

    @pl.when(end)
    def _():
        def at(distance, which):
            return (chip + far * distance) * 2 + which

        def handle(distance, which, send, fill=None):
            @pl.loop(0, pieces)
            def _(piece):
                await_query(at(distance, which), piece)
                attend(job(at(distance, which), piece))
                if send:
                    if distance == 1:
                        begin(give_result(at(distance, which), piece, far_side))
                    else:
                        begin(pass_result(at(distance, which), piece, chip + far))
                if fill is not None:
                    fill(piece)

        def fill_two(piece):
            @pl.loop(2 * piece, 2 * piece + 2)
            def _(step):
                project_mixer(step)

        def fill_one(piece):
            project_mixer(2 * pieces + piece)

        with jax.named_scope("end01"):
            handle(1, core, False)
        with jax.named_scope("end23"):
            handle(2, core, True, fill_two)
        with jax.named_scope("end45"):
            handle(3, core, True, fill_one)
        with jax.named_scope("end_here"):
            attend_here()
        with jax.named_scope("end67"):
            handle(3, other, True)
        with jax.named_scope("end89"):
            handle(2, other, True)
        for piece in range(pieces):
            begin(give_result(at(1, core), piece, far_side))
        project_gates()
        with jax.named_scope("end1011"):
            handle(1, other, True)

    with jax.named_scope("gates"):
        spans = gate_rows(gate_ref[...], extra_ref, rate_ref)
        for span, held in enumerate(spans):
            for side in range(2):
                rgate = held[6][side * here : (side + 1) * here]
                gsel[side, span * SPAN : (span + 1) * SPAN, :8] = jnp.transpose(
                    jnp.concatenate([rgate, jnp.zeros((8 - here, SPAN), F32)], axis=0)
                )

    def read(name, head, span):
        return qkv[
            "qkv".index(name),
            span * SPAN : (span + 1) * SPAN,
            head * head_dim : (head + 1) * head_dim,
        ]

    def keep(head, span, value):
        normed[span * SPAN : (span + 1) * SPAN, head * head_dim : (head + 1) * head_dim] = value

    with jax.named_scope("delta"):
        delta_body(spans, read, gain_ref[...], heads, keep)

    def finish(which, piece, sides):
        @pl.when(which == other)
        def _():
            await_final(2, which, piece)

        for side in sides[:-1]:
            await_final(side, which, piece)
        refs = [fin.at[side, which, piece] for side in sides]
        shares, _ = shares_of([fstat[side, which, piece] for side in sides])
        for block in range(piece_blocks):
            at = pl.ds(pl.multiple_of(piece * piece_rows + block * BLOCK, BLOCK), BLOCK)
            for local in range(here):
                cols = pl.ds(
                    pl.multiple_of(which * half + local * head_dim, head_dim), head_dim
                )
                value = blend(refs, shares, block, local, head_dim)
                rgate = gsel[which, at, local : local + 1]
                o_ref[at, cols] = (normed[at, cols] + rgate * value).astype(BF16)

    def finish_all(sides):
        @pl.loop(0, 2 * pieces)
        def _(step):
            finish(lax.rem(core + step // pieces, 2), lax.rem(step, pieces), sides)

    with jax.named_scope("finish"):

        @pl.when(inner)
        def _():
            finish_all((0, 1, 2))

        @pl.when(end)
        def _():
            finish_all((1 - far_side, 2))

    all_of(want_all.at[pl.ds(0, devices - 1)], send_w).wait()
    all_of(qbuf.at[0], send_h).wait()
    all_of(obuf.at[pl.ds(0, devices - 1)], send_r).wait()
    all_of(sbuf.at[pl.ds(0, devices - 1)], send_s).wait()

    @pl.when(inner)
    def _():
        all_of(qbuf.at[pl.ds(0, 6)], send_q.at[0]).wait()
        all_of(qbuf.at[pl.ds(0, 4)], send_q.at[1]).wait()

    @pl.when(end)
    def _():
        all_of(qbuf.at[pl.ds(0, 2)], send_q.at[1]).wait()


def line_device(
    chips,
    tokens,
    owners,
    entries,
    store,
    mixer_query_weight,
    mixer_key_weight,
    mixer_value_weight,
    strength_weight,
    decay_weight,
    head_decay_rate,
    extra_forgetting_exponent,
    output_norm_gain,
    retrieval_query_weight,
    passage_key_weight,
    passage_value_weight,
    retrieval_gate_weight,
):
    heads = head_decay_rate.shape[0]
    head_dim = output_norm_gain.shape[0]
    length, depth = tokens.shape
    passage_rows = store.shape[1]
    rows = store.shape[0] * passage_rows
    width = heads * head_dim
    half = width // 2
    devices = 2 * chips
    blocks = owners.shape[0]
    pieces = 2
    piece_rows, piece_blocks = length // pieces, blocks // pieces
    lanes = 2 * BLOCK
    vmem = pl.BlockSpec(memory_space=pltpu.VMEM)
    anywhere = pl.BlockSpec(memory_space=pltpu.HBM)
    weights = [
        retrieval_query_weight,
        passage_key_weight,
        passage_value_weight,
        mixer_query_weight,
        mixer_key_weight,
        mixer_value_weight,
    ]

    def body(*refs):
        whole_kernel(
            chips, head_dim, passage_rows, refs[:8], refs[8], refs[9], refs[10:16], *refs[16:]
        )

    dma = pltpu.SemaphoreType.DMA
    call = pl.pallas_call(
        body,
        out_shape=jax.ShapeDtypeStruct((length, width), BF16),
        in_specs=[anywhere] * 16,
        out_specs=vmem,
        scratch_shapes=[
            pltpu.VMEM(owners.shape[::-1], jnp.int32),
            pltpu.VMEM(owners.shape[::-1], jnp.int32),
            pltpu.VMEM((heads, length), F32),
            pltpu.VMEM((heads, depth), BF16),
            pltpu.VMEM((heads, depth), BF16),
            pltpu.VMEM((heads, depth), BF16),
            pltpu.VMEM((1, head_dim), F32),
            pltpu.VMEM((1, heads), F32),
            pltpu.VMEM((length, 16), F32),
            pltpu.VMEM((length, depth), BF16),
            pltpu.VMEM((rows, depth), BF16),
            pltpu.VMEM((6, depth, width), BF16),
            pltpu.VMEM((2, pieces, piece_rows, half), BF16),
            pltpu.VMEM((3, length, width), BF16),
            pltpu.VMEM((store.shape[0], passage_rows, width), BF16),
            pltpu.VMEM((store.shape[0], passage_rows, width), BF16),
            pltpu.VMEM((store.shape[0], passage_rows, width), BF16),
            pltpu.VMEM((devices, pieces, piece_rows, half), BF16),
            pltpu.VMEM((devices, pieces, piece_rows, half), BF16),
            pltpu.VMEM((devices, pieces, piece_blocks, lanes), F32),
            pltpu.VMEM((devices, pieces, piece_rows, half), BF16),
            pltpu.VMEM((devices, pieces, piece_blocks, lanes), F32),
            pltpu.VMEM((3, 2, pieces, piece_rows, half), BF16),
            pltpu.VMEM((3, 2, pieces, piece_blocks, lanes), F32),
            pltpu.VMEM((length, width), F32),
            pltpu.VMEM((2, length, 128), F32),
            pltpu.VMEM((1, 128), jnp.int32),
            pltpu.VMEM((devices, 1, 128), jnp.int32),
            pltpu.SMEM((devices, 1, 128), jnp.int32),
            dma((6 + pieces + 8,)),
            dma,
            dma((2,)),
            dma((2,)),
            dma((devices, pieces)),
            dma,
            dma,
            dma((devices, pieces)),
            dma((3, 2, pieces)),
            dma((3, 2, pieces)),
            dma,
            dma,
            dma,
        ],
        compiler_params=pltpu.CompilerParams(
            collective_id=0, has_side_effects=True, vmem_limit_bytes=54000 * 1024
        ),
        cost_estimate=pl.CostEstimate(
            flops=12_000_000_000, bytes_accessed=20_000_000, transcendentals=0
        ),
        name="whole",
    )
    operands = (
        owners.T,
        entries.T,
        extra_forgetting_exponent.T,
        strength_weight.T,
        decay_weight.T,
        retrieval_gate_weight.T,
        output_norm_gain[None, :],
        head_decay_rate[None, :],
        tokens,
        store.reshape(rows, depth),
        *weights,
    )
    return call(*[pltpu.with_memory_space_constraint(array, pltpu.HBM) for array in operands])


def ring_attend(q_ref, named, me, sibling, kv_own, kv_sib, o_ref, stat_ref, passage_rows, head_dim):
    length, half = q_ref.shape
    heads = half // head_dim
    blocks = length // BLOCK
    scale = head_dim ** (-0.5)
    nothing = jnp.zeros((BLOCK, head_dim), BF16)

    def find(pairs, device):
        hit = jnp.int32(0)
        for owner, entry in pairs:
            hit = hit + (owner == device).astype(jnp.int32) * (entry + 1)
        found = jnp.minimum(hit, 1)
        return hit - found, (1 - found).astype(F32) * MISSING

    places, scores = [], []
    for block in range(blocks):
        pairs = named(block)
        row_own, bias_own = find(pairs, me)
        row_sib, bias_sib = find(pairs, sibling)
        places.append((row_own, bias_own, row_sib, bias_sib))
        query = q_ref[block * BLOCK : (block + 1) * BLOCK, :]
        spread = jnp.concatenate(
            [
                jnp.concatenate(
                    [
                        query[:, head * head_dim : (head + 1) * head_dim] if head == place else nothing
                        for place in range(heads)
                    ],
                    axis=1,
                )
                for head in range(heads)
            ],
            axis=0,
        )
        keys = jnp.concatenate(
            [
                kv_own[row_own, :, :half],
                kv_sib[row_sib, :, :half],
            ],
            axis=0,
        )
        scores.append(dot_nt(keys, spread))
    weights, stats = [], []
    for block in range(blocks):
        _, bias_own, _, bias_sib = places[block]
        raw = scores[block]
        own = raw[:passage_rows] * scale + bias_own
        sib = raw[passage_rows:] * scale + bias_sib
        peak = jnp.max(jnp.maximum(own, sib), axis=0, keepdims=True)
        e_own = jnp.exp(own - peak)
        e_sib = jnp.exp(sib - peak)
        total = jnp.sum(e_own + e_sib, axis=0, keepdims=True)
        inv = 1.0 / total
        weights.append(jnp.concatenate([e_own * inv, e_sib * inv], axis=0).astype(BF16))
        stats.append(peak + jnp.log(total))
    for block in range(blocks):
        row_own, _, row_sib, _ = places[block]
        values = jnp.concatenate(
            [
                kv_own[row_own, :, half:],
                kv_sib[row_sib, :, half:],
            ],
            axis=0,
        )
        result = dot_tn(weights[block], values)
        for head in range(heads):
            cols = slice(head * head_dim, (head + 1) * head_dim)
            o_ref[block * BLOCK : (block + 1) * BLOCK, cols] = result[
                head * BLOCK : (head + 1) * BLOCK, cols
            ].astype(BF16)
    rows = jnp.concatenate(stats, axis=0)
    spare = stat_ref.shape[1] - rows.shape[1]
    if spare:
        rows = jnp.concatenate([rows, jnp.zeros((blocks, spare), F32)], axis=1)
    stat_ref[...] = rows


def ring_kernel(
    chips,
    head_dim,
    passage_rows,
    owners_ref,
    entries_ref,
    extra_ref,
    small_refs,
    gain_ref,
    rate_ref,
    tokens_hbm,
    store_hbm,
    weights_hbm,
    o_ref,
    tok,
    sto,
    wts,
    rq,
    qkv,
    kv_own,
    kv_sib,
    kv_out,
    qbuf,
    obuf,
    sbuf,
    part,
    pstat,
    normed,
    want_mine,
    want_all,
    want_smem,
    load_sem,
    want_sem,
    kv_sem,
    send_q,
    recv_q,
    send_r,
    recv_r,
    send_s,
    recv_s,
    send_w,
    recv_w,
):
    devices = 2 * chips
    reach = chips // 2
    me = lax.axis_index("st")
    core, chip = lax.rem(me, 2), me // 2
    other = 1 - core
    sibling = chip * 2 + other
    length, width = normed.shape
    half = width // 2
    heads = width // head_dim

    def device(dz, which):
        return lax.rem(chip + dz, chips) * 2 + which

    def rcopy(src, dst, ssem, rsem, target):
        return pltpu.make_async_remote_copy(
            src_ref=src,
            dst_ref=dst,
            send_sem=ssem,
            recv_sem=rsem,
            device_id={"st": target},
            device_id_type=pl.DeviceIdType.MESH,
        )

    barrier = pltpu.get_barrier_semaphore()

    @pl.loop(1, devices)
    def _(off):
        pl.semaphore_signal(
            barrier,
            inc=1,
            device_id={"st": lax.rem(me + off, devices)},
            device_id_type=pl.DeviceIdType.MESH,
        )

    rq_w, pk_w, pv_w, q_w = 0, 1, 2, 3
    loads = [pltpu.make_async_copy(tokens_hbm, tok, load_sem.at[0])]
    loads += [
        pltpu.make_async_copy(weights_hbm[i], wts.at[i], load_sem.at[1 + i]) for i in range(6)
    ]
    loads.append(pltpu.make_async_copy(store_hbm, sto, load_sem.at[7]))
    loads[0].start()
    loads[1].start()

    want_mine[...] = jnp.zeros_like(want_mine)
    per = owners_ref.shape[0]
    blocks = owners_ref.shape[1]
    want_mine[:per, :blocks] = owners_ref[...]
    want_mine[per : 2 * per, :blocks] = entries_ref[...]
    want_all[me] = want_mine[...]

    loads[0].wait()
    loads[1].wait()
    loads[7].start()
    loads[1 + pk_w].start()
    loads[1 + pv_w].start()

    @pl.loop(0, 2)
    def _(side):
        cols = pl.ds(pl.multiple_of(side * half, half), half)
        rq[side] = dot_nn(tok[...], wts[rq_w, :, cols]).astype(BF16)

    pl.semaphore_wait(barrier, devices - 1)

    def slot(dz, which):
        return (dz % chips) * 2 + which

    hop1 = []
    for count, (dz, which) in enumerate(
        [(1, core), (chips - 1, other), (1, other), (chips - 1, core)]
    ):
        there = slot(chips - dz, core)
        hop1.append(
            rcopy(
                rq.at[which], qbuf.at[there], send_q.at[count], recv_q.at[there], device(dz, which)
            )
        )
    hop1.append(
        rcopy(rq.at[other], qbuf.at[core], send_q.at[4], recv_q.at[core], sibling)
    )
    for copy in hop1:
        copy.start()

    def want_copy(off):
        return rcopy(
            want_mine,
            want_all.at[me],
            send_w.at[off - 1],
            recv_w.at[me],
            lax.rem(me + off, devices),
        )

    @pl.loop(1, devices)
    def _(off):
        want_copy(off).start()

    qbuf[core] = rq[core]

    loads[7].wait()
    loads[1 + pk_w].wait()
    for i in range(3):
        loads[1 + q_w + i].start()

    rows = sto.shape[0]
    tile = min(512, rows)

    def project_store(which, weight, dst, place):
        cols = pl.ds(pl.multiple_of(which * half, half), half)

        @pl.loop(0, rows // tile)
        def _(m):
            at = pl.ds(pl.multiple_of(m * tile, tile), tile)
            held = dot_nn(sto[at, :], wts[weight, :, cols]).astype(BF16)
            count = tile // passage_rows
            dst[pl.ds(m * count, count), :, place * half : (place + 1) * half] = held.reshape(
                count, passage_rows, half
            )

    project_store(other, pk_w, kv_out, 0)
    loads[1 + pv_w].wait()
    project_store(other, pv_w, kv_out, 1)
    project_store(core, pk_w, kv_own, 0)
    swap = rcopy(kv_out, kv_sib, kv_sem.at[0], kv_sem.at[1], sibling)
    swap.start()
    project_store(core, pv_w, kv_own, 1)

    for i in range(3):
        loads[1 + q_w + i].wait()

    @pl.loop(0, 6)
    def _(step):
        i, side = step // 2, lax.rem(step, 2)
        cols = pl.ds(pl.multiple_of(side * half, half), half)
        qkv[i, :, cols] = dot_nn(tok[...], wts[q_w + i, :, cols]).astype(BF16)

    small = jnp.concatenate(
        [ref[...] for ref in small_refs] + [jnp.zeros((16 - 3 * heads, tok.shape[1]), BF16)], axis=0
    )
    gates = dot_nt(tok[...], small)
    spans = gate_rows(gates, extra_ref, rate_ref)

    @pl.loop(1, devices)
    def _(off):
        source = lax.rem(me + off, devices)
        rcopy(want_mine, want_all.at[source], send_w.at[0], recv_w.at[source], source).wait_recv()

    fetch = pltpu.make_async_copy(want_all, want_smem, want_sem)
    fetch.start()
    fetch.wait()
    swap.wait()

    def await_query(at):
        rcopy(rq.at[0], qbuf.at[at], send_q.at[0], recv_q.at[at], sibling).wait_recv()

    def attend(dz, which):
        at = slot(dz, which)
        source = device(dz, which)

        def named(block):
            return [
                (want_smem[source, place, block], want_smem[source, per + place, block])
                for place in range(per)
            ]

        ring_attend(
            qbuf.at[at],
            named,
            me,
            sibling,
            kv_own,
            kv_sib,
            obuf.at[at],
            sbuf.at[at],
            passage_rows,
            head_dim,
        )

    def reply(dz, which):
        at = slot(dz, which)
        back = (chips - dz) % chips
        target = device(dz, which)
        return (
            rcopy(
                obuf.at[at], part.at[back, core], send_r.at[at], recv_r.at[back, core], target
            ),
            rcopy(
                sbuf.at[at], pstat.at[back, core], send_s.at[at], recv_s.at[back, core], target
            ),
        )

    relays = []

    def relay(src, dst, count, target):
        copy = rcopy(qbuf.at[src], qbuf.at[dst], send_q.at[count], recv_q.at[dst], target)
        copy.start()
        relays.append(copy)

    count = 5
    await_query(other)

    @pl.loop(0, 2)
    def _(which):
        attend(0, which)

    part[0, core] = obuf[core]
    pstat[0, core] = sbuf[core]
    for copy in reply(0, other):
        copy.start()

    for hop in range(1, reach):
        back = chips - hop
        if hop < reach - 1:
            for which in range(2):
                await_query(slot(back, which))
                relay(slot(back, which), slot(back - 1, which), count, device(1, core))
                await_query(slot(hop, which))
                relay(slot(hop, which), slot(hop + 1, which), count + 1, device(chips - 1, core))
                count += 2
        else:
            await_query(slot(back, core))
            relay(slot(back, core), slot(reach, core), count, device(1, core))
            await_query(slot(hop, other))
            relay(slot(hop, other), slot(reach, other), count + 1, device(chips - 1, core))
            count += 2
            await_query(slot(back, other))
            await_query(slot(hop, core))
        for dz in (back, hop):

            @pl.loop(0, 2)
            def _(which):
                attend(dz, which)
                for copy in reply(dz, which):
                    copy.start()

    await_query(slot(reach, 0))
    await_query(slot(reach, 1))

    @pl.loop(0, 2)
    def _(which):
        attend(reach, which)
        for copy in reply(reach, which):
            copy.start()

    def read(name, head, span):
        return qkv[
            "qkv".index(name),
            span * SPAN : (span + 1) * SPAN,
            head * head_dim : (head + 1) * head_dim,
        ]

    def keep(head, span, value):
        normed[span * SPAN : (span + 1) * SPAN, head * head_dim : (head + 1) * head_dim] = value

    delta_body(spans, read, gain_ref[...], heads, keep)

    def await_part(back, side):
        rcopy(
            obuf.at[0], part.at[back, side], send_r.at[0], recv_r.at[back, side], sibling
        ).wait_recv()
        rcopy(
            sbuf.at[0], pstat.at[back, side], send_s.at[0], recv_s.at[back, side], sibling
        ).wait_recv()

    await_part(0, other)
    for back in range(1, chips):
        for side in range(2):
            await_part(back, side)

    here = heads // 2
    for side in range(2):
        stats = [pstat[back, side] for back in range(chips)]
        peak = functools.reduce(jnp.maximum, stats)
        expo = [jnp.exp(stat - peak) for stat in stats]
        inv = 1.0 / functools.reduce(jnp.add, expo)
        shares = [jnp.transpose(e * inv) for e in expo]
        for block in range(blocks):
            at = slice(block * BLOCK, (block + 1) * BLOCK)
            span, inside = divmod(block * BLOCK, SPAN)
            for local in range(here):
                cols = slice(local * head_dim, (local + 1) * head_dim)
                head = side * here + local
                where = slice(head * head_dim, (head + 1) * head_dim)
                value = functools.reduce(
                    jnp.add,
                    [
                        part[back, side, at, cols].astype(F32)
                        * shares[back][local * BLOCK : (local + 1) * BLOCK, block : block + 1]
                        for back in range(chips)
                    ],
                )
                rgate = spans[span][5][
                    inside : inside + BLOCK, 3 * heads + head : 3 * heads + head + 1
                ]
                o_ref[at, where] = (normed[at, where] + rgate * value).astype(BF16)

    for copy in hop1 + relays:
        copy.wait_send()

    @pl.loop(1, devices)
    def _(off):
        want_copy(off).wait_send()

    for copy in reply(0, other):
        copy.wait_send()
    for dz in range(1, chips):
        for which in range(2):
            for copy in reply(dz, which):
                copy.wait_send()


def ring_device(
    chips,
    tokens,
    owners,
    entries,
    store,
    mixer_query_weight,
    mixer_key_weight,
    mixer_value_weight,
    strength_weight,
    decay_weight,
    head_decay_rate,
    extra_forgetting_exponent,
    output_norm_gain,
    retrieval_query_weight,
    passage_key_weight,
    passage_value_weight,
    retrieval_gate_weight,
):
    heads = head_decay_rate.shape[0]
    head_dim = output_norm_gain.shape[0]
    length, depth = tokens.shape
    passage_rows = store.shape[1]
    rows = store.shape[0] * passage_rows
    width = heads * head_dim
    half = width // 2
    devices = 2 * chips
    blocks = owners.shape[0]
    vmem = pl.BlockSpec(memory_space=pltpu.VMEM)
    anywhere = pl.BlockSpec(memory_space=pl.ANY)
    weights = [
        retrieval_query_weight,
        passage_key_weight,
        passage_value_weight,
        mixer_query_weight,
        mixer_key_weight,
        mixer_value_weight,
    ]

    def body(owners_ref, entries_ref, extra_ref, s1, s2, s3, gain_ref, rate_ref, tok, sto, *rest):
        ring_kernel(
            chips, head_dim, passage_rows, owners_ref, entries_ref, extra_ref, (s1, s2, s3),
            gain_ref, rate_ref, tok, sto, rest[:6], *rest[6:],
        )

    dma = pltpu.SemaphoreType.DMA
    return pl.pallas_call(
        body,
        out_shape=jax.ShapeDtypeStruct((length, width), BF16),
        in_specs=[vmem] * 8 + [anywhere] * 8,
        out_specs=vmem,
        scratch_shapes=[
            pltpu.VMEM((length, depth), BF16),
            pltpu.VMEM((rows, depth), BF16),
            pltpu.VMEM((6, depth, width), BF16),
            pltpu.VMEM((2, length, half), BF16),
            pltpu.VMEM((3, length, width), BF16),
            pltpu.VMEM((store.shape[0], passage_rows, width), BF16),
            pltpu.VMEM((store.shape[0], passage_rows, width), BF16),
            pltpu.VMEM((store.shape[0], passage_rows, width), BF16),
            pltpu.VMEM((devices, length, half), BF16),
            pltpu.VMEM((devices, length, half), BF16),
            pltpu.VMEM((devices, blocks, 2 * BLOCK), F32),
            pltpu.VMEM((chips, 2, length, half), BF16),
            pltpu.VMEM((chips, 2, blocks, 2 * BLOCK), F32),
            pltpu.VMEM((length, width), F32),
            pltpu.VMEM((8, 128), jnp.int32),
            pltpu.VMEM((devices, 8, 128), jnp.int32),
            pltpu.SMEM((devices, 8, 128), jnp.int32),
            dma((8,)),
            dma,
            dma((2,)),
            dma((5 + 2 * devices,)),
            dma((devices,)),
            dma((devices,)),
            dma((chips, 2)),
            dma((devices,)),
            dma((chips, 2)),
            dma((devices,)),
            dma((devices,)),
        ],
        compiler_params=pltpu.CompilerParams(
            collective_id=0, has_side_effects=True, vmem_limit_bytes=60 * 1024 * 1024
        ),
        cost_estimate=pl.CostEstimate(
            flops=12_000_000_000, bytes_accessed=20_000_000, transcendentals=0
        ),
        name="ring",
    )(
        owners.T,
        entries.T,
        extra_forgetting_exponent.T,
        strength_weight.T,
        decay_weight.T,
        retrieval_gate_weight.T,
        output_norm_gain[None, :],
        head_decay_rate[None, :],
        tokens,
        store.reshape(rows, depth),
        *weights,
    )


def solution(mesh):
    rows = ("grp", "st")
    chips = mesh.shape["st"] // 2
    return jax.shard_map(
        functools.partial(line_device if chips // 2 == 2 else ring_device, chips),
        mesh=mesh,
        in_specs=(
            P(rows, None),
            P(rows, None),
            P(rows, None),
            P(rows, None, None),
            P(None, "tp"),
            P(None, "tp"),
            P(None, "tp"),
            P(None, "tp"),
            P(None, "tp"),
            P("tp"),
            P(rows, "tp"),
            P(),
            P(None, "tp"),
            P(None, "tp"),
            P(None, "tp"),
            P(None, "tp"),
        ),
        out_specs=P(rows, "tp"),
        check_vma=False,
    )
```

```python
import functools

import jax
import jax.numpy as jnp
from jax import lax
from jax.experimental import pallas as pl
from jax.experimental.pallas import tpu as pltpu
from jax.sharding import PartitionSpec as P

BLOCK = 64
EPS = 1e-06
MISSING = -1e30
F32 = jnp.float32
BF16 = jnp.bfloat16
SPAN = 128


def dot_nn(left, right):
    return jnp.dot(left, right, preferred_element_type=F32)


def dot_nt(left, right):
    return lax.dot_general(left, right, (((1,), (1,)), ((), ())), preferred_element_type=F32)


def dot_tn(left, right):
    return lax.dot_general(left, right, (((0,), (0,)), ((), ())), preferred_element_type=F32)


def attend_jobs(jobs, me, sibling, kv_own, kv_sib, head_dim):
    passage_rows, half = kv_own.shape[1], kv_own.shape[2] // 2
    heads = half // head_dim
    scale = head_dim ** (-0.5)
    nothing = jnp.zeros((BLOCK, head_dim), BF16)

    def find(pairs, device):
        hit = jnp.int32(0)
        for owner, entry in pairs:
            hit = hit + (owner == device).astype(jnp.int32) * (entry + 1)
        found = jnp.minimum(hit, 1)
        return hit - found, (1 - found).astype(F32) * MISSING

    work = []
    for q_ref, named, o_ref, stat_ref in jobs:
        for block in range(q_ref.shape[0] // BLOCK):
            pairs = named(block)
            work.append((q_ref, o_ref, block, find(pairs, me), find(pairs, sibling)))
    scores = []
    for q_ref, _, block, (row_own, _), (row_sib, _) in work:
        query = q_ref[block * BLOCK : (block + 1) * BLOCK, :]
        spread = jnp.concatenate(
            [
                jnp.concatenate(
                    [
                        query[:, head * head_dim : (head + 1) * head_dim] if head == place else nothing
                        for place in range(heads)
                    ],
                    axis=1,
                )
                for head in range(heads)
            ],
            axis=0,
        )
        keys = jnp.concatenate([kv_own[row_own, :, :half], kv_sib[row_sib, :, :half]], axis=0)
        scores.append(dot_nt(keys, spread))
    weights, stats = [], []
    for (_, _, _, (_, bias_own), (_, bias_sib)), raw in zip(work, scores):
        own = raw[:passage_rows] * scale + bias_own
        sib = raw[passage_rows:] * scale + bias_sib
        peak = jnp.max(jnp.maximum(own, sib), axis=0, keepdims=True)
        e_own = jnp.exp(own - peak)
        e_sib = jnp.exp(sib - peak)
        total = jnp.sum(e_own + e_sib, axis=0, keepdims=True)
        inv = 1.0 / total
        weights.append(jnp.concatenate([e_own * inv, e_sib * inv], axis=0).astype(BF16))
        stats.append(peak + jnp.log(total))
    for (_, o_ref, block, (row_own, _), (row_sib, _)), weight in zip(work, weights):
        values = jnp.concatenate([kv_own[row_own, :, half:], kv_sib[row_sib, :, half:]], axis=0)
        result = dot_tn(weight, values)
        for head in range(heads):
            cols = slice(head * head_dim, (head + 1) * head_dim)
            o_ref[block * BLOCK : (block + 1) * BLOCK, cols] = result[
                head * BLOCK : (head + 1) * BLOCK, cols
            ].astype(BF16)
    done = 0
    for q_ref, _, _, stat_ref in jobs:
        blocks = q_ref.shape[0] // BLOCK
        rows = jnp.concatenate(stats[done : done + blocks], axis=0)
        done += blocks
        spare = stat_ref.shape[1] - rows.shape[1]
        if spare:
            rows = jnp.concatenate([rows, jnp.zeros((blocks, spare), F32)], axis=1)
        stat_ref[...] = rows


def shares_of(stats):
    peak = functools.reduce(jnp.maximum, stats)
    expo = [jnp.exp(stat - peak) for stat in stats]
    total = functools.reduce(jnp.add, expo)
    inv = 1.0 / total
    pad = (-peak.shape[0]) % 8
    rows = [e * inv for e in expo]
    if pad:
        rows = [jnp.concatenate([r, jnp.zeros((pad, r.shape[1]), F32)], axis=0) for r in rows]
    return [jnp.transpose(r) for r in rows], peak + jnp.log(total)


def blend(refs, shares, block, local, head_dim):
    at = slice(block * BLOCK, (block + 1) * BLOCK)
    cols = slice(local * head_dim, (local + 1) * head_dim)
    return functools.reduce(
        jnp.add,
        [
            ref[at, cols].astype(F32) * share[local * BLOCK : (local + 1) * BLOCK, block : block + 1]
            for ref, share in zip(refs, shares)
        ],
    )


def gate_rows(gates, extra_ref, rate_ref):
    heads, length = extra_ref.shape
    rows = jnp.transpose(gates)
    beta = jax.nn.sigmoid(rows[:heads])
    raw = rows[heads : 2 * heads]
    softplus = jnp.maximum(raw, 0.0) + jnp.log1p(jnp.exp(-jnp.abs(raw)))
    which = lax.broadcasted_iota(jnp.int32, (heads, length), 0)
    rate = jnp.zeros((heads, length), F32)
    for head in range(heads):
        rate = jnp.where(which == head, rate_ref[:, head : head + 1], rate)
    decay = -rate * softplus + extra_ref[...]
    rgate = jax.nn.sigmoid(rows[2 * heads : 3 * heads])
    tri = jnp.where(
        lax.broadcasted_iota(jnp.int32, (SPAN, SPAN), 0)
        <= lax.broadcasted_iota(jnp.int32, (SPAN, SPAN), 1),
        1.0,
        0.0,
    ).astype(F32)
    pad = jnp.zeros((8 - heads, SPAN), F32)
    spans = []
    for span in range(length // SPAN):
        at = slice(span * SPAN, (span + 1) * SPAN)
        cum = jnp.dot(
            jnp.concatenate([decay[:, at], pad], axis=0),
            tri,
            precision=lax.Precision.HIGHEST,
            preferred_element_type=F32,
        )[:heads]
        ends = cum[:, SPAN - 1 : SPAN]
        grow = jnp.exp(cum)
        cols = jnp.transpose(jnp.concatenate([cum, beta[:, at], grow, rgate[:, at]], axis=0))
        spans.append((cum, beta[:, at], beta[:, at] * grow, jnp.exp(ends - cum), jnp.exp(ends), cols, rgate[:, at]))
    return spans


def delta_body(spans, read, gain, heads, store):
    head_dim = gain.shape[1]
    count = len(spans)
    half = SPAN // 2
    row = lax.broadcasted_iota(jnp.int32, (SPAN, SPAN), 0)
    col = lax.broadcasted_iota(jnp.int32, (SPAN, SPAN), 1)
    lower = row >= col
    strict = row > col
    prow = lax.broadcasted_iota(jnp.int32, (half, SPAN), 0)
    plane = lax.broadcasted_iota(jnp.int32, (half, SPAN), 1)
    pcol = plane % half
    is_left = plane < half
    left = jnp.where(is_left, 1.0, 0.0).astype(BF16)
    right = jnp.where(is_left, 0.0, 1.0).astype(BF16)
    eye = jnp.where(prow == pcol, 1.0, 0.0).astype(F32)
    sizes = []
    size = 2
    while size < half:
        sizes.append(size)
        size *= 2

    def cut_of(size):
        return ((prow // (2 * size)) == (pcol // (2 * size))) & ((prow // size) != (pcol // size))

    first = jnp.where(cut_of(1), 1.0, 0.0).astype(F32)
    cuts = []
    for size in sizes:
        cut = jnp.where(cut_of(size), 1.0, 0.0).astype(BF16)
        cuts.append((cut * left, cut * right))
    units = [(head, span) for head in range(heads) for span in range(count)]
    kb, kt, grams, mixes = {}, {}, {}, {}
    for unit in units:
        k32 = read("k", *unit).astype(F32)
        kn = k32 * lax.rsqrt(jnp.sum(k32 * k32, axis=1, keepdims=True) + EPS)
        kb[unit] = kn.astype(BF16)
        kt[unit] = jnp.transpose(kn)
    for unit in units:
        turned = kt[unit].astype(BF16)
        grams[unit] = dot_nn(kb[unit], turned)
        mixes[unit] = dot_nn(read("q", *unit), turned)
    within, packed, corner, inverse = {}, {}, {}, {}
    for unit in units:
        head, span = unit
        cum, _, _, _, _, cols, _ = spans[span]
        spread = cols[:, head : head + 1] - cum[head : head + 1, :]
        damp = jnp.where(lower, jnp.exp(jnp.minimum(spread, 0.0)), 0.0)
        within[unit] = (mixes[unit] * damp).astype(BF16)
        inner = jnp.where(strict, grams[unit] * damp * cols[:, heads + head : heads + head + 1], 0.0)
        pack = jnp.where(is_left, inner[:half], inner[half:])
        packed[unit] = pack.astype(BF16)
        corner[unit] = jnp.where(is_left, inner[half:], 0.0).astype(BF16)
        inverse[unit] = eye - pack * first
    for cut_left, cut_right in cuts:
        parts = {}
        for unit in units:
            piece = packed[unit]
            parts[unit] = dot_nn(
                inverse[unit].astype(BF16),
                jnp.concatenate([piece * cut_left, piece * cut_right], axis=0),
            )
        for unit in units:
            now = inverse[unit].astype(BF16)
            inverse[unit] = inverse[unit] - dot_nn(
                parts[unit].astype(BF16), jnp.concatenate([now * left, now * right], axis=0)
            )
    parts = {}
    for unit in units:
        now = inverse[unit].astype(BF16)
        parts[unit] = dot_nn(corner[unit], jnp.concatenate([now * left, now * right], axis=0))
    zeros = jnp.zeros((half, SPAN), BF16)
    full = {}
    for unit in units:
        now = inverse[unit]
        link = dot_nn(
            now.astype(BF16) * right, jnp.concatenate([zeros, parts[unit].astype(BF16)], axis=0)
        )
        full[unit] = jnp.concatenate(
            [jnp.where(is_left, now, 0.0), jnp.where(is_left, -link, now)], axis=0
        )
    base, key_mix, tails = {}, {}, {}
    for unit in units:
        head, span = unit
        _, beta, beta_grow, tail, _, _, _ = spans[span]
        base[unit] = dot_nn((full[unit] * beta[head : head + 1, :]).astype(BF16), read("v", *unit))
        key_mix[unit] = dot_nn(
            (full[unit] * beta_grow[head : head + 1, :]).astype(BF16), kb[unit]
        ).astype(BF16)
        tails[unit] = (kt[unit] * tail[head : head + 1, :]).astype(BF16)
    state = [jnp.zeros((head_dim, head_dim), F32) for _ in range(heads)]
    for span in range(count):
        reads = [
            dot_nn(
                jnp.concatenate([key_mix[head, span], read("q", head, span)], axis=0),
                state[head].astype(BF16),
            )
            for head in range(heads)
        ]
        fresh = [(base[head, span] - reads[head][:SPAN]).astype(BF16) for head in range(heads)]
        carry = spans[span][4]
        state = [
            state[head] * carry[head : head + 1, :] + dot_nn(tails[head, span], fresh[head])
            for head in range(heads)
        ]
        for head in range(heads):
            cols = spans[span][5]
            grow = cols[:, 2 * heads + head : 2 * heads + head + 1]
            result = reads[head][SPAN:] * grow + dot_nn(within[head, span], fresh[head])
            q32 = read("q", head, span).astype(F32)
            square = jnp.sum(q32 * q32, axis=1, keepdims=True)
            norm = lax.rsqrt(
                jnp.mean(result * result, axis=1, keepdims=True)
                + EPS * head_dim * (square + EPS)
            )
            store(head, span, result * norm * gain)


def whole_kernel(
    chips,
    head_dim,
    passage_rows,
    lesser,
    tokens_hbm,
    store_hbm,
    weights_hbm,
    o_ref,
    owners_ref,
    entries_ref,
    extra_ref,
    small_a,
    small_b,
    small_c,
    gain_ref,
    rate_ref,
    gate_ref,
    tok,
    sto,
    wts,
    rq,
    qkv,
    kv_own,
    kv_sib,
    kv_out,
    qbuf,
    obuf,
    sbuf,
    rbuf,
    rstat,
    fin,
    fstat,
    normed,
    gsel,
    want_mine,
    want_all,
    want_smem,
    load_sem,
    want_sem,
    kv_sem,
    send_q,
    recv_q,
    send_r,
    send_s,
    recv_s,
    recv_f,
    recv_g,
    send_w,
    recv_w,
    send_h,
):
    devices = 2 * chips
    reach = chips // 2
    me = lax.axis_index("st")
    core, chip = lax.rem(me, 2), me // 2
    other = 1 - core
    sibling = chip * 2 + other
    length, width = normed.shape
    half = width // 2
    heads = width // head_dim
    here = heads // 2
    pieces = rq.shape[1]
    piece_rows = length // pieces
    piece_blocks = piece_rows // BLOCK
    per = owners_ref.shape[0]
    blocks = owners_ref.shape[1]

    def rcopy(src, dst, ssem, rsem, target):
        return pltpu.make_async_remote_copy(
            src_ref=src,
            dst_ref=dst,
            send_sem=ssem,
            recv_sem=rsem,
            device_id={"st": target},
            device_id_type=pl.DeviceIdType.MESH,
        )

    rq_w, pk_w, pv_w, q_w = 0, 1, 2, 3

    def token_rows(piece):
        at = pl.ds(piece * piece_rows, piece_rows)
        return pltpu.make_async_copy(tokens_hbm.at[at], tok.at[at], load_sem.at[6 + piece])

    def query_weight(which, index):
        at = pl.ds(pl.multiple_of(which * half, half), half)
        return pltpu.make_async_copy(
            weights_hbm[rq_w].at[:, at], wts.at[rq_w, :, at], load_sem.at[index]
        )

    loads = [None, None]
    loads += [
        pltpu.make_async_copy(weights_hbm[i], wts.at[i], load_sem.at[min(1 + i, 4)])
        for i in range(1, 6)
    ]
    loads.append(pltpu.make_async_copy(store_hbm, sto, load_sem.at[5]))
    first_loads = [token_rows(0), query_weight(core, 0)]
    second_loads = [token_rows(piece) for piece in range(1, pieces)] + [query_weight(other, 1)]
    small_refs = (small_a, small_b, small_c)
    lesser_loads = [
        pltpu.make_async_copy(src, dst, load_sem.at[6 + pieces + i])
        for i, (src, dst) in enumerate(
            zip(lesser, (owners_ref, entries_ref, extra_ref) + small_refs + (gain_ref, rate_ref))
        )
    ]
    barrier = pltpu.get_barrier_semaphore()

    @pl.loop(1, devices)
    def _(off):
        pl.semaphore_signal(
            barrier,
            inc=1,
            device_id={"st": lax.rem(me + off, devices)},
            device_id_type=pl.DeviceIdType.MESH,
        )

    for copy in lesser_loads[:2] + first_loads:
        copy.start()
    lesser_loads[0].wait()
    lesser_loads[1].wait()
    named_rows = [
        ref[place : place + 1, :] for ref in (owners_ref, entries_ref) for place in range(per)
    ]
    want = jnp.concatenate(
        named_rows + [jnp.zeros((1, want_mine.shape[1] - 2 * per * blocks), jnp.int32)], axis=1
    )
    want_mine[...] = want
    want_all[me] = want

    for copy in second_loads:
        copy.start()
    with jax.named_scope("wait_tok"):
        for copy in first_loads:
            copy.wait()
    loads[7].start()
    loads[1 + pk_w].start()

    def project_query(side, piece):
        at = pl.ds(piece * piece_rows, piece_rows)
        cols = pl.ds(pl.multiple_of(side * half, half), half)
        rq[side, piece] = dot_nn(tok[at, :], wts[rq_w, :, cols]).astype(BF16)

    def all_of(shaped, sem):
        return pltpu.make_async_copy(shaped, shaped, sem)

    def want_copy(off):
        return rcopy(
            want_mine,
            want_all.at[me],
            send_w,
            recv_w,
            lax.rem(me + off, devices),
        )

    def own_query(there, side, piece, way):
        return rcopy(
            rq.at[side, piece],
            qbuf.at[me, piece],
            send_q.at[way],
            recv_q.at[me, piece],
            there * 2 + side,
        )

    def pass_query(source, piece, there, way):
        return rcopy(
            qbuf.at[source, piece],
            qbuf.at[source, piece],
            send_q.at[way],
            recv_q.at[source, piece],
            there * 2 + core,
        )

    def await_query(source, piece):
        pass_query(source, piece, sibling // 2, 0).wait_recv()

    def result_to(source, piece, dst, dstat, rsem, gsem, target):
        return (
            rcopy(obuf.at[source, piece], dst, send_r, rsem, target),
            rcopy(sbuf.at[source, piece], dstat, send_s, gsem, target),
        )

    def pass_result(source, piece, there):
        return result_to(
            source,
            piece,
            rbuf.at[source, piece],
            rstat.at[source, piece],
            recv_q.at[source, piece],
            recv_s.at[source, piece],
            there * 2 + core,
        )

    def give_result(source, piece, side):
        return result_to(
            source,
            piece,
            fin.at[side, core, piece],
            fstat.at[side, core, piece],
            recv_f.at[side, core, piece],
            recv_g.at[side, core, piece],
            source,
        )

    def await_result(source, piece):
        for copy in pass_result(source, piece, sibling // 2):
            copy.wait_recv()

    def await_final(side, which, piece):
        copies = result_to(
            me,
            piece,
            fin.at[side, which, piece],
            fstat.at[side, which, piece],
            recv_f.at[side, which, piece],
            recv_g.at[side, which, piece],
            sibling,
        )
        for copy in copies:
            copy.wait_recv()

    def begin(copies):
        for copy in copies if isinstance(copies, tuple) else (copies,):
            copy.start()

    def job(source, piece, own=False):
        def named(block):
            at = piece * piece_blocks + block
            return [
                (
                    want_smem[source, 0, place * blocks + at],
                    want_smem[source, 0, (per + place) * blocks + at],
                )
                for place in range(per)
            ]

        if own:
            return (
                rq.at[core, piece], named, fin.at[2, core, piece], fstat.at[2, core, piece]
            )
        return (qbuf.at[source, piece], named, obuf.at[source, piece], sbuf.at[source, piece])

    def attend(*jobs):
        attend_jobs(jobs, me, sibling, kv_own, kv_sib, head_dim)

    def attend_here():
        @pl.loop(0, pieces)
        def _(piece):
            await_query(sibling, piece)
            attend(job(me, piece, own=True), job(sibling, piece))
            begin(give_result(sibling, piece, 2))

    def merge(source, piece):
        await_result(source, piece)
        refs = [obuf.at[source, piece], rbuf.at[source, piece]]
        shares, stat = shares_of([sbuf[source, piece], rstat[source, piece]])
        for block in range(piece_blocks):
            for local in range(here):
                value = blend(refs, shares, block, local, head_dim)
                obuf[
                    source,
                    piece,
                    block * BLOCK : (block + 1) * BLOCK,
                    local * head_dim : (local + 1) * head_dim,
                ] = value.astype(BF16)
        sbuf[source, piece] = stat

    inner = jnp.logical_and(chip > 0, chip < chips - 1)
    end = jnp.logical_or(chip == 0, chip == chips - 1)
    near = 2 * (chip // reach) - 1
    far = -near
    near_side, far_side = (1 - near) // 2, (1 - far) // 2

    def own_first(piece):
        @pl.when(inner)
        def _():
            own_query(chip + near, core, piece, 0).start()
            own_query(chip + far, core, piece, 1).start()

        @pl.when(end)
        def _():
            own_query(chip + far, core, piece, 1).start()

    with jax.named_scope("rq0"):
        project_query(core, 0)
    with jax.named_scope("barrier_wait"):
        pl.semaphore_wait(barrier, devices - 1)
    with jax.named_scope("rq1"):

        @pl.loop(1, devices)
        def _(off):
            want_copy(off).start()

        own_first(0)
        for copy in second_loads:
            copy.wait()
        loads[1 + pv_w].start()
        for piece in range(1, pieces):
            project_query(core, piece)
        for copy in lesser_loads[2:]:
            copy.start()
        for piece in range(pieces):
            project_query(other, piece)
            if piece + 1 < pieces:
                own_first(piece + 1)

    @pl.when(end)
    def _():
        for piece in range(pieces):
            own_query(chip + far, other, piece, 1).start()

    def sib_copy(piece):
        return rcopy(
            rq.at[other, piece], qbuf.at[me, piece], send_h, recv_q.at[me, piece], sibling
        )

    rows = sto.shape[0]
    tile = min(512, rows)

    def project_store(which, weight, dst, place, m):
        cols = pl.ds(pl.multiple_of(which * half, half), half)
        at = pl.ds(pl.multiple_of(m * tile, tile), tile)
        held = dot_nn(sto[at, :], wts[weight, :, cols]).astype(BF16)
        count = tile // passage_rows
        dst[pl.ds(m * count, count), :, place * half : (place + 1) * half] = held.reshape(
            count, passage_rows, half
        )

    def relay_first(piece):
        edge, peer = chip + near, chip + far

        @pl.when(inner)
        def _():
            await_query(edge * 2 + core, piece)
            pass_query(edge * 2 + core, piece, peer, 1).start()
            await_query(peer * 2 + core, piece)
            pass_query(peer * 2 + core, piece, edge, 0).start()

    tiles = rows // tile
    with jax.named_scope("kv"):
        loads[7].wait()
        loads[1 + pk_w].wait()
        for i in range(3):
            loads[1 + q_w + i].start()

        @pl.loop(0, tiles)
        def _(m):
            project_store(other, pk_w, kv_out, 0, m)

        loads[1 + pv_w].wait()

        @pl.loop(0, tiles)
        def _(m):
            project_store(other, pv_w, kv_out, 1, m)

        swap = rcopy(kv_out, kv_sib, kv_sem.at[0], kv_sem.at[1], sibling)
        swap.start()
        for piece in range(pieces):
            sib_copy(piece).start()

        project_store(core, pk_w, kv_own, 0, 0)
    with jax.named_scope("relay0"):
        relay_first(0)
    with jax.named_scope("kv2"):

        @pl.loop(1, tiles)
        def _(m):
            project_store(core, pk_w, kv_own, 0, m)

        all_of(want_all.at[pl.ds(0, devices - 1)], recv_w).wait()
        fetch = pltpu.make_async_copy(want_all, want_smem, want_sem)
        fetch.start()

        @pl.loop(0, tiles)
        def _(m):
            project_store(core, pv_w, kv_own, 1, m)

    with jax.named_scope("relay1"):
        for piece in range(1, pieces):
            relay_first(piece)

    def project_mixer(step):
        i, side = step // 2, lax.rem(step, 2)
        cols = pl.ds(pl.multiple_of(side * half, half), half)
        qkv[i, :, cols] = dot_nn(tok[...], wts[q_w + i, :, cols]).astype(BF16)

    def project_gates():
        small = jnp.concatenate(
            [ref[...] for ref in small_refs]
            + [jnp.zeros((16 - 3 * heads, tok.shape[1]), BF16)],
            axis=0,
        )
        gate_ref[...] = dot_nt(tok[...], small)

    with jax.named_scope("wants"):

        fetch.wait()
        swap.wait()
        for copy in lesser_loads[2:]:
            copy.wait()
        all_of(wts.at[pl.ds(q_w, 3)], load_sem.at[4]).wait()

    @pl.when(inner)
    def _():
        edge, peer, beyond = chip + near, chip + far, chip + 2 * far

        def at(where, which):
            return where * 2 + which

        with jax.named_scope("in01"):

            @pl.loop(0, pieces)
            def _(piece):
                attend(job(at(edge, core), piece), job(at(peer, core), piece))

        with jax.named_scope("in23"):

            @pl.loop(0, pieces)
            def _(piece):
                await_query(at(edge, other), piece)
                pass_query(at(edge, other), piece, peer, 1).start()
                await_query(at(beyond, core), piece)
                pass_query(at(beyond, core), piece, edge, 0).start()
                attend(job(at(edge, other), piece), job(at(beyond, core), piece))

                @pl.loop(2 * piece, 2 * piece + 2)
                def _(step):
                    project_mixer(step)


        for piece in range(pieces):
            own_query(peer, other, piece, 1).start()
        with jax.named_scope("in45"):

            @pl.loop(0, pieces)
            def _(piece):
                await_query(at(beyond, other), piece)
                pass_query(at(beyond, other), piece, edge, 0).start()
                attend(job(at(beyond, other), piece))
                project_mixer(2 * pieces + piece)

        with jax.named_scope("in_here"):
            attend_here()
        with jax.named_scope("in67"):

            @pl.loop(0, pieces)
            def _(piece):
                await_query(at(peer, other), piece)
                pass_query(at(peer, other), piece, edge, 0).start()
                merge(at(beyond, core), piece)
                begin(pass_result(at(beyond, core), piece, peer))
                attend(job(at(peer, other), piece))

        for piece in range(pieces):
            own_query(edge, other, piece, 0).start()
        with jax.named_scope("in89"):

            @pl.loop(0, pieces)
            def _(piece):
                merge(at(beyond, other), piece)
                begin(pass_result(at(beyond, other), piece, peer))
                merge(at(edge, core), piece)
                begin(give_result(at(edge, core), piece, near_side))

        project_gates()
        with jax.named_scope("in1011"):

            @pl.loop(0, pieces)
            def _(piece):
                merge(at(peer, core), piece)
                begin(give_result(at(peer, core), piece, far_side))
                merge(at(edge, other), piece)
                begin(give_result(at(edge, other), piece, near_side))

        with jax.named_scope("in12"):

            @pl.loop(0, pieces)
            def _(piece):
                merge(at(peer, other), piece)
                begin(give_result(at(peer, other), piece, far_side))

    @pl.when(end)
    def _():
        def at(distance, which):
            return (chip + far * distance) * 2 + which

        def handle(distance, which, send, fill=None):
            @pl.loop(0, pieces)
            def _(piece):
                await_query(at(distance, which), piece)
                attend(job(at(distance, which), piece))
                if send:
                    if distance == 1:
                        begin(give_result(at(distance, which), piece, far_side))
                    else:
                        begin(pass_result(at(distance, which), piece, chip + far))
                if fill is not None:
                    fill(piece)

        def fill_two(piece):
            @pl.loop(2 * piece, 2 * piece + 2)
            def _(step):
                project_mixer(step)

        def fill_one(piece):
            project_mixer(2 * pieces + piece)

        with jax.named_scope("end01"):
            handle(1, core, False)
        with jax.named_scope("end23"):
            handle(2, core, True, fill_two)
        with jax.named_scope("end45"):
            handle(3, core, True, fill_one)
        with jax.named_scope("end_here"):
            attend_here()
        with jax.named_scope("end67"):
            handle(3, other, True)
        with jax.named_scope("end89"):
            handle(2, other, True)
        for piece in range(pieces):
            begin(give_result(at(1, core), piece, far_side))
        project_gates()
        with jax.named_scope("end1011"):
            handle(1, other, True)

    with jax.named_scope("gates"):
        spans = gate_rows(gate_ref[...], extra_ref, rate_ref)
        for span, held in enumerate(spans):
            for side in range(2):
                rgate = held[6][side * here : (side + 1) * here]
                gsel[side, span * SPAN : (span + 1) * SPAN, :8] = jnp.transpose(
                    jnp.concatenate([rgate, jnp.zeros((8 - here, SPAN), F32)], axis=0)
                )

    def read(name, head, span):
        return qkv[
            "qkv".index(name),
            span * SPAN : (span + 1) * SPAN,
            head * head_dim : (head + 1) * head_dim,
        ]

    def keep(head, span, value):
        normed[span * SPAN : (span + 1) * SPAN, head * head_dim : (head + 1) * head_dim] = value

    with jax.named_scope("delta"):
        delta_body(spans, read, gain_ref[...], heads, keep)

    def finish(which, piece, sides):
        @pl.when(which == other)
        def _():
            await_final(2, which, piece)

        for side in sides[:-1]:
            await_final(side, which, piece)
        refs = [fin.at[side, which, piece] for side in sides]
        shares, _ = shares_of([fstat[side, which, piece] for side in sides])
        for block in range(piece_blocks):
            at = pl.ds(pl.multiple_of(piece * piece_rows + block * BLOCK, BLOCK), BLOCK)
            for local in range(here):
                cols = pl.ds(
                    pl.multiple_of(which * half + local * head_dim, head_dim), head_dim
                )
                value = blend(refs, shares, block, local, head_dim)
                rgate = gsel[which, at, local : local + 1]
                o_ref[at, cols] = (normed[at, cols] + rgate * value).astype(BF16)

    def finish_all(sides):
        @pl.loop(0, 2 * pieces)
        def _(step):
            finish(lax.rem(core + step // pieces, 2), lax.rem(step, pieces), sides)

    with jax.named_scope("finish"):

        @pl.when(inner)
        def _():
            finish_all((0, 1, 2))

        @pl.when(end)
        def _():
            finish_all((1 - far_side, 2))

    all_of(want_all.at[pl.ds(0, devices - 1)], send_w).wait()
    all_of(qbuf.at[0], send_h).wait()
    all_of(obuf.at[pl.ds(0, devices - 1)], send_r).wait()
    all_of(sbuf.at[pl.ds(0, devices - 1)], send_s).wait()

    @pl.when(inner)
    def _():
        all_of(qbuf.at[pl.ds(0, 6)], send_q.at[0]).wait()
        all_of(qbuf.at[pl.ds(0, 4)], send_q.at[1]).wait()

    @pl.when(end)
    def _():
        all_of(qbuf.at[pl.ds(0, 2)], send_q.at[1]).wait()


def line_device(
    chips,
    tokens,
    owners,
    entries,
    store,
    mixer_query_weight,
    mixer_key_weight,
    mixer_value_weight,
    strength_weight,
    decay_weight,
    head_decay_rate,
    extra_forgetting_exponent,
    output_norm_gain,
    retrieval_query_weight,
    passage_key_weight,
    passage_value_weight,
    retrieval_gate_weight,
):
    heads = head_decay_rate.shape[0]
    head_dim = output_norm_gain.shape[0]
    length, depth = tokens.shape
    passage_rows = store.shape[1]
    rows = store.shape[0] * passage_rows
    width = heads * head_dim
    half = width // 2
    devices = 2 * chips
    blocks = owners.shape[0]
    pieces = 2
    piece_rows, piece_blocks = length // pieces, blocks // pieces
    lanes = 2 * BLOCK
    vmem = pl.BlockSpec(memory_space=pltpu.VMEM)
    anywhere = pl.BlockSpec(memory_space=pltpu.HBM)
    weights = [
        retrieval_query_weight,
        passage_key_weight,
        passage_value_weight,
        mixer_query_weight,
        mixer_key_weight,
        mixer_value_weight,
    ]

    def body(*refs):
        whole_kernel(
            chips, head_dim, passage_rows, refs[:8], refs[8], refs[9], refs[10:16], *refs[16:]
        )

    dma = pltpu.SemaphoreType.DMA
    call = pl.pallas_call(
        body,
        out_shape=jax.ShapeDtypeStruct((length, width), BF16),
        in_specs=[anywhere] * 16,
        out_specs=vmem,
        scratch_shapes=[
            pltpu.VMEM(owners.shape[::-1], jnp.int32),
            pltpu.VMEM(owners.shape[::-1], jnp.int32),
            pltpu.VMEM((heads, length), F32),
            pltpu.VMEM((heads, depth), BF16),
            pltpu.VMEM((heads, depth), BF16),
            pltpu.VMEM((heads, depth), BF16),
            pltpu.VMEM((1, head_dim), F32),
            pltpu.VMEM((1, heads), F32),
            pltpu.VMEM((length, 16), F32),
            pltpu.VMEM((length, depth), BF16),
            pltpu.VMEM((rows, depth), BF16),
            pltpu.VMEM((6, depth, width), BF16),
            pltpu.VMEM((2, pieces, piece_rows, half), BF16),
            pltpu.VMEM((3, length, width), BF16),
            pltpu.VMEM((store.shape[0], passage_rows, width), BF16),
            pltpu.VMEM((store.shape[0], passage_rows, width), BF16),
            pltpu.VMEM((store.shape[0], passage_rows, width), BF16),
            pltpu.VMEM((devices, pieces, piece_rows, half), BF16),
            pltpu.VMEM((devices, pieces, piece_rows, half), BF16),
            pltpu.VMEM((devices, pieces, piece_blocks, lanes), F32),
            pltpu.VMEM((devices, pieces, piece_rows, half), BF16),
            pltpu.VMEM((devices, pieces, piece_blocks, lanes), F32),
            pltpu.VMEM((3, 2, pieces, piece_rows, half), BF16),
            pltpu.VMEM((3, 2, pieces, piece_blocks, lanes), F32),
            pltpu.VMEM((length, width), F32),
            pltpu.VMEM((2, length, 128), F32),
            pltpu.VMEM((1, 128), jnp.int32),
            pltpu.VMEM((devices, 1, 128), jnp.int32),
            pltpu.SMEM((devices, 1, 128), jnp.int32),
            dma((6 + pieces + 8,)),
            dma,
            dma((2,)),
            dma((2,)),
            dma((devices, pieces)),
            dma,
            dma,
            dma((devices, pieces)),
            dma((3, 2, pieces)),
            dma((3, 2, pieces)),
            dma,
            dma,
            dma,
        ],
        compiler_params=pltpu.CompilerParams(
            collective_id=0, has_side_effects=True, vmem_limit_bytes=54000 * 1024
        ),
        cost_estimate=pl.CostEstimate(
            flops=12_000_000_000, bytes_accessed=20_000_000, transcendentals=0
        ),
        name="whole",
    )
    operands = (
        owners.T,
        entries.T,
        extra_forgetting_exponent.T,
        strength_weight.T,
        decay_weight.T,
        retrieval_gate_weight.T,
        output_norm_gain[None, :],
        head_decay_rate[None, :],
        tokens,
        store.reshape(rows, depth),
        *weights,
    )
    return call(*[pltpu.with_memory_space_constraint(array, pltpu.HBM) for array in operands])


def ring_attend(q_ref, named, me, sibling, kv_own, kv_sib, o_ref, stat_ref, passage_rows, head_dim):
    length, half = q_ref.shape
    heads = half // head_dim
    blocks = length // BLOCK
    scale = head_dim ** (-0.5)
    nothing = jnp.zeros((BLOCK, head_dim), BF16)

    def find(pairs, device):
        hit = jnp.int32(0)
        for owner, entry in pairs:
            hit = hit + (owner == device).astype(jnp.int32) * (entry + 1)
        found = jnp.minimum(hit, 1)
        return hit - found, (1 - found).astype(F32) * MISSING

    places, scores = [], []
    for block in range(blocks):
        pairs = named(block)
        row_own, bias_own = find(pairs, me)
        row_sib, bias_sib = find(pairs, sibling)
        places.append((row_own, bias_own, row_sib, bias_sib))
        query = q_ref[block * BLOCK : (block + 1) * BLOCK, :]
        spread = jnp.concatenate(
            [
                jnp.concatenate(
                    [
                        query[:, head * head_dim : (head + 1) * head_dim] if head == place else nothing
                        for place in range(heads)
                    ],
                    axis=1,
                )
                for head in range(heads)
            ],
            axis=0,
        )
        keys = jnp.concatenate(
            [
                kv_own[row_own, :, :half],
                kv_sib[row_sib, :, :half],
            ],
            axis=0,
        )
        scores.append(dot_nt(keys, spread))
    weights, stats = [], []
    for block in range(blocks):
        _, bias_own, _, bias_sib = places[block]
        raw = scores[block]
        own = raw[:passage_rows] * scale + bias_own
        sib = raw[passage_rows:] * scale + bias_sib
        peak = jnp.max(jnp.maximum(own, sib), axis=0, keepdims=True)
        e_own = jnp.exp(own - peak)
        e_sib = jnp.exp(sib - peak)
        total = jnp.sum(e_own + e_sib, axis=0, keepdims=True)
        inv = 1.0 / total
        weights.append(jnp.concatenate([e_own * inv, e_sib * inv], axis=0).astype(BF16))
        stats.append(peak + jnp.log(total))
    for block in range(blocks):
        row_own, _, row_sib, _ = places[block]
        values = jnp.concatenate(
            [
                kv_own[row_own, :, half:],
                kv_sib[row_sib, :, half:],
            ],
            axis=0,
        )
        result = dot_tn(weights[block], values)
        for head in range(heads):
            cols = slice(head * head_dim, (head + 1) * head_dim)
            o_ref[block * BLOCK : (block + 1) * BLOCK, cols] = result[
                head * BLOCK : (head + 1) * BLOCK, cols
            ].astype(BF16)
    rows = jnp.concatenate(stats, axis=0)
    spare = stat_ref.shape[1] - rows.shape[1]
    if spare:
        rows = jnp.concatenate([rows, jnp.zeros((blocks, spare), F32)], axis=1)
    stat_ref[...] = rows


def ring_kernel(
    chips,
    head_dim,
    passage_rows,
    owners_ref,
    entries_ref,
    extra_ref,
    small_refs,
    gain_ref,
    rate_ref,
    tokens_hbm,
    store_hbm,
    weights_hbm,
    o_ref,
    tok,
    sto,
    wts,
    rq,
    qkv,
    kv_own,
    kv_sib,
    kv_out,
    qbuf,
    obuf,
    sbuf,
    part,
    pstat,
    normed,
    want_mine,
    want_all,
    want_smem,
    load_sem,
    want_sem,
    kv_sem,
    send_q,
    recv_q,
    send_r,
    recv_r,
    send_s,
    recv_s,
    send_w,
    recv_w,
):
    devices = 2 * chips
    reach = chips // 2
    me = lax.axis_index("st")
    core, chip = lax.rem(me, 2), me // 2
    other = 1 - core
    sibling = chip * 2 + other
    length, width = normed.shape
    half = width // 2
    heads = width // head_dim

    def device(dz, which):
        return lax.rem(chip + dz, chips) * 2 + which

    def rcopy(src, dst, ssem, rsem, target):
        return pltpu.make_async_remote_copy(
            src_ref=src,
            dst_ref=dst,
            send_sem=ssem,
            recv_sem=rsem,
            device_id={"st": target},
            device_id_type=pl.DeviceIdType.MESH,
        )

    barrier = pltpu.get_barrier_semaphore()

    @pl.loop(1, devices)
    def _(off):
        pl.semaphore_signal(
            barrier,
            inc=1,
            device_id={"st": lax.rem(me + off, devices)},
            device_id_type=pl.DeviceIdType.MESH,
        )

    rq_w, pk_w, pv_w, q_w = 0, 1, 2, 3
    loads = [pltpu.make_async_copy(tokens_hbm, tok, load_sem.at[0])]
    loads += [
        pltpu.make_async_copy(weights_hbm[i], wts.at[i], load_sem.at[1 + i]) for i in range(6)
    ]
    loads.append(pltpu.make_async_copy(store_hbm, sto, load_sem.at[7]))
    loads[0].start()
    loads[1].start()

    want_mine[...] = jnp.zeros_like(want_mine)
    per = owners_ref.shape[0]
    blocks = owners_ref.shape[1]
    want_mine[:per, :blocks] = owners_ref[...]
    want_mine[per : 2 * per, :blocks] = entries_ref[...]
    want_all[me] = want_mine[...]

    loads[0].wait()
    loads[1].wait()
    loads[7].start()
    loads[1 + pk_w].start()
    loads[1 + pv_w].start()

    @pl.loop(0, 2)
    def _(side):
        cols = pl.ds(pl.multiple_of(side * half, half), half)
        rq[side] = dot_nn(tok[...], wts[rq_w, :, cols]).astype(BF16)

    pl.semaphore_wait(barrier, devices - 1)

    def slot(dz, which):
        return (dz % chips) * 2 + which

    hop1 = []
    for count, (dz, which) in enumerate(
        [(1, core), (chips - 1, other), (1, other), (chips - 1, core)]
    ):
        there = slot(chips - dz, core)
        hop1.append(
            rcopy(
                rq.at[which], qbuf.at[there], send_q.at[count], recv_q.at[there], device(dz, which)
            )
        )
    hop1.append(
        rcopy(rq.at[other], qbuf.at[core], send_q.at[4], recv_q.at[core], sibling)
    )
    for copy in hop1:
        copy.start()

    def want_copy(off):
        return rcopy(
            want_mine,
            want_all.at[me],
            send_w.at[off - 1],
            recv_w.at[me],
            lax.rem(me + off, devices),
        )

    @pl.loop(1, devices)
    def _(off):
        want_copy(off).start()

    qbuf[core] = rq[core]

    loads[7].wait()
    loads[1 + pk_w].wait()
    for i in range(3):
        loads[1 + q_w + i].start()

    rows = sto.shape[0]
    tile = min(512, rows)

    def project_store(which, weight, dst, place):
        cols = pl.ds(pl.multiple_of(which * half, half), half)

        @pl.loop(0, rows // tile)
        def _(m):
            at = pl.ds(pl.multiple_of(m * tile, tile), tile)
            held = dot_nn(sto[at, :], wts[weight, :, cols]).astype(BF16)
            count = tile // passage_rows
            dst[pl.ds(m * count, count), :, place * half : (place + 1) * half] = held.reshape(
                count, passage_rows, half
            )

    project_store(other, pk_w, kv_out, 0)
    loads[1 + pv_w].wait()
    project_store(other, pv_w, kv_out, 1)
    project_store(core, pk_w, kv_own, 0)
    swap = rcopy(kv_out, kv_sib, kv_sem.at[0], kv_sem.at[1], sibling)
    swap.start()
    project_store(core, pv_w, kv_own, 1)

    for i in range(3):
        loads[1 + q_w + i].wait()

    @pl.loop(0, 6)
    def _(step):
        i, side = step // 2, lax.rem(step, 2)
        cols = pl.ds(pl.multiple_of(side * half, half), half)
        qkv[i, :, cols] = dot_nn(tok[...], wts[q_w + i, :, cols]).astype(BF16)

    small = jnp.concatenate(
        [ref[...] for ref in small_refs] + [jnp.zeros((16 - 3 * heads, tok.shape[1]), BF16)], axis=0
    )
    gates = dot_nt(tok[...], small)
    spans = gate_rows(gates, extra_ref, rate_ref)

    @pl.loop(1, devices)
    def _(off):
        source = lax.rem(me + off, devices)
        rcopy(want_mine, want_all.at[source], send_w.at[0], recv_w.at[source], source).wait_recv()

    fetch = pltpu.make_async_copy(want_all, want_smem, want_sem)
    fetch.start()
    fetch.wait()
    swap.wait()

    def await_query(at):
        rcopy(rq.at[0], qbuf.at[at], send_q.at[0], recv_q.at[at], sibling).wait_recv()

    def attend(dz, which):
        at = slot(dz, which)
        source = device(dz, which)

        def named(block):
            return [
                (want_smem[source, place, block], want_smem[source, per + place, block])
                for place in range(per)
            ]

        ring_attend(
            qbuf.at[at],
            named,
            me,
            sibling,
            kv_own,
            kv_sib,
            obuf.at[at],
            sbuf.at[at],
            passage_rows,
            head_dim,
        )

    def reply(dz, which):
        at = slot(dz, which)
        back = (chips - dz) % chips
        target = device(dz, which)
        return (
            rcopy(
                obuf.at[at], part.at[back, core], send_r.at[at], recv_r.at[back, core], target
            ),
            rcopy(
                sbuf.at[at], pstat.at[back, core], send_s.at[at], recv_s.at[back, core], target
            ),
        )

    relays = []

    def relay(src, dst, count, target):
        copy = rcopy(qbuf.at[src], qbuf.at[dst], send_q.at[count], recv_q.at[dst], target)
        copy.start()
        relays.append(copy)

    count = 5
    await_query(other)

    @pl.loop(0, 2)
    def _(which):
        attend(0, which)

    part[0, core] = obuf[core]
    pstat[0, core] = sbuf[core]
    for copy in reply(0, other):
        copy.start()

    for hop in range(1, reach):
        back = chips - hop
        if hop < reach - 1:
            for which in range(2):
                await_query(slot(back, which))
                relay(slot(back, which), slot(back - 1, which), count, device(1, core))
                await_query(slot(hop, which))
                relay(slot(hop, which), slot(hop + 1, which), count + 1, device(chips - 1, core))
                count += 2
        else:
            await_query(slot(back, core))
            relay(slot(back, core), slot(reach, core), count, device(1, core))
            await_query(slot(hop, other))
            relay(slot(hop, other), slot(reach, other), count + 1, device(chips - 1, core))
            count += 2
            await_query(slot(back, other))
            await_query(slot(hop, core))
        for dz in (back, hop):

            @pl.loop(0, 2)
            def _(which):
                attend(dz, which)
                for copy in reply(dz, which):
                    copy.start()

    await_query(slot(reach, 0))
    await_query(slot(reach, 1))

    @pl.loop(0, 2)
    def _(which):
        attend(reach, which)
        for copy in reply(reach, which):
            copy.start()

    def read(name, head, span):
        return qkv[
            "qkv".index(name),
            span * SPAN : (span + 1) * SPAN,
            head * head_dim : (head + 1) * head_dim,
        ]

    def keep(head, span, value):
        normed[span * SPAN : (span + 1) * SPAN, head * head_dim : (head + 1) * head_dim] = value

    delta_body(spans, read, gain_ref[...], heads, keep)

    def await_part(back, side):
        rcopy(
            obuf.at[0], part.at[back, side], send_r.at[0], recv_r.at[back, side], sibling
        ).wait_recv()
        rcopy(
            sbuf.at[0], pstat.at[back, side], send_s.at[0], recv_s.at[back, side], sibling
        ).wait_recv()

    await_part(0, other)
    for back in range(1, chips):
        for side in range(2):
            await_part(back, side)

    here = heads // 2
    for side in range(2):
        stats = [pstat[back, side] for back in range(chips)]
        peak = functools.reduce(jnp.maximum, stats)
        expo = [jnp.exp(stat - peak) for stat in stats]
        inv = 1.0 / functools.reduce(jnp.add, expo)
        shares = [jnp.transpose(e * inv) for e in expo]
        for block in range(blocks):
            at = slice(block * BLOCK, (block + 1) * BLOCK)
            span, inside = divmod(block * BLOCK, SPAN)
            for local in range(here):
                cols = slice(local * head_dim, (local + 1) * head_dim)
                head = side * here + local
                where = slice(head * head_dim, (head + 1) * head_dim)
                value = functools.reduce(
                    jnp.add,
                    [
                        part[back, side, at, cols].astype(F32)
                        * shares[back][local * BLOCK : (local + 1) * BLOCK, block : block + 1]
                        for back in range(chips)
                    ],
                )
                rgate = spans[span][5][
                    inside : inside + BLOCK, 3 * heads + head : 3 * heads + head + 1
                ]
                o_ref[at, where] = (normed[at, where] + rgate * value).astype(BF16)

    for copy in hop1 + relays:
        copy.wait_send()

    @pl.loop(1, devices)
    def _(off):
        want_copy(off).wait_send()

    for copy in reply(0, other):
        copy.wait_send()
    for dz in range(1, chips):
        for which in range(2):
            for copy in reply(dz, which):
                copy.wait_send()


def ring_device(
    chips,
    tokens,
    owners,
    entries,
    store,
    mixer_query_weight,
    mixer_key_weight,
    mixer_value_weight,
    strength_weight,
    decay_weight,
    head_decay_rate,
    extra_forgetting_exponent,
    output_norm_gain,
    retrieval_query_weight,
    passage_key_weight,
    passage_value_weight,
    retrieval_gate_weight,
):
    heads = head_decay_rate.shape[0]
    head_dim = output_norm_gain.shape[0]
    length, depth = tokens.shape
    passage_rows = store.shape[1]
    rows = store.shape[0] * passage_rows
    width = heads * head_dim
    half = width // 2
    devices = 2 * chips
    blocks = owners.shape[0]
    vmem = pl.BlockSpec(memory_space=pltpu.VMEM)
    anywhere = pl.BlockSpec(memory_space=pl.ANY)
    weights = [
        retrieval_query_weight,
        passage_key_weight,
        passage_value_weight,
        mixer_query_weight,
        mixer_key_weight,
        mixer_value_weight,
    ]

    def body(owners_ref, entries_ref, extra_ref, s1, s2, s3, gain_ref, rate_ref, tok, sto, *rest):
        ring_kernel(
            chips, head_dim, passage_rows, owners_ref, entries_ref, extra_ref, (s1, s2, s3),
            gain_ref, rate_ref, tok, sto, rest[:6], *rest[6:],
        )

    dma = pltpu.SemaphoreType.DMA
    return pl.pallas_call(
        body,
        out_shape=jax.ShapeDtypeStruct((length, width), BF16),
        in_specs=[vmem] * 8 + [anywhere] * 8,
        out_specs=vmem,
        scratch_shapes=[
            pltpu.VMEM((length, depth), BF16),
            pltpu.VMEM((rows, depth), BF16),
            pltpu.VMEM((6, depth, width), BF16),
            pltpu.VMEM((2, length, half), BF16),
            pltpu.VMEM((3, length, width), BF16),
            pltpu.VMEM((store.shape[0], passage_rows, width), BF16),
            pltpu.VMEM((store.shape[0], passage_rows, width), BF16),
            pltpu.VMEM((store.shape[0], passage_rows, width), BF16),
            pltpu.VMEM((devices, length, half), BF16),
            pltpu.VMEM((devices, length, half), BF16),
            pltpu.VMEM((devices, blocks, 2 * BLOCK), F32),
            pltpu.VMEM((chips, 2, length, half), BF16),
            pltpu.VMEM((chips, 2, blocks, 2 * BLOCK), F32),
            pltpu.VMEM((length, width), F32),
            pltpu.VMEM((8, 128), jnp.int32),
            pltpu.VMEM((devices, 8, 128), jnp.int32),
            pltpu.SMEM((devices, 8, 128), jnp.int32),
            dma((8,)),
            dma,
            dma((2,)),
            dma((5 + 2 * devices,)),
            dma((devices,)),
            dma((devices,)),
            dma((chips, 2)),
            dma((devices,)),
            dma((chips, 2)),
            dma((devices,)),
            dma((devices,)),
        ],
        compiler_params=pltpu.CompilerParams(
            collective_id=0, has_side_effects=True, vmem_limit_bytes=60 * 1024 * 1024
        ),
        cost_estimate=pl.CostEstimate(
            flops=12_000_000_000, bytes_accessed=20_000_000, transcendentals=0
        ),
        name="ring",
    )(
        owners.T,
        entries.T,
        extra_forgetting_exponent.T,
        strength_weight.T,
        decay_weight.T,
        retrieval_gate_weight.T,
        output_norm_gain[None, :],
        head_decay_rate[None, :],
        tokens,
        store.reshape(rows, depth),
        *weights,
    )


def solution(mesh):
    rows = ("grp", "st")
    chips = mesh.shape["st"] // 2
    return jax.shard_map(
        functools.partial(line_device if chips // 2 == 2 else ring_device, chips),
        mesh=mesh,
        in_specs=(
            P(rows, None),
            P(rows, None),
            P(rows, None),
            P(rows, None, None),
            P(None, "tp"),
            P(None, "tp"),
            P(None, "tp"),
            P(None, "tp"),
            P(None, "tp"),
            P("tp"),
            P(rows, "tp"),
            P(),
            P(None, "tp"),
            P(None, "tp"),
            P(None, "tp"),
            P(None, "tp"),
        ),
        out_specs=P(rows, "tp"),
        check_vma=False,
    )
```
